32 devices in a mesh: grp: 2 (over y), sp: 4 (over z), tp: 4 (over x, core).
Axes of the slice: x: 2, y: 2, z: 4, core: 2. Of those that a mesh axis runs over, the one named last changes fastest.
Arguments:
- latent: bfloat16 [2048, 512], P(('grp', 'sp')), parts along dimension 0, may hold values from -6 to 6
- rope_key: bfloat16 [2048, 64], P(('grp', 'sp')), parts along dimension 0, may hold values from -6 to 6
- wide_query: bfloat16 [2048, 1536], P(('grp', 'sp'), 'tp'), parts along dimension 0, may hold values from -1300 to 1300
- narrow_query: bfloat16 [2048, 1024], P(('grp', 'sp'), 'tp'), parts along dimension 0, may hold values from -1300 to 1300
- wide_key_weight: bfloat16 [512, 1024], P(None, 'tp'), may hold values from -0.25 to 0.25
- wide_value_weight: bfloat16 [512, 1024], P(None, 'tp'), may hold values from -0.25 to 0.25
- narrow_key_weight: bfloat16 [512, 512], P(None, 'tp'), may hold values from -0.25 to 0.25
- narrow_value_weight: bfloat16 [512, 512], P(None, 'tp'), may hold values from -0.25 to 0.25
- latent_norm_scale: float32 [512], replicated, may hold values from 0.1 to 1.9
- out_wide: bfloat16 [1024, 4096], P('tp'), may hold values from -0.4375 to 0.4375
- out_narrow: bfloat16 [512, 4096], P('tp'), may hold values from -0.4375 to 0.4375
- residual: bfloat16 [2048, 4096], P(('grp', 'sp', 'tp')), parts along dimension 0, may hold values from -6 to 6
- ffn_gain: float32 [4096], replicated, may hold values from 0.1 to 1.9
- shared_gate: bfloat16 [4096, 512], P(None, 'tp'), may hold values from -0.09375 to 0.09375
- shared_up: bfloat16 [4096, 512], P(None, 'tp'), may hold values from -0.09375 to 0.09375
- shared_down: bfloat16 [512, 4096], P('tp'), may hold values from -0.25 to 0.25
- expert_gate: bfloat16 [16, 4096, 192], P(('sp', 'tp')), may hold values from -0.09375 to 0.09375
- expert_up: bfloat16 [16, 4096, 192], P(('sp', 'tp')), may hold values from -0.09375 to 0.09375
- expert_down: bfloat16 [16, 192, 4096], P(('sp', 'tp')), may hold values from -0.4375 to 0.4375
- routes: int32 [2048, 2], P(('grp', 'sp', 'tp')), parts along dimension 0, may hold values from 0 to 15, all different within a row; in each aligned block of 64 rows (0 to 63, 64 to 127, ...) at most 16 rows name the same one
- route_weights: float32 [2048, 2], P(('grp', 'sp', 'tp')), parts along dimension 0, may hold values from 0.25 to 1.5
Outputs:
- layer_out: bfloat16 [2048, 4096], P(('grp', 'sp', 'tp')), parts along dimension 0
The draws below stay inside these ranges and needn't reach their ends.
There are 2 independent parts, one for each index of `grp`. The reference program is written for one: setup_inputs(seed, part) draws one part's arguments, and reference() takes and returns one part's arrays. A program takes and returns all parts, laid end to end along the dimension named above; an argument that names none is the same for every part. Nothing has to cross between parts.
Inputs may be any that keep to these rules, and one draw needn't show every extreme that they name: `routes`: each row names 2 different experts; in each aligned block of 64 rows no expert is named by more than 16 rows, and some block has an expert named exactly 16 times.
All inputs are finite; a program needn't handle non-finite values.
Results may differ from the reference program's by a relative error of at most 0.023.
Values may be sent and summed in bfloat16 or wider, within the bound.
A program may use at most 128 MiB of HBM per device.

```python
import math
import jax
import jax.numpy as jnp
import numpy as np
from jax import lax

D = 4096
LATENT_WIDTH = 512
ROPE = 64
FIRST_HEADS = 8
WIDE_HEAD_SIZE = 128
SECOND_HEADS = 8
NARROW_HEAD_SIZE = 64
SHARED_FF = 512
EXPERT_FF = 192
TOPK = 2
TOKEN_COUNT = 1024
ROWS = 64
EXPERTS = 16
CAP = 16
N_SP = 4
N_TP = 4


def query_values(key, columns):
    values = jnp.clip(2.5 * jax.random.normal(key, (TOKEN_COUNT, columns), jnp.float32), -15.0, 15.0)
    return values.astype(jnp.bfloat16)


def draw_wide_query(key, part):
    return query_values(jax.random.fold_in(key, 11), FIRST_HEADS * (WIDE_HEAD_SIZE + ROPE))


def draw_narrow_query(key, part):
    return query_values(jax.random.fold_in(key, 23), SECOND_HEADS * (NARROW_HEAD_SIZE + ROPE))


def levels(own_key, shape, cuts, low, largest):
    level = 1.0
    for dim, blocks in cuts:
        heights = jax.random.uniform(jax.random.fold_in(jax.random.fold_in(own_key, 6), dim), (blocks,), jnp.float32, low / len(cuts), largest / len(cuts))
        level = level * jnp.repeat(jnp.exp(heights), shape[dim] // blocks).reshape((-1,) + (1,) * (len(shape) - 1 - dim))
    return level


def deal_out(stream_key, own, number, rows, count, top, limit, skew):
    order = jax.random.permutation(stream_key, count)
    crowded, ordinary = portions_of(count, rows * top, limit, skew, True), portions_of(count, rows * top, limit, skew, False)
    places = jnp.arange(count)

    def named(lengths, turn):
        used = int((lengths > 0).sum())
        fixed = max(1, used // 4)
        passed = fixed + (places - fixed + turn * (used - fixed)) % max(1, count - fixed)
        return jnp.zeros((count,), jnp.int32).at[order[jnp.where(places < fixed, places, passed)]].set(jnp.asarray(lengths, jnp.int32))

    lengths = jnp.where(number % 4 == 0, named(crowded, number // 4), named(ordinary, number - number // 4 - 1))
    mixed = jax.random.permutation(jax.random.fold_in(own, 3), count)
    source_of, receiver = mixed[0:count // 2 * 2:2], mixed[1:count // 2 * 2:2]
    slack = jnp.minimum(lengths[source_of] - 1, limit - lengths[receiver]) // 2
    slack = jnp.where((source_of == order[0]) | (receiver == order[0]) | (lengths[receiver] == 0), 0, jnp.maximum(slack, 0))
    passed = jax.random.randint(jax.random.fold_in(own, 4), (count // 2,), 0, 1 << 20) % (slack + 1)
    lengths = lengths.at[source_of].add(-passed).at[receiver].add(passed)
    items = jnp.searchsorted(jnp.cumsum(lengths), jnp.arange(rows * top), side="right").astype(jnp.int32)
    grid = items.reshape(top, rows).T
    grid = grid[jax.random.permutation(jax.random.fold_in(own, 1), rows)]
    turn = jax.random.randint(jax.random.fold_in(own, 2), (rows, 1), 0, top)
    return jnp.take_along_axis(grid, (jnp.arange(top)[None, :] + turn) % top, axis=1)


def portions_of(number_of, total, reach, slope, full):
    weights = [(1 << 20) // math.isqrt(standing ** slope) + 1 for standing in range(1, number_of + 1)]
    largest = reach if full else min(reach, max(-(-total // number_of), total * weights[0] // sum(weights)))
    least = 1 if total - largest >= number_of - 1 else 0
    counts, surplus = [largest] + [least] * (number_of - 1), total - largest - least * (number_of - 1)
    while surplus > 0:
        free = [i for i in range(1, number_of) if counts[i] < largest] or [i for i in range(1, number_of) if counts[i] < reach]
        whole, budget = sum([weights[i] for i in free]), surplus
        for i in free:
            addition = min(reach - counts[i], max(1, budget * weights[i] // whole), surplus)
            counts[i] = counts[i] + addition
            surplus = surplus - addition
    return np.array(counts)


def centred(stream_key, extent, width, bound, shards=(), kind=jnp.bfloat16):
    level = levels(stream_key, extent, shards, -0.22, 0.18) if shards else 1.0
    drawn = jax.random.normal(stream_key, extent, jnp.float32) * width * level
    return jnp.minimum(jnp.maximum(drawn, -bound), bound).astype(kind)


def setup_inputs(seed: int = 0, part: int = 0) -> dict:
    key_list = jax.random.split(jax.random.key(seed), 22)
    part_splits = jax.random.split(jax.random.fold_in(key_list[21], part), 22)
    latent = centred(part_splits[0], (TOKEN_COUNT, LATENT_WIDTH), 1.0, 6.0, ((0, 4),))
    rope_key = centred(part_splits[1], (TOKEN_COUNT, ROPE), 1.0, 6.0, ((0, 4),))
    wide_query = draw_wide_query(jax.random.fold_in(jax.random.fold_in(key_list[21], part), 71), part)
    narrow_query = draw_narrow_query(jax.random.fold_in(jax.random.fold_in(key_list[21], part), 71), part)
    wide_key_weight = centred(key_list[4], (LATENT_WIDTH, FIRST_HEADS * WIDE_HEAD_SIZE), LATENT_WIDTH ** -0.5, 0.25, ((1, 4),))
    wide_value_weight = centred(key_list[5], (LATENT_WIDTH, FIRST_HEADS * WIDE_HEAD_SIZE), LATENT_WIDTH ** -0.5, 0.25, ((1, 4),))
    narrow_key_weight = centred(key_list[6], (LATENT_WIDTH, SECOND_HEADS * NARROW_HEAD_SIZE), LATENT_WIDTH ** -0.5, 0.25, ((1, 4),))
    narrow_value_weight = centred(key_list[7], (LATENT_WIDTH, SECOND_HEADS * NARROW_HEAD_SIZE), LATENT_WIDTH ** -0.5, 0.25, ((1, 4),))
    latent_norm_scale = jnp.clip(1.0 + 0.18 * jax.random.normal(key_list[8], (LATENT_WIDTH,), jnp.float32), 0.1, 1.9)
    out_wide = centred(key_list[9], (FIRST_HEADS * WIDE_HEAD_SIZE, D), ((FIRST_HEADS * WIDE_HEAD_SIZE + SECOND_HEADS * NARROW_HEAD_SIZE) // 8) ** -0.5, 0.4375, ((0, 4),))
    out_narrow = centred(key_list[10], (SECOND_HEADS * NARROW_HEAD_SIZE, D), ((FIRST_HEADS * WIDE_HEAD_SIZE + SECOND_HEADS * NARROW_HEAD_SIZE) // 8) ** -0.5, 0.4375, ((0, 4),))
    residual = centred(part_splits[11], (TOKEN_COUNT, D), 1.0, 6.0, ((0, 16),))
    ffn_gain = jnp.clip(1.0 + 0.18 * jax.random.normal(key_list[12], (D,), jnp.float32), 0.1, 1.9)
    shared_gate = centred(key_list[13], (D, SHARED_FF), D ** -0.5, 0.09375, ((1, 4),))
    shared_up = centred(key_list[14], (D, SHARED_FF), D ** -0.5, 0.09375, ((1, 4),))
    shared_down = centred(key_list[15], (SHARED_FF, D), SHARED_FF ** -0.5, 0.25, ((0, 4),))
    expert_gate = centred(key_list[16], (EXPERTS, D, EXPERT_FF), D ** -0.5, 0.09375, ((0, 16),))
    expert_up = centred(key_list[17], (EXPERTS, D, EXPERT_FF), D ** -0.5, 0.09375, ((0, 16),))
    expert_down = centred(key_list[18], (EXPERTS, EXPERT_FF, D), EXPERT_FF ** -0.5, 0.4375, ((0, 16),))
    routes_keys = jax.random.split(jax.random.fold_in(part_splits[19], 1), TOKEN_COUNT // ROWS)
    routes_turns = jax.random.permutation(jax.random.fold_in(part_splits[19], 3), TOKEN_COUNT // ROWS)
    routes = jax.vmap(lambda own, number: deal_out(jax.random.fold_in(part_splits[19], 2), own, number, ROWS, EXPERTS, TOPK, CAP, 1))(routes_keys, routes_turns).reshape((TOKEN_COUNT, TOPK))
    route_weights = jnp.clip(0.25 + 1.25 * jax.random.uniform(part_splits[20], (TOKEN_COUNT, TOPK), jnp.float32) ** levels(part_splits[20], (TOKEN_COUNT, TOPK), ((0, 16),), -0.2, 0.2), 0.25, 1.5)
    return {"latent": latent, "rope_key": rope_key, "wide_query": wide_query, "narrow_query": narrow_query, "wide_key_weight": wide_key_weight, "wide_value_weight": wide_value_weight, "narrow_key_weight": narrow_key_weight, "narrow_value_weight": narrow_value_weight, "latent_norm_scale": latent_norm_scale, "out_wide": out_wide, "out_narrow": out_narrow, "residual": residual, "ffn_gain": ffn_gain, "shared_gate": shared_gate, "shared_up": shared_up, "shared_down": shared_down, "expert_gate": expert_gate, "expert_up": expert_up, "expert_down": expert_down, "routes": routes, "route_weights": route_weights}


EPS = 1e-06
ROPE_BASE = 10000.0
NEG_FILL = -1e+30

def rounded(values):
    return lax.optimization_barrier(values.astype(jnp.bfloat16)).astype(jnp.float32)

def rotate(values, positions):
    half_size = values.shape[-1] // 2
    inverse = ROPE_BASE ** (-jnp.arange(half_size, dtype=jnp.float32) * 2.0 / values.shape[-1])
    angles = positions.astype(jnp.float32)[:, None] * inverse[None, :]
    shaped = (angles.shape[0],) + (1,) * (values.ndim - 2) + (half_size,)
    cosine_table = jnp.cos(angles).reshape(shaped)
    sine_table = jnp.sin(angles).reshape(shaped)
    first_half = values[..., :half_size]
    second_half = values[..., half_size:]
    return jnp.concatenate([first_half * cosine_table - second_half * sine_table, second_half * cosine_table + first_half * sine_table], axis=-1)

def rms_scale(values, gain):
    return values * lax.rsqrt(lax.optimization_barrier(jnp.mean(values * values, axis=-1, keepdims=True)) + EPS) * gain

def update(state, query_plain, query_turned, keys, turned_rows, values, visible, factor):
    running_max, running_sum, weighted = state
    scores = jnp.einsum('qhd,khd->hqk', query_plain.astype(jnp.float32), keys.astype(jnp.float32))
    scores = scores + jnp.einsum('qhr,kr->hqk', query_turned.astype(jnp.float32), turned_rows.astype(jnp.float32))
    scores = jnp.where(visible[None], scores * factor, NEG_FILL)
    new_max = jnp.maximum(running_max, lax.optimization_barrier(jnp.max(scores, axis=2)))
    probs = jnp.where(visible[None], jnp.exp(scores - new_max[:, :, None]), 0.0)
    fading = jnp.exp(running_max - new_max)
    running_sum = running_sum * fading + lax.optimization_barrier(jnp.sum(probs, axis=2))
    weighted = weighted * fading[:, :, None] + jnp.einsum('hqk,khd->hqd', rounded(probs), values.astype(jnp.float32))
    return (new_max, running_sum, weighted)

def attend_group(query_plain, query_turned, keys, values, turned_keys, factor):
    tokens_all, heads, value_size = values.shape
    block = math.gcd(tokens_all, 512)
    blocks_all = tokens_all // block

    def per_query(block_index):
        query_start = block_index * block
        plain_rows = lax.dynamic_slice_in_dim(query_plain, query_start, block, 0)
        turned_rows_q = lax.dynamic_slice_in_dim(query_turned, query_start, block, 0)
        query_pos = query_start + jnp.arange(block, dtype=jnp.int32)

        def per_key(key_index, state):
            key_start = key_index * block
            key_pos = key_start + jnp.arange(block, dtype=jnp.int32)
            visible = key_pos[None, :] <= query_pos[:, None]
            return update(state, plain_rows, turned_rows_q, lax.dynamic_slice_in_dim(keys, key_start, block, 0), lax.dynamic_slice_in_dim(turned_keys, key_start, block, 0), lax.dynamic_slice_in_dim(values, key_start, block, 0), visible, factor)
        initial = (jnp.full((heads, block), NEG_FILL, jnp.float32), jnp.zeros((heads, block), jnp.float32), jnp.zeros((heads, block, value_size), jnp.float32))
        final = lax.fori_loop(0, block_index + 1, per_key, initial)
        normal_sampler = final[2] / final[1][:, :, None]
        return normal_sampler.astype(jnp.bfloat16).transpose(1, 0, 2).reshape(block, heads * value_size)
    outputs = lax.map(per_query, jnp.arange(blocks_all, dtype=jnp.int32))
    return outputs.reshape(tokens_all, heads * value_size)

def reference(latent, rope_key, wide_query, narrow_query, wide_key_weight, wide_value_weight, narrow_key_weight, narrow_value_weight, latent_norm_scale, out_wide, out_narrow, residual, ffn_gain, shared_gate, shared_up, shared_down, expert_gate, expert_up, expert_down, routes, route_weights):
    positions = jnp.arange(TOKEN_COUNT, dtype=jnp.int32)
    normed_latent = rms_scale(latent.astype(jnp.float32), latent_norm_scale).astype(jnp.bfloat16)
    turned_key = rotate(rope_key.astype(jnp.float32), positions).astype(jnp.bfloat16)
    wide_heads_q = wide_query.reshape(TOKEN_COUNT, FIRST_HEADS, WIDE_HEAD_SIZE + ROPE)
    wide_plain = wide_heads_q[..., :WIDE_HEAD_SIZE]
    wide_turned = rotate(wide_heads_q[..., WIDE_HEAD_SIZE:].astype(jnp.float32), positions).astype(jnp.bfloat16)
    narrow_heads_q = narrow_query.reshape(TOKEN_COUNT, SECOND_HEADS, NARROW_HEAD_SIZE + ROPE)
    narrow_plain = narrow_heads_q[..., :NARROW_HEAD_SIZE]
    narrow_turned = rotate(narrow_heads_q[..., NARROW_HEAD_SIZE:].astype(jnp.float32), positions).astype(jnp.bfloat16)
    wide_keys = jnp.dot(normed_latent, wide_key_weight, preferred_element_type=jnp.float32).astype(jnp.bfloat16).reshape(TOKEN_COUNT, FIRST_HEADS, WIDE_HEAD_SIZE)
    wide_values = jnp.dot(normed_latent, wide_value_weight, preferred_element_type=jnp.float32).astype(jnp.bfloat16).reshape(TOKEN_COUNT, FIRST_HEADS, WIDE_HEAD_SIZE)
    narrow_keys = jnp.dot(normed_latent, narrow_key_weight, preferred_element_type=jnp.float32).astype(jnp.bfloat16).reshape(TOKEN_COUNT, SECOND_HEADS, NARROW_HEAD_SIZE)
    narrow_values = jnp.dot(normed_latent, narrow_value_weight, preferred_element_type=jnp.float32).astype(jnp.bfloat16).reshape(TOKEN_COUNT, SECOND_HEADS, NARROW_HEAD_SIZE)
    wide_mix = attend_group(wide_plain, wide_turned, wide_keys, wide_values, turned_key, (WIDE_HEAD_SIZE + ROPE) ** (-0.5))
    narrow_mix = attend_group(narrow_plain, narrow_turned, narrow_keys, narrow_values, turned_key, (NARROW_HEAD_SIZE + ROPE) ** (-0.5))
    wide_share = FIRST_HEADS * WIDE_HEAD_SIZE // N_TP
    narrow_share = SECOND_HEADS * NARROW_HEAD_SIZE // N_TP
    projected = jnp.zeros((TOKEN_COUNT, D), jnp.float32)
    for member in range(N_TP):
        partial_value = jnp.dot(wide_mix[:, member * wide_share:(member + 1) * wide_share], out_wide[member * wide_share:(member + 1) * wide_share], preferred_element_type=jnp.float32)
        partial_value = partial_value + jnp.dot(narrow_mix[:, member * narrow_share:(member + 1) * narrow_share], out_narrow[member * narrow_share:(member + 1) * narrow_share], preferred_element_type=jnp.float32)
        projected = projected + rounded(partial_value)
    stream = (residual.astype(jnp.float32) + projected).astype(jnp.bfloat16)
    normed = rms_scale(stream.astype(jnp.float32), ffn_gain).astype(jnp.bfloat16)
    shared_share = SHARED_FF // N_TP
    shared = jnp.zeros((TOKEN_COUNT, D), jnp.float32)
    for member in range(N_TP):
        lower = member * shared_share
        upper = lower + shared_share
        gate_part = jnp.dot(normed, shared_gate[:, lower:upper], preferred_element_type=jnp.float32)
        up_part = jnp.dot(normed, shared_up[:, lower:upper], preferred_element_type=jnp.float32)
        active = (jax.nn.silu(gate_part) * up_part).astype(jnp.bfloat16)
        shared = shared + rounded(jnp.dot(active, shared_down[lower:upper], preferred_element_type=jnp.float32))
    devices_all = N_SP * N_TP
    flat_routes = routes.reshape(devices_all, ROWS * TOPK)
    choose = (flat_routes[:, :, None] == jnp.arange(EXPERTS, dtype=jnp.int32)[None, None, :]).astype(jnp.int32)
    earlier = jnp.cumsum(choose, axis=1) - choose
    slots = lax.optimization_barrier(jnp.sum(earlier * choose, axis=2)).astype(jnp.int32)
    device_ids = jnp.broadcast_to(jnp.arange(devices_all, dtype=jnp.int32)[:, None], flat_routes.shape)
    token_of = (device_ids * ROWS + jnp.arange(ROWS * TOPK, dtype=jnp.int32)[None, :] // TOPK).astype(jnp.int32)
    table = jnp.zeros((EXPERTS, devices_all, CAP), jnp.int32).at[flat_routes, device_ids, slots].set(token_of)

    def run_expert(member):
        rows_in = normed[table[member].reshape(-1)]
        gate_part = jnp.dot(rows_in, expert_gate[member], preferred_element_type=jnp.float32)
        up_part = jnp.dot(rows_in, expert_up[member], preferred_element_type=jnp.float32)
        active = (jax.nn.silu(gate_part) * up_part).astype(jnp.bfloat16)
        return jnp.dot(active, expert_down[member], preferred_element_type=jnp.float32).astype(jnp.bfloat16)
    results = lax.map(run_expert, jnp.arange(EXPERTS, dtype=jnp.int32))
    picked = results[flat_routes, device_ids * CAP + slots]
    routed = lax.optimization_barrier(jnp.sum(picked.reshape(TOKEN_COUNT, TOPK, D).astype(jnp.float32) * route_weights[:, :, None], axis=1))
    return (stream.astype(jnp.float32) + shared + routed).astype(jnp.bfloat16)
```

```python
import jax
import jax.numpy as jnp
from jax import lax
from jax.experimental import pallas as pl
from jax.experimental.pallas import tpu as pltpu
from jax.sharding import PartitionSpec as P

ROPE = 64
WIDE_HEAD_SIZE = 128
NARROW_HEAD_SIZE = 64


MESH = pl.DeviceIdType.MESH
VMEM = pl.BlockSpec(memory_space=pltpu.VMEM)


def flip(index, bits):
    mask = 1
    while mask <= bits:
        if bits & mask:
            index = index + mask - 2 * mask * ((index // mask) % 2)
        mask *= 2
    return index


def masks_of(count):
    return [1 << k for k in range(count.bit_length() - 1)]


def low_bit(number):
    return number & -number


def greet(partners):
    barrier = pltpu.get_barrier_semaphore()
    for partner in partners:
        pl.semaphore_signal(barrier, inc=1, device_id=partner, device_id_type=MESH)
    pl.semaphore_wait(barrier, len(partners))


def doubling_order(count):
    return sorted(range(count), key=lambda d: (bin(d).count("1"), -d))


def remote(src, dst, send_sem, recv_sem, target):
    return pltpu.make_async_remote_copy(
        src_ref=src,
        dst_ref=dst,
        send_sem=send_sem,
        recv_sem=recv_sem,
        device_id=target,
        device_id_type=MESH,
    )


def spread_kernel(n_sp, n_tp, x_ref, *refs):
    if len(refs) > 6:
        meta_ref, out_ref, all_ref = refs[:3]
        z_send, z_recv, t_send, t_recv, own_sem = refs[3:8]
        toll = Exchange(None, None, *refs[8:11])
    else:
        out_ref, z_send, z_recv, t_send, t_recv, own_sem = refs
        toll = None
    sp, tp = lax.axis_index("sp"), lax.axis_index("tp")
    tok = x_ref.shape[0]
    part = tok // n_tp
    targets = [{"sp": lax.rem(sp + r, n_sp)} for r in range(1, n_sp)]
    if toll is None:
        greet(targets + [{"tp": flip(tp, m)} for m in masks_of(n_tp)])
    else:
        toll.greet()

    def rows(block, member):
        return pl.ds(pl.multiple_of(block * tok + member * part, part), part)

    own = pltpu.make_async_copy(
        x_ref, out_ref.at[pl.ds(pl.multiple_of(sp * tok, tok), tok)], own_sem
    )
    sends = []
    for r in range(1, n_sp):
        copy = remote(
            x_ref.at[pl.ds(pl.multiple_of(tp * part, part), part)],
            out_ref.at[rows(sp, tp)],
            z_send.at[r],
            z_recv.at[r],
            targets[r - 1],
        )
        copy.start()
        sends.append(copy)
    own.start()
    if toll is not None:
        tolls = [toll.toll(k, meta_ref, all_ref) for k in range(1, toll.count)]
        for copy in tolls:
            copy.start()
        all_ref[toll.me] = meta_ref[...]

    def piece(r, d):
        return out_ref.at[rows(lax.rem(sp + n_sp - r, n_sp), flip(tp, d))]

    for d in doubling_order(n_tp):
        for r in range(1, n_sp):
            block = piece(r, d)
            if d == 0:
                sends[r - 1].wait_recv()
            else:
                remote(
                    block, block, t_send.at[r, d], t_recv.at[r, d], {"tp": flip(tp, low_bit(d))}
                ).wait_recv()
            for mask in reversed(masks_of(low_bit(d) if d else n_tp)):
                copy = remote(
                    block,
                    block,
                    t_send.at[r, d + mask],
                    t_recv.at[r, d + mask],
                    {"tp": flip(tp, mask)},
                )
                copy.start()
                sends.append(copy)
    for copy in sends:
        copy.wait_send()
    own.wait()
    if toll is not None:
        for copy in tolls:
            copy.wait()


def spread(x, n_sp, n_tp, meta=None):
    tok, width = x.shape
    out_shape = [jax.ShapeDtypeStruct((n_sp * tok, width), x.dtype)]
    operands, extra = (x,), []
    if meta is not None:
        operands += (meta,)
        out_shape.append(jax.ShapeDtypeStruct((n_sp * n_tp,) + meta.shape, meta.dtype))
        extra = exchange_semaphores(n_sp * n_tp)
    return pl.pallas_call(
        lambda *refs: spread_kernel(n_sp, n_tp, *refs),
        out_shape=out_shape,
        in_specs=[VMEM] * len(operands),
        out_specs=[VMEM] * len(out_shape),
        scratch_shapes=[
            pltpu.SemaphoreType.DMA((n_sp,)),
            pltpu.SemaphoreType.DMA((n_sp,)),
            pltpu.SemaphoreType.DMA((n_sp, n_tp)),
            pltpu.SemaphoreType.DMA((n_sp, n_tp)),
            pltpu.SemaphoreType.DMA,
        ]
        + extra,
        compiler_params=pltpu.CompilerParams(collective_id=0, has_side_effects=True),
        cost_estimate=pl.CostEstimate(flops=0, bytes_accessed=30_000_000, transcendentals=0),
    )(*operands)


def gather_kernel(
    n_tp, pieces, x_ref, blocks_ref, out_ref, moved_ref, send, recv, own_sem, *semaphores
):
    exchange = Exchange(blocks_ref, moved_ref, *semaphores)
    tp = lax.axis_index("tp")
    rows, width = x_ref.shape
    part = width // pieces
    exchange.greet()

    def block(d, c):
        start = pl.multiple_of(flip(tp, d) * rows, rows)
        return out_ref.at[pl.ds(start, rows), pl.ds(c * part, part)]

    own = pltpu.make_async_copy(
        x_ref, out_ref.at[pl.ds(pl.multiple_of(tp * rows, rows), rows)], own_sem
    )
    sends = []
    for d in doubling_order(n_tp):
        for c in range(pieces):
            source = x_ref.at[:, pl.ds(c * part, part)] if d == 0 else block(d, c)
            if d:
                remote(
                    source, source, send.at[d, c], recv.at[d, c], {"tp": flip(tp, low_bit(d))}
                ).wait_recv()
            for mask in reversed(masks_of(low_bit(d) if d else n_tp)):
                copy = remote(
                    source,
                    block(d, c),
                    send.at[d + mask, c],
                    recv.at[d + mask, c],
                    {"tp": flip(tp, mask)},
                )
                copy.start()
                sends.append(copy)
        if d == 0:
            exchange.start()
            own.start()
    for copy in sends:
        copy.wait_send()
    own.wait()
    exchange.finish()


def gather_rows(x, blocks, n_tp, pieces=2):
    rows, width = x.shape
    return pl.pallas_call(
        lambda *refs: gather_kernel(n_tp, pieces, *refs),
        out_shape=[
            jax.ShapeDtypeStruct((n_tp * rows, width), x.dtype),
            jax.ShapeDtypeStruct(blocks.shape, blocks.dtype),
        ],
        in_specs=[VMEM] * 2,
        out_specs=[VMEM] * 2,
        scratch_shapes=[
            pltpu.SemaphoreType.DMA((n_tp, pieces)),
            pltpu.SemaphoreType.DMA((n_tp, pieces)),
            pltpu.SemaphoreType.DMA,
        ]
        + exchange_semaphores(blocks.shape[0]),
        compiler_params=pltpu.CompilerParams(collective_id=1, has_side_effects=True),
        cost_estimate=pl.CostEstimate(flops=0, bytes_accessed=40_000_000, transcendentals=0),
    )(x, blocks)


def scatter_kernel(n_tp, pieces, pairs, moving, *refs):
    lefts, rights = refs[:pairs], refs[pairs : 2 * pairs]
    refs = refs[2 * pairs :]
    exchange = None
    if moving:
        blocks_ref, out_ref, moved_ref, sent, got, send, recv = refs[:7]
        exchange = Exchange(blocks_ref, moved_ref, *refs[7:])
    else:
        out_ref, sent, got, send, recv = refs
    tp = lax.axis_index("tp")
    rows, width = out_ref.shape
    part = width // pieces
    if moving:
        exchange.greet()
        exchange.start()
    else:
        greet([{"tp": flip(tp, m)} for m in masks_of(n_tp)])
    copies = {}

    def product(d, c):
        start = pl.multiple_of(flip(tp, d) * rows, rows)
        total = None
        for left, right in zip(lefts, rights):
            term = jnp.dot(
                left[pl.ds(start, rows), :],
                right[:, pl.ds(c * part, part)],
                preferred_element_type=jnp.float32,
            )
            total = term if total is None else total + term
        return total

    def summed(d, c, below):
        total = product(d, c)
        if below > 1:
            total = total.astype(jnp.bfloat16).astype(jnp.float32)
        for mask in masks_of(below):
            copies[d + mask, c].wait_recv()
            total = total + got[d + mask, :, pl.ds(c * part, part)].astype(jnp.float32)
        return total

    def pass_on(mask, c):
        for d in range(mask, n_tp, 2 * mask):
            sent[d, :, pl.ds(c * part, part)] = summed(d, c, mask).astype(jnp.bfloat16)
            copies[d, c] = remote(
                sent.at[d, :, pl.ds(c * part, part)],
                got.at[d, :, pl.ds(c * part, part)],
                send.at[d, c],
                recv.at[d, c],
                {"tp": flip(tp, mask)},
            )
            copies[d, c].start()

    masks = masks_of(n_tp)
    for step in range(pieces + len(masks) - 1):
        for stage, mask in enumerate(masks):
            if 0 <= step - stage < pieces:
                pass_on(mask, step - stage)
    for c in range(pieces):
        out_ref[:, pl.ds(c * part, part)] = summed(0, c, n_tp)
    for copy in copies.values():
        copy.wait_send()
    if moving:
        exchange.finish()


def dot_scatter(lefts, rights, n_tp, collective, blocks=None, pieces=4):
    rows, width = lefts[0].shape[0] // n_tp, rights[0].shape[1]
    pairs, moving = len(lefts), blocks is not None
    shapes = [jax.ShapeDtypeStruct((rows, width), jnp.float32)]
    operands = (*lefts, *rights)
    scratch = [
        pltpu.VMEM((n_tp, rows, width), jnp.bfloat16),
        pltpu.VMEM((n_tp, rows, width), jnp.bfloat16),
        pltpu.SemaphoreType.DMA((n_tp, pieces)),
        pltpu.SemaphoreType.DMA((n_tp, pieces)),
    ]
    if moving:
        shapes.append(jax.ShapeDtypeStruct(blocks.shape, blocks.dtype))
        operands += (blocks,)
        scratch += exchange_semaphores(blocks.shape[0])
    return pl.pallas_call(
        lambda *refs: scatter_kernel(n_tp, pieces, pairs, moving, *refs),
        out_shape=shapes,
        in_specs=[VMEM] * len(operands),
        out_specs=[VMEM] * len(shapes),
        scratch_shapes=scratch,
        compiler_params=pltpu.CompilerParams(collective_id=collective, has_side_effects=True),
        cost_estimate=pl.CostEstimate(flops=0, bytes_accessed=40_000_000, transcendentals=0),
    )(*operands)


def moe_kernel(chunks, cap, *refs):
    x_ref, stream_ref, meta_ref = refs[:3]
    hbm = refs[3:9]
    out_ref = refs[9]
    blk, plane, gbuf, crow, obuf, ret, chs, chin, fin, sent, got = refs[10:21]
    local = refs[21:27]
    sg, su, sd, eg, eu, ed = local
    smat, som, wcol, hg, hu, act, shg, shu, sact, facc = refs[27:37]
    wsem, psend, precv, csend, crecv, gsend, grecv, osend, orecv = refs[37:46]
    dsend, drecv, frecv, rsend, rrecv = refs[46:51]
    z, tp = lax.axis_index("sp"), lax.axis_index("tp")
    n_sp, n_tp = lax.axis_size("sp"), lax.axis_size("tp")
    rows, width = x_ref.shape
    part = width // chunks
    slots = n_tp * cap
    way = 1 - 2 * (z // 2)
    f32, bf16 = jnp.float32, jnp.bfloat16

    def cols(q):
        return pl.ds(pl.multiple_of(q * part, part), part)

    def peer(d):
        return {"tp": flip(tp, d)}

    def dot(a, b):
        return jnp.dot(a, b, preferred_element_type=f32)

    def dot_nt(a, b):
        return lax.dot_general(a, b, (((1,), (1,)), ((), ())), preferred_element_type=f32)

    def dot_tn(a, b):
        return lax.dot_general(a, b, (((0,), (0,)), ((), ())), preferred_element_type=f32)

    barrier = pltpu.get_barrier_semaphore()

    def signal(target):
        pl.semaphore_signal(barrier, inc=1, device_id=target, device_id_type=MESH)

    for d in range(1, n_tp):
        signal(peer(d))

    @pl.when(z > 0)
    def _():
        signal({"sp": z - 1})

    @pl.when(z < n_sp - 1)
    def _():
        signal({"sp": z + 1})

    loads = [
        pltpu.make_async_copy(a, b, wsem.at[k]) for k, (a, b) in enumerate(zip(hbm, local))
    ]
    for k in (3, 4, 0, 1, 5, 2):
        loads[k].start()
    pl.semaphore_wait(
        barrier, n_tp - 1 + (z + n_sp - 1) // n_sp + (2 * n_sp - 2 - z) // n_sp
    )

    def block_out(p, q, k, target, source=None):
        source = blk.at[p, :, cols(q)] if source is None else source
        return remote(source, blk.at[p, :, cols(q)], csend.at[k, q], crecv.at[p, q], target)

    def own_out(q, step):
        return block_out(z, q, (1 - step) // 2, {"sp": z + step}, x_ref.at[:, cols(q)])

    def gather_out(m, q):
        return remote(
            x_ref.at[:, cols(q)],
            plane.at[pl.ds(m * rows, rows), cols(q)],
            psend.at[m, q],
            precv.at[m, q],
            peer(m),
        )

    def gather_on(q):
        return remote(
            plane.at[pl.ds(2 * rows, rows), cols(q)],
            plane.at[pl.ds(3 * rows, rows), cols(q)],
            psend.at[3, q],
            precv.at[3, q],
            peer(1),
        )

    for q in range(chunks):

        @pl.when(z < n_sp - 1)
        def _():
            own_out(q, 1).start()

        @pl.when(z > 0)
        def _():
            own_out(q, -1).start()

        if q == 0:
            gather_out(2, 0).start()
            gather_out(1, 0).start()

    plane[:rows, :] = x_ref[...]
    hg[...] = jnp.zeros_like(hg)
    hu[...] = jnp.zeros_like(hu)
    shg[...] = jnp.zeros_like(shg)
    shu[...] = jnp.zeros_like(shu)
    som[...] = jnp.zeros_like(som)
    lanes = meta_ref.shape[2]
    iota = lax.broadcasted_iota(jnp.int32, (cap, lanes), 0)
    for step in range(n_sp):
        p = lax.rem(z + step, n_sp)
        for d in range(n_tp):
            if step:
                info = meta_ref[p * n_tp + tp]
                slot = ((z * n_tp + flip(tp, d)) * cap + iota).astype(f32)
                hit = (info[0:1, :] == slot) | (info[1:2, :] == slot)
                smat[p, d * cap : (d + 1) * cap, :] = hit.astype(f32)[:, :rows].astype(bf16)
            info = meta_ref[p * n_tp + flip(tp, d)]
            slot = ((z * n_tp + tp) * cap + iota).astype(f32)
            first, second = info[0:1, :] == slot, info[1:2, :] == slot
            weight = jnp.where(first, info[2:3, :], 0.0) + jnp.where(second, info[3:4, :], 0.0)
            wcol[p, d * cap : (d + 1) * cap, :] = jnp.sum(weight, axis=1, keepdims=True)
            if not step:
                hit = (first | second).astype(f32)[:, :rows].astype(bf16)
                som[d * cap : (d + 1) * cap, d * rows : (d + 1) * rows] = hit

    def piece(p, d, q):
        return p, pl.ds(d * cap, cap), cols(q)

    def spread_out(p, d, q):
        at = piece(p, d, q)
        return remote(gbuf.at[at], crow.at[at], gsend.at[p, d, q], grecv.at[p, d, q], peer(d))

    def c_unit(p, q, k=None, target=None):
        block_out(p, q, 0, peer(1)).wait_recv()
        if k is not None:
            block_out(p, q, k, target).start()
        picked = dot(smat[p], blk[p, :, cols(q)]).astype(bf16)
        gbuf[p, :, cols(q)] = picked
        crow[p, :cap, cols(q)] = picked[:cap]
        for d in (2, 3, 1):
            spread_out(p, d, q).start()

    def hidden(p, q):
        taken = crow[p, :, cols(q)]
        hg[p] += dot_nt(taken, eg[:, cols(q)])
        hu[p] += dot_nt(taken, eu[:, cols(q)])

    def h_unit(p, q):
        for d in (1, 2, 3):
            spread_out(p, d, q).wait_recv()
        hidden(p, q)

    def activate(p):
        gate = hg[p]
        act[p] = (gate / (1.0 + jnp.exp(-gate)) * hu[p]).astype(bf16)

    def own_unit(q):
        @pl.when(q < chunks - 1)
        def _():
            gather_out(2, q + 1).start()
            gather_out(1, q + 1).start()

        gather_out(2, q).wait_recv()
        gather_on(q).start()
        gather_out(1, q).wait_recv()
        gather_on(q).wait_recv()
        full = plane[:, cols(q)]
        crow[z, :, cols(q)] = dot(som[...], full).astype(bf16)
        deep = pl.ds(pl.multiple_of(q * part, part), part)
        shg[...] += dot(full, sg[deep, :])
        shu[...] += dot(full, su[deep, :])
        hidden(z, q)

    def own_activate():
        activate(z)
        gate = shg[...]
        sact[...] = (gate / (1.0 + jnp.exp(-gate)) * shu[...]).astype(bf16)

    def outcome(p, q):
        made = dot(act[p], ed[:, cols(q)]).astype(bf16).astype(f32)
        return (made * wcol[p]).astype(bf16)

    def back_out(p, d, q):
        at = piece(p, d, q)
        return remote(obuf.at[at], ret.at[at], osend.at[p, d, q], orecv.at[p, d, q], peer(d))

    def o_unit(p, q):
        made = outcome(p, q)
        obuf[p, :, cols(q)] = made
        ret[p, :cap, cols(q)] = made[:cap]
        for d in (2, 3, 1):
            back_out(p, d, q).start()

    def chain_out(p, q, last, step):
        into, sem = chin.at[p, :, cols(q)], drecv.at[p, q]
        if last:
            side = (1 - step) // 2
            into, sem = fin.at[side, :, cols(q)], frecv.at[side, q]
        return remote(chs.at[p, :, cols(q)], into, dsend.at[p, q], sem, {"sp": z + step})

    def d_unit(p, q, incoming, last, step):
        for d in (1, 2, 3):
            back_out(p, d, q).wait_recv()
        total = dot_tn(smat[p], ret[p, :, cols(q)])
        if incoming:
            chain_out(p, q, False, step).wait_recv()
            total = total + chin[p, :, cols(q)].astype(f32)
        chs[p, :, cols(q)] = total.astype(bf16)
        chain_out(p, q, last, step).start()

    def product(d, q):
        return dot(sact[d * rows : (d + 1) * rows, :], sd[:, cols(q)]) + dot_tn(
            som[:, d * rows : (d + 1) * rows], obuf[z, :, cols(q)]
        )

    def fold(d, q, mask):
        return remote(
            sent.at[d, :, cols(q)],
            got.at[d, :, cols(q)],
            rsend.at[d, q],
            rrecv.at[d, q],
            peer(mask),
        )

    def rs1(q):
        obuf[z, :, cols(q)] = outcome(z, q)
        for d in (3, 1):
            sent[d, :, cols(q)] = product(d, q).astype(bf16)
            fold(d, q, 1).start()

    def rs2(q):
        total = product(2, q)
        fold(3, q, 1).wait_recv()
        sent[2, :, cols(q)] = (total + got[3, :, cols(q)].astype(f32)).astype(bf16)
        fold(2, q, 2).start()

    def base(q):
        total = product(0, q) + stream_ref[:, cols(q)].astype(f32)
        fold(1, q, 1).wait_recv()
        total = total + got[1, :, cols(q)].astype(f32)
        fold(2, q, 2).wait_recv()
        facc[:, cols(q)] = total + got[2, :, cols(q)].astype(f32)

    def arrive(side, q):
        remote(
            fin.at[side, :, cols(q)],
            fin.at[side, :, cols(q)],
            dsend.at[0, q],
            frecv.at[side, q],
            peer(1),
        ).wait_recv()
        return fin[side, :, cols(q)].astype(f32)

    def staged(first, later=None):
        def one(q, carry):
            @pl.when(q < chunks)
            def _():
                first(q)

            if later is not None:

                @pl.when(q > 0)
                def _():
                    later(q - 1)

            return carry

        lax.fori_loop(0, chunks + (later is not None), one, 0)

    def run(*steps):
        def each(q):
            for step in steps:
                step(q)

        return each

    def sends_done(copies):
        def one(q, carry):
            for copy in copies(q):
                copy.wait_send()
            return carry

        lax.fori_loop(0, chunks, one, 0)

    for k in (3, 4, 0, 1, 5, 2):
        loads[k].wait()

    is_end = (z == 0) | (z == n_sp - 1)

    @pl.when(is_end)
    def _():
        p0, p1, p2 = z + way, z + 2 * way, z + 3 * way
        staged(run(own_unit, lambda q: c_unit(p0, q)), lambda q: h_unit(p0, q))
        activate(p0)
        own_activate()
        staged(
            run(lambda q: c_unit(p1, q), lambda q: o_unit(p0, q)),
            run(lambda q: h_unit(p1, q), lambda q: d_unit(p0, q, False, True, way)),
        )
        activate(p1)
        staged(
            run(lambda q: c_unit(p2, q), lambda q: o_unit(p1, q), rs1),
            run(lambda q: h_unit(p2, q), lambda q: d_unit(p1, q, False, False, way)),
        )
        activate(p2)
        staged(
            run(lambda q: o_unit(p2, q), rs2), lambda q: d_unit(p2, q, False, False, way)
        )
        staged(base)

        def last(q):
            out_ref[:, cols(q)] = (facc[:, cols(q)] + arrive((1 + way) // 2, q)).astype(bf16)

        staged(last)
        sends_done(
            lambda q: [own_out(q, way)]
            + [spread_out(p, d, q) for p in (p0, p1, p2) for d in (1, 2, 3)]
            + [back_out(p, d, q) for p in (p0, p1, p2) for d in (1, 2, 3)]
            + [chain_out(p, q, False, way) for p in (p0, p1, p2)]
        )

    @pl.when(jnp.logical_not(is_end))
    def _():
        s0, s1, s2 = z - way, z + way, z + 2 * way
        ahead, behind = {"sp": z + way}, {"sp": z - way}
        staged(
            run(
                lambda q: c_unit(s0, q, 2, ahead),
                lambda q: c_unit(s1, q, 3, behind),
                own_unit,
            ),
            run(lambda q: h_unit(s0, q), lambda q: h_unit(s1, q)),
        )
        activate(s0)
        activate(s1)
        own_activate()
        staged(
            run(lambda q: c_unit(s2, q, 4, behind), lambda q: o_unit(s1, q), rs1),
            run(lambda q: h_unit(s2, q), rs2),
        )
        activate(s2)
        staged(
            run(lambda q: o_unit(s2, q), lambda q: o_unit(s0, q)),
            run(lambda q: d_unit(s1, q, True, True, way), base),
        )
        staged(
            run(
                lambda q: d_unit(s2, q, True, False, way),
                lambda q: d_unit(s0, q, True, True, -way),
            )
        )

        def last(q):
            total = facc[:, cols(q)] + arrive(0, q) + arrive(1, q)
            out_ref[:, cols(q)] = total.astype(bf16)

        staged(last)
        sends_done(
            lambda q: [own_out(q, way), own_out(q, -way)]
            + [block_out(s0, q, 2, ahead), block_out(s1, q, 3, behind)]
            + [block_out(s2, q, 4, behind)]
            + [spread_out(p, d, q) for p in (s0, s1, s2) for d in (1, 2, 3)]
            + [back_out(p, d, q) for p in (s0, s1, s2) for d in (1, 2, 3)]
            + [chain_out(p, q, False, way) for p in (s0, s1, s2)]
        )

    sends_done(
        lambda q: [gather_out(2, q), gather_out(1, q), gather_on(q)]
        + [fold(3, q, 1), fold(1, q, 1), fold(2, q, 2)]
    )


def moe(normed, stream, meta, weights, n_sp, n_tp, cap, chunks=4):
    rows, width = normed.shape
    sg, su, sd, eg, eu, ed = weights
    slots = n_tp * cap
    hidden, share = eg.shape[0], sg.shape[1]
    bf16, f32 = jnp.bfloat16, jnp.float32
    any_space = pl.BlockSpec(memory_space=pl.ANY)
    per_plane = pltpu.VMEM((n_sp, slots, width), bf16)
    blocks = pltpu.VMEM((n_sp, rows, width), bf16)
    folds = pltpu.VMEM((n_tp, rows, width), bf16)

    def sems(*shape):
        return pltpu.SemaphoreType.DMA(shape)

    scratch = [blocks, pltpu.VMEM((n_tp * rows, width), bf16)]
    scratch += [per_plane] * 4 + [blocks] * 2
    scratch += [pltpu.VMEM((2, rows, width), bf16), folds, folds]
    scratch += [pltpu.VMEM(w.shape, w.dtype) for w in weights]
    scratch += [
        pltpu.VMEM((n_sp, slots, rows), bf16),
        pltpu.VMEM((slots, n_tp * rows), bf16),
        pltpu.VMEM((n_sp, slots, 1), f32),
        pltpu.VMEM((n_sp, slots, hidden), f32),
        pltpu.VMEM((n_sp, slots, hidden), f32),
        pltpu.VMEM((n_sp, slots, hidden), bf16),
        pltpu.VMEM((n_tp * rows, share), f32),
        pltpu.VMEM((n_tp * rows, share), f32),
        pltpu.VMEM((n_tp * rows, share), bf16),
        pltpu.VMEM((rows, width), f32),
    ]
    scratch += [sems(6), sems(n_tp, chunks), sems(n_tp, chunks)]
    scratch += [sems(5, chunks), sems(n_sp, chunks)]
    scratch += [sems(n_sp, n_tp, chunks)] * 4
    scratch += [sems(n_sp, chunks), sems(n_sp, chunks), sems(2, chunks)]
    scratch += [sems(n_tp, chunks), sems(n_tp, chunks)]
    return pl.pallas_call(
        lambda *refs: moe_kernel(chunks, cap, *refs),
        out_shape=jax.ShapeDtypeStruct((rows, width), bf16),
        in_specs=[VMEM] * 3 + [any_space] * 6,
        out_specs=VMEM,
        scratch_shapes=scratch,
        compiler_params=pltpu.CompilerParams(
            collective_id=4, has_side_effects=True, vmem_limit_bytes=60 << 20
        ),
    )(normed, stream, meta, *weights)


EPS = 1e-06
ROPE_BASE = 10000.0
NEG_FILL = -1e30


def attend_kernel(sizes, packed, cosine, sine, *refs):
    groups = len(sizes)
    queries, key_ws, value_ws = refs[:groups], refs[groups : 2 * groups], refs[2 * groups : 3 * groups]
    outs = refs[3 * groups : 4 * groups]
    scratch = refs[4 * groups :]
    sp = lax.axis_index("sp")
    tok = cosine.shape[0]
    latent_width = key_ws[0].shape[0]
    lanes = packed.shape[1] - latent_width
    half = ROPE // 2

    def grid(shape):
        return lax.broadcasted_iota(jnp.int32, shape, 0), lax.broadcasted_iota(jnp.int32, shape, 1)

    for g, size in enumerate(sizes):
        plain, turned, peak, total, mixed = scratch[5 * g : 5 * g + 5]
        query = queries[g][...]
        width = query.shape[1]
        for h in range(plain.shape[0]):
            i, j = grid((width, key_ws[g].shape[1]))
            select = (i == j + h * ROPE) & (j >= h * size) & (j < (h + 1) * size)
            plain[h] = jnp.dot(
                query, select.astype(jnp.bfloat16), preferred_element_type=jnp.float32
            ).astype(jnp.bfloat16)
            i, j = grid((width, lanes))
            base = h * (size + ROPE) + size
            same = ((i == j + base) & (j < ROPE)).astype(jnp.float32)
            upper = ((i == j + base + half) & (j < half)).astype(jnp.float32)
            lower = ((i == j + base - half) & (j >= half) & (j < ROPE)).astype(jnp.float32)
            straight = jnp.dot(
                query, same.astype(jnp.bfloat16), preferred_element_type=jnp.float32
            )
            crossed = jnp.dot(
                query, (lower - upper).astype(jnp.bfloat16), preferred_element_type=jnp.float32
            )
            turned[h] = (straight * cosine[...] + crossed * sine[...]).astype(jnp.bfloat16)
        peak[...] = jnp.full_like(peak, NEG_FILL)
        total[...] = jnp.zeros_like(total)
        mixed[...] = jnp.zeros_like(mixed)

    def one_block(index, carry):
        start = pl.ds(pl.multiple_of(index * tok, tok), tok)
        latent = packed[start, :latent_width]
        turned_rows = packed[start, latent_width:]
        i, j = grid((tok, tok))
        visible = index * tok + j <= sp * tok + i
        across = (((1,), (1,)), ((), ()))
        for g, size in enumerate(sizes):
            plain, turned, peak, total, mixed = scratch[5 * g : 5 * g + 5]
            factor = (size + ROPE) ** (-0.5)
            keys = jnp.dot(latent, key_ws[g][...], preferred_element_type=jnp.float32)
            keys = keys.astype(jnp.bfloat16)
            values = jnp.dot(latent, value_ws[g][...], preferred_element_type=jnp.float32)
            values = values.astype(jnp.bfloat16)
            for h in range(plain.shape[0]):
                scores = lax.dot_general(
                    plain[h], keys, across, preferred_element_type=jnp.float32
                ) + lax.dot_general(
                    turned[h], turned_rows, across, preferred_element_type=jnp.float32
                )
                scores = jnp.where(visible, scores * factor, NEG_FILL)
                old = peak[h]
                new = jnp.maximum(old, jnp.max(scores, axis=1, keepdims=True))
                probs = jnp.where(visible, jnp.exp(scores - new), 0.0)
                fading = jnp.exp(old - new)
                peak[h] = new
                total[h] = total[h] * fading + jnp.sum(probs, axis=1, keepdims=True)
                mixed[h] = mixed[h] * fading + jnp.dot(
                    probs.astype(jnp.bfloat16), values, preferred_element_type=jnp.float32
                )
        return carry

    lax.fori_loop(0, sp + 1, one_block, 0)
    for g, size in enumerate(sizes):
        plain, turned, peak, total, mixed = scratch[5 * g : 5 * g + 5]
        i, j = grid(outs[g].shape)
        result = jnp.zeros(outs[g].shape, jnp.float32)
        for h in range(plain.shape[0]):
            own = (j >= h * size) & (j < (h + 1) * size)
            result = jnp.where(own, mixed[h] / total[h], result)
        outs[g][...] = result.astype(jnp.bfloat16)


def attend(packed, cosine, sine, queries, key_ws, value_ws, sizes):
    tok, lanes = cosine.shape
    scratch = []
    for g, size in enumerate(sizes):
        heads = value_ws[g].shape[1] // size
        scratch += [
            pltpu.VMEM((heads, tok, key_ws[g].shape[1]), jnp.bfloat16),
            pltpu.VMEM((heads, tok, lanes), jnp.bfloat16),
            pltpu.VMEM((heads, tok, 1), jnp.float32),
            pltpu.VMEM((heads, tok, 1), jnp.float32),
            pltpu.VMEM((heads, tok, value_ws[g].shape[1]), jnp.float32),
        ]
    return pl.pallas_call(
        lambda *refs: attend_kernel(sizes, *refs),
        out_shape=[jax.ShapeDtypeStruct((tok, w.shape[1]), jnp.bfloat16) for w in value_ws],
        in_specs=[VMEM] * (3 + 3 * len(sizes)),
        out_specs=[VMEM] * len(sizes),
        scratch_shapes=scratch,
    )(packed, cosine, sine, *queries, *key_ws, *value_ws)


class Exchange:
    def __init__(self, source, dest, send, recv, own_sem):
        self.refs = source, dest, send, recv
        self.sp, self.tp = lax.axis_index("sp"), lax.axis_index("tp")
        self.n_sp, self.n_tp = lax.axis_size("sp"), lax.axis_size("tp")
        self.count = self.n_sp * self.n_tp
        self.me = self.sp * self.n_tp + self.tp
        if source is not None:
            self.own = pltpu.make_async_copy(source.at[self.me], dest.at[self.me], own_sem)

    def toll(self, k, source, dest):
        sp, tp = self.target(k)
        send, recv = self.refs[2:]
        return remote(source, dest.at[self.me], send.at[k], recv.at[k], {"sp": sp, "tp": tp})

    def target(self, k):
        return (
            lax.rem(self.sp + k // self.n_tp, self.n_sp),
            lax.rem(self.tp + lax.rem(k, self.n_tp), self.n_tp),
        )

    def greet(self):
        barrier = pltpu.get_barrier_semaphore()

        def one(k, carry):
            sp, tp = self.target(k)
            pl.semaphore_signal(
                barrier, inc=1, device_id={"sp": sp, "tp": tp}, device_id_type=MESH
            )
            return carry

        lax.fori_loop(1, self.count, one, 0)
        pl.semaphore_wait(barrier, self.count - 1)

    def copy(self, k):
        source, dest, send, recv = self.refs
        sp, tp = self.target(k)
        return remote(
            source.at[sp * self.n_tp + tp],
            dest.at[self.me],
            send.at[k],
            recv.at[k],
            {"sp": sp, "tp": tp},
        )

    def start(self):
        def one(k, carry):
            self.copy(self.count - k).start()
            return carry

        lax.fori_loop(1, self.count, one, 0)
        self.own.start()

    def finish(self):
        def one(k, carry):
            self.copy(k).wait()
            return carry

        lax.fori_loop(1, self.count, one, 0)
        self.own.wait()


def exchange_semaphores(count):
    return [
        pltpu.SemaphoreType.DMA((count,)),
        pltpu.SemaphoreType.DMA((count,)),
        pltpu.SemaphoreType.DMA,
    ]


def rms_scale(values, gain):
    return values * lax.rsqrt(jnp.mean(values * values, axis=-1, keepdims=True) + EPS) * gain


def body(
    latent,
    rope_key,
    wide_query,
    narrow_query,
    wide_key_weight,
    wide_value_weight,
    narrow_key_weight,
    narrow_value_weight,
    latent_norm_scale,
    out_wide,
    out_narrow,
    residual,
    ffn_gain,
    shared_gate,
    shared_up,
    shared_down,
    expert_gate,
    expert_up,
    expert_down,
    routes,
    route_weights,
):
    tok_dev = latent.shape[0]
    seq_index = lax.axis_index("sp")
    own_pos = seq_index * tok_dev + jnp.arange(tok_dev, dtype=jnp.int32)
    n_sp, n_tp = lax.axis_size("sp"), lax.axis_size("tp")
    normed_latent = rms_scale(latent.astype(jnp.float32), latent_norm_scale).astype(jnp.bfloat16)
    half = ROPE // 2
    lane = jnp.arange(ROPE + -ROPE % 128, dtype=jnp.int32)
    inverse = ROPE_BASE ** (-(lane % half).astype(jnp.float32) * 2.0 / ROPE)
    angles = own_pos.astype(jnp.float32)[:, None] * inverse[None, :]
    cosine, sine = jnp.cos(angles), jnp.sin(angles)
    row = jnp.arange(ROPE, dtype=jnp.int32)[:, None]
    same = (row == lane[None, :]).astype(jnp.bfloat16)
    cross = (row == lane[None, :] - half).astype(jnp.bfloat16) * (lane < ROPE)[None, :] - (
        (row == lane[None, :] + half) & (lane < half)[None, :]
    ).astype(jnp.bfloat16)
    turned_key = (
        jnp.dot(rope_key, same, preferred_element_type=jnp.float32) * cosine
        + jnp.dot(rope_key, cross.astype(jnp.bfloat16), preferred_element_type=jnp.float32) * sine
    ).astype(jnp.bfloat16)
    rows_here, top_count = routes.shape
    local_experts = expert_gate.shape[0]
    experts_all = local_experts * lax.axis_size(("sp", "tp"))
    capacity = max(2, 2 * top_count * rows_here // experts_all)
    flat_routes = routes.reshape(-1)
    assigned = flat_routes.shape[0]
    choose = (flat_routes[:, None] == jnp.arange(experts_all, dtype=jnp.int32)[None, :]).astype(
        jnp.float32
    )
    lower_mask = (jnp.arange(assigned)[:, None] > jnp.arange(assigned)[None, :]).astype(jnp.float32)
    earlier = jnp.dot(lower_mask, choose, precision=lax.Precision.HIGHEST)
    slots = jnp.sum(earlier * choose, axis=1).astype(jnp.int32)
    target = flat_routes * capacity + slots
    by_choice = target.reshape(rows_here, top_count)
    planes = n_sp == 4 and n_tp == 4 and local_experts == 1 and capacity % 16 == 0
    fused = planes and top_count == 2 and rows_here <= 128
    rows_packed = jnp.concatenate([normed_latent, turned_key], axis=1)
    if fused:
        spare = (-rows_here) % 128
        facts = jnp.concatenate([by_choice.astype(jnp.float32).T, route_weights.T], axis=0)
        facts = jnp.pad(facts, ((0, 4), (0, spare)), constant_values=-1.0)
        packed, meta = spread(rows_packed, n_sp, n_tp, facts)
    else:
        (packed,) = spread(rows_packed, n_sp, n_tp)
    wide_mix, narrow_mix = attend(
        packed,
        cosine,
        sine,
        (wide_query, narrow_query),
        (wide_key_weight, narrow_key_weight),
        (wide_value_weight, narrow_value_weight),
        (WIDE_HEAD_SIZE, NARROW_HEAD_SIZE),
    )
    (projected,) = dot_scatter((wide_mix, narrow_mix), (out_wide, out_narrow), n_tp, 2)
    stream = (residual.astype(jnp.float32) + projected).astype(jnp.bfloat16)
    normed = rms_scale(stream.astype(jnp.float32), ffn_gain).astype(jnp.bfloat16)
    if fused:
        weights = (shared_gate, shared_up, shared_down)
        weights += (expert_gate[0].T, expert_up[0].T, expert_down[0])
        return moe(normed, stream, meta, weights, n_sp, n_tp, capacity)
    model_width = normed.shape[1]
    send_map = jnp.any(
        target.reshape(rows_here, top_count)[None, :, :]
        == jnp.arange(experts_all * capacity, dtype=jnp.int32)[:, None, None],
        axis=2,
    ).astype(jnp.bfloat16)
    outgoing = jnp.dot(send_map, normed, preferred_element_type=jnp.float32).astype(jnp.bfloat16)
    devices = n_sp * n_tp
    outgoing = outgoing.reshape(devices, local_experts * capacity, model_width)
    piece, incoming = gather_rows(normed, outgoing, n_tp)
    sources = devices
    incoming = incoming.reshape(experts_all, capacity, model_width)
    grouped = incoming.reshape(sources, local_experts, incoming.shape[1], model_width)
    gate_part = jnp.einsum(
        "sxcd,xdf->sxcf", grouped, expert_gate, preferred_element_type=jnp.float32
    )
    up_part = jnp.einsum("sxcd,xdf->sxcf", grouped, expert_up, preferred_element_type=jnp.float32)
    active = (jax.nn.silu(gate_part) * up_part).astype(jnp.bfloat16)
    finished = jnp.einsum(
        "sxcf,xfd->sxcd", active, expert_down, preferred_element_type=jnp.float32
    ).astype(jnp.bfloat16)
    gate_part = jnp.dot(piece, shared_gate, preferred_element_type=jnp.float32)
    up_part = jnp.dot(piece, shared_up, preferred_element_type=jnp.float32)
    active = (jax.nn.silu(gate_part) * up_part).astype(jnp.bfloat16)
    shared, returned = dot_scatter(
        (active,), (shared_down,), n_tp, 3, finished.reshape(outgoing.shape)
    )
    slot_rows = returned.reshape(experts_all * capacity, model_width)
    routed = jnp.zeros((rows_here, model_width), jnp.float32)
    for choice in range(top_count):
        hot = by_choice[:, choice : choice + 1] == jnp.arange(experts_all * capacity)[None, :]
        picked = jnp.dot(
            hot.astype(jnp.bfloat16), slot_rows, preferred_element_type=jnp.float32
        )
        routed = routed + picked * route_weights[:, choice : choice + 1]
    return (stream.astype(jnp.float32) + shared + routed).astype(jnp.bfloat16)


def solution(mesh):
    placed = (
        P(("grp", "sp"), None),
        P(("grp", "sp"), None),
        P(("grp", "sp"), "tp"),
        P(("grp", "sp"), "tp"),
        P(None, "tp"),
        P(None, "tp"),
        P(None, "tp"),
        P(None, "tp"),
        P(),
        P("tp", None),
        P("tp", None),
        P(("grp", "sp", "tp"), None),
        P(),
        P(None, "tp"),
        P(None, "tp"),
        P("tp", None),
        P(("sp", "tp"), None, None),
        P(("sp", "tp"), None, None),
        P(("sp", "tp"), None, None),
        P(("grp", "sp", "tp"), None),
        P(("grp", "sp", "tp"), None),
    )
    return jax.shard_map(
        body, mesh=mesh, in_specs=placed, out_specs=P(("grp", "sp", "tp"), None), check_vma=False
    )
```

```python
import jax
import jax.numpy as jnp
from jax import lax
from jax.experimental import pallas as pl
from jax.experimental.pallas import tpu as pltpu
from jax.sharding import PartitionSpec as P

ROPE = 64
WIDE_HEAD_SIZE = 128
NARROW_HEAD_SIZE = 64
EPS = 1e-06
ROPE_BASE = 10000.0
NEG_FILL = -1e30


MESH = pl.DeviceIdType.MESH
VMEM = pl.BlockSpec(memory_space=pltpu.VMEM)


def flip(index, bits):
    mask = 1
    while mask <= bits:
        if bits & mask:
            index = index + mask - 2 * mask * ((index // mask) % 2)
        mask *= 2
    return index


def masks_of(count):
    return [1 << k for k in range(count.bit_length() - 1)]


def low_bit(number):
    return number & -number


def greet(partners):
    barrier = pltpu.get_barrier_semaphore()
    for partner in partners:
        pl.semaphore_signal(barrier, inc=1, device_id=partner, device_id_type=MESH)
    pl.semaphore_wait(barrier, len(partners))


def doubling_order(count):
    return sorted(range(count), key=lambda d: (bin(d).count("1"), -d))


def remote(src, dst, send_sem, recv_sem, target):
    return pltpu.make_async_remote_copy(
        src_ref=src,
        dst_ref=dst,
        send_sem=send_sem,
        recv_sem=recv_sem,
        device_id=target,
        device_id_type=MESH,
    )


def spread_kernel(n_sp, n_tp, x_ref, out_ref, z_send, z_recv, t_send, t_recv, own_sem):
    sp, tp = lax.axis_index("sp"), lax.axis_index("tp")
    tok = x_ref.shape[0]
    part = tok // n_tp
    targets = [{"sp": lax.rem(sp + r, n_sp)} for r in range(1, n_sp)]
    greet(targets + [{"tp": flip(tp, m)} for m in masks_of(n_tp)])

    def rows(block, member):
        return pl.ds(pl.multiple_of(block * tok + member * part, part), part)

    own = pltpu.make_async_copy(
        x_ref, out_ref.at[pl.ds(pl.multiple_of(sp * tok, tok), tok)], own_sem
    )
    sends = []
    for r in range(1, n_sp):
        copy = remote(
            x_ref.at[pl.ds(pl.multiple_of(tp * part, part), part)],
            out_ref.at[rows(sp, tp)],
            z_send.at[r],
            z_recv.at[r],
            targets[r - 1],
        )
        copy.start()
        sends.append(copy)
    own.start()

    def piece(r, d):
        return out_ref.at[rows(lax.rem(sp + n_sp - r, n_sp), flip(tp, d))]

    for d in doubling_order(n_tp):
        for r in range(1, n_sp):
            block = piece(r, d)
            if d == 0:
                sends[r - 1].wait_recv()
            else:
                remote(
                    block, block, t_send.at[r, d], t_recv.at[r, d], {"tp": flip(tp, low_bit(d))}
                ).wait_recv()
            for mask in reversed(masks_of(low_bit(d) if d else n_tp)):
                copy = remote(
                    block,
                    block,
                    t_send.at[r, d + mask],
                    t_recv.at[r, d + mask],
                    {"tp": flip(tp, mask)},
                )
                copy.start()
                sends.append(copy)
    for copy in sends:
        copy.wait_send()
    own.wait()


def spread(x, n_sp, n_tp):
    tok, width = x.shape
    return pl.pallas_call(
        lambda *refs: spread_kernel(n_sp, n_tp, *refs),
        out_shape=jax.ShapeDtypeStruct((n_sp * tok, width), x.dtype),
        in_specs=[VMEM],
        out_specs=VMEM,
        scratch_shapes=[
            pltpu.SemaphoreType.DMA((n_sp,)),
            pltpu.SemaphoreType.DMA((n_sp,)),
            pltpu.SemaphoreType.DMA((n_sp, n_tp)),
            pltpu.SemaphoreType.DMA((n_sp, n_tp)),
            pltpu.SemaphoreType.DMA,
        ],
        compiler_params=pltpu.CompilerParams(collective_id=0, has_side_effects=True),
        cost_estimate=pl.CostEstimate(flops=0, bytes_accessed=30_000_000, transcendentals=0),
    )(x)


def gather_kernel(
    n_tp, pieces, x_ref, blocks_ref, out_ref, moved_ref, send, recv, own_sem, *semaphores
):
    exchange = Exchange(blocks_ref, moved_ref, *semaphores)
    tp = lax.axis_index("tp")
    rows, width = x_ref.shape
    part = width // pieces
    exchange.greet()

    def block(d, c):
        start = pl.multiple_of(flip(tp, d) * rows, rows)
        return out_ref.at[pl.ds(start, rows), pl.ds(c * part, part)]

    own = pltpu.make_async_copy(
        x_ref, out_ref.at[pl.ds(pl.multiple_of(tp * rows, rows), rows)], own_sem
    )
    sends = []
    for d in doubling_order(n_tp):
        for c in range(pieces):
            source = x_ref.at[:, pl.ds(c * part, part)] if d == 0 else block(d, c)
            if d:
                remote(
                    source, source, send.at[d, c], recv.at[d, c], {"tp": flip(tp, low_bit(d))}
                ).wait_recv()
            for mask in reversed(masks_of(low_bit(d) if d else n_tp)):
                copy = remote(
                    source,
                    block(d, c),
                    send.at[d + mask, c],
                    recv.at[d + mask, c],
                    {"tp": flip(tp, mask)},
                )
                copy.start()
                sends.append(copy)
        if d == 0:
            exchange.start()
            own.start()
    for copy in sends:
        copy.wait_send()
    own.wait()
    exchange.finish()


def gather_rows(x, blocks, n_tp, pieces=2):
    rows, width = x.shape
    return pl.pallas_call(
        lambda *refs: gather_kernel(n_tp, pieces, *refs),
        out_shape=[
            jax.ShapeDtypeStruct((n_tp * rows, width), x.dtype),
            jax.ShapeDtypeStruct(blocks.shape, blocks.dtype),
        ],
        in_specs=[VMEM] * 2,
        out_specs=[VMEM] * 2,
        scratch_shapes=[
            pltpu.SemaphoreType.DMA((n_tp, pieces)),
            pltpu.SemaphoreType.DMA((n_tp, pieces)),
            pltpu.SemaphoreType.DMA,
        ]
        + exchange_semaphores(blocks.shape[0]),
        compiler_params=pltpu.CompilerParams(collective_id=1, has_side_effects=True),
        cost_estimate=pl.CostEstimate(flops=0, bytes_accessed=40_000_000, transcendentals=0),
    )(x, blocks)


def scatter_kernel(n_tp, pieces, pairs, moving, *refs):
    lefts, rights = refs[:pairs], refs[pairs : 2 * pairs]
    refs = refs[2 * pairs :]
    exchange = None
    if moving:
        blocks_ref, out_ref, moved_ref, sent, got, send, recv = refs[:7]
        exchange = Exchange(blocks_ref, moved_ref, *refs[7:])
    else:
        out_ref, sent, got, send, recv = refs
    tp = lax.axis_index("tp")
    rows, width = out_ref.shape
    part = width // pieces
    if moving:
        exchange.greet()
        exchange.start()
    else:
        greet([{"tp": flip(tp, m)} for m in masks_of(n_tp)])
    copies = {}

    def product(d, c):
        start = pl.multiple_of(flip(tp, d) * rows, rows)
        total = None
        for left, right in zip(lefts, rights):
            term = jnp.dot(
                left[pl.ds(start, rows), :],
                right[:, pl.ds(c * part, part)],
                preferred_element_type=jnp.float32,
            )
            total = term if total is None else total + term
        return total

    def summed(d, c, below):
        total = product(d, c)
        if below > 1:
            total = total.astype(jnp.bfloat16).astype(jnp.float32)
        for mask in masks_of(below):
            copies[d + mask, c].wait_recv()
            total = total + got[d + mask, :, pl.ds(c * part, part)].astype(jnp.float32)
        return total

    def pass_on(mask, c):
        for d in range(mask, n_tp, 2 * mask):
            sent[d, :, pl.ds(c * part, part)] = summed(d, c, mask).astype(jnp.bfloat16)
            copies[d, c] = remote(
                sent.at[d, :, pl.ds(c * part, part)],
                got.at[d, :, pl.ds(c * part, part)],
                send.at[d, c],
                recv.at[d, c],
                {"tp": flip(tp, mask)},
            )
            copies[d, c].start()

    masks = masks_of(n_tp)
    for step in range(pieces + len(masks) - 1):
        for stage, mask in enumerate(masks):
            if 0 <= step - stage < pieces:
                pass_on(mask, step - stage)
    for c in range(pieces):
        out_ref[:, pl.ds(c * part, part)] = summed(0, c, n_tp)
    for copy in copies.values():
        copy.wait_send()
    if moving:
        exchange.finish()


def dot_scatter(lefts, rights, n_tp, collective, blocks=None, pieces=4):
    rows, width = lefts[0].shape[0] // n_tp, rights[0].shape[1]
    pairs, moving = len(lefts), blocks is not None
    shapes = [jax.ShapeDtypeStruct((rows, width), jnp.float32)]
    operands = (*lefts, *rights)
    scratch = [
        pltpu.VMEM((n_tp, rows, width), jnp.bfloat16),
        pltpu.VMEM((n_tp, rows, width), jnp.bfloat16),
        pltpu.SemaphoreType.DMA((n_tp, pieces)),
        pltpu.SemaphoreType.DMA((n_tp, pieces)),
    ]
    if moving:
        shapes.append(jax.ShapeDtypeStruct(blocks.shape, blocks.dtype))
        operands += (blocks,)
        scratch += exchange_semaphores(blocks.shape[0])
    return pl.pallas_call(
        lambda *refs: scatter_kernel(n_tp, pieces, pairs, moving, *refs),
        out_shape=shapes,
        in_specs=[VMEM] * len(operands),
        out_specs=[VMEM] * len(shapes),
        scratch_shapes=scratch,
        compiler_params=pltpu.CompilerParams(collective_id=collective, has_side_effects=True),
        cost_estimate=pl.CostEstimate(flops=0, bytes_accessed=40_000_000, transcendentals=0),
    )(*operands)


def grid(shape):
    return lax.broadcasted_iota(jnp.int32, shape, 0), lax.broadcasted_iota(jnp.int32, shape, 1)


def attend_start(sizes, cosine, sine, queries, widths, scratch):
    half = ROPE // 2
    lanes = cosine.shape[1]
    for g, size in enumerate(sizes):
        plain, turned, peak, total, mixed = scratch[5 * g : 5 * g + 5]
        query = queries[g][...]
        width = query.shape[1]
        for h in range(plain.shape[0]):
            i, j = grid((width, widths[g]))
            select = (i == j + h * ROPE) & (j >= h * size) & (j < (h + 1) * size)
            plain[h] = jnp.dot(
                query, select.astype(jnp.bfloat16), preferred_element_type=jnp.float32
            ).astype(jnp.bfloat16)
            i, j = grid((width, lanes))
            base = h * (size + ROPE) + size
            same = ((i == j + base) & (j < ROPE)).astype(jnp.float32)
            upper = ((i == j + base + half) & (j < half)).astype(jnp.float32)
            lower = ((i == j + base - half) & (j >= half) & (j < ROPE)).astype(jnp.float32)
            straight = jnp.dot(
                query, same.astype(jnp.bfloat16), preferred_element_type=jnp.float32
            )
            crossed = jnp.dot(
                query, (lower - upper).astype(jnp.bfloat16), preferred_element_type=jnp.float32
            )
            turned[h] = (straight * cosine[...] + crossed * sine[...]).astype(jnp.bfloat16)
        peak[...] = jnp.full_like(peak, NEG_FILL)
        total[...] = jnp.zeros_like(total)
        mixed[...] = jnp.zeros_like(mixed)


def attend_block(sizes, packed, index, sp, key_ws, value_ws, scratch):
    latent_width = key_ws[0].shape[0]
    tok = scratch[0].shape[1]
    start = pl.ds(pl.multiple_of(index * tok, tok), tok)
    latent = packed[start, :latent_width]
    turned_rows = packed[start, latent_width:]
    i, j = grid((tok, tok))
    visible = index * tok + j <= sp * tok + i
    across = (((1,), (1,)), ((), ()))
    for g, size in enumerate(sizes):
        plain, turned, peak, total, mixed = scratch[5 * g : 5 * g + 5]
        factor = (size + ROPE) ** (-0.5)
        keys = jnp.dot(latent, key_ws[g][...], preferred_element_type=jnp.float32)
        keys = keys.astype(jnp.bfloat16)
        values = jnp.dot(latent, value_ws[g][...], preferred_element_type=jnp.float32)
        values = values.astype(jnp.bfloat16)
        for h in range(plain.shape[0]):
            scores = lax.dot_general(
                plain[h], keys, across, preferred_element_type=jnp.float32
            ) + lax.dot_general(
                turned[h], turned_rows, across, preferred_element_type=jnp.float32
            )
            scores = jnp.where(visible, scores * factor, NEG_FILL)
            old = peak[h]
            new = jnp.maximum(old, jnp.max(scores, axis=1, keepdims=True))
            probs = jnp.where(visible, jnp.exp(scores - new), 0.0)
            fading = jnp.exp(old - new)
            peak[h] = new
            total[h] = total[h] * fading + jnp.sum(probs, axis=1, keepdims=True)
            mixed[h] = mixed[h] * fading + jnp.dot(
                probs.astype(jnp.bfloat16), values, preferred_element_type=jnp.float32
            )


def attend_end(sizes, outs, scratch):
    for g, size in enumerate(sizes):
        plain, turned, peak, total, mixed = scratch[5 * g : 5 * g + 5]
        i, j = grid(outs[g].shape)
        result = jnp.zeros(outs[g].shape, jnp.float32)
        for h in range(plain.shape[0]):
            own = (j >= h * size) & (j < (h + 1) * size)
            result = jnp.where(own, mixed[h] / total[h], result)
        outs[g][...] = result.astype(jnp.bfloat16)


def attend_kernel(sizes, packed, cosine, sine, *refs):
    groups = len(sizes)
    queries, key_ws, value_ws = refs[:groups], refs[groups : 2 * groups], refs[2 * groups : 3 * groups]
    outs = refs[3 * groups : 4 * groups]
    scratch = refs[4 * groups :]
    sp = lax.axis_index("sp")
    attend_start(sizes, cosine, sine, queries, [w.shape[1] for w in key_ws], scratch)

    def one_block(index, carry):
        attend_block(sizes, packed, index, sp, key_ws, value_ws, scratch)
        return carry

    lax.fori_loop(0, sp + 1, one_block, 0)
    attend_end(sizes, outs, scratch)


def attend_scratch(tok, lanes, key_ws, value_ws, sizes):
    scratch = []
    for g, size in enumerate(sizes):
        heads = value_ws[g].shape[1] // size
        scratch += [
            pltpu.VMEM((heads, tok, key_ws[g].shape[1]), jnp.bfloat16),
            pltpu.VMEM((heads, tok, lanes), jnp.bfloat16),
            pltpu.VMEM((heads, tok, 1), jnp.float32),
            pltpu.VMEM((heads, tok, 1), jnp.float32),
            pltpu.VMEM((heads, tok, value_ws[g].shape[1]), jnp.float32),
        ]
    return scratch


def attend(packed, cosine, sine, queries, key_ws, value_ws, sizes):
    tok, lanes = cosine.shape
    scratch = attend_scratch(tok, lanes, key_ws, value_ws, sizes)
    return pl.pallas_call(
        lambda *refs: attend_kernel(sizes, *refs),
        out_shape=[jax.ShapeDtypeStruct((tok, w.shape[1]), jnp.bfloat16) for w in value_ws],
        in_specs=[VMEM] * (3 + 3 * len(sizes)),
        out_specs=[VMEM] * len(sizes),
        scratch_shapes=scratch,
    )(packed, cosine, sine, *queries, *key_ws, *value_ws)


class Exchange:
    def __init__(self, source, dest, send, recv, own_sem):
        self.refs = source, dest, send, recv
        self.sp, self.tp = lax.axis_index("sp"), lax.axis_index("tp")
        self.n_sp, self.n_tp = lax.axis_size("sp"), lax.axis_size("tp")
        self.count = self.n_sp * self.n_tp
        self.me = self.sp * self.n_tp + self.tp
        self.own = pltpu.make_async_copy(source.at[self.me], dest.at[self.me], own_sem)

    def target(self, k):
        return (
            lax.rem(self.sp + k // self.n_tp, self.n_sp),
            lax.rem(self.tp + lax.rem(k, self.n_tp), self.n_tp),
        )

    def greet(self):
        barrier = pltpu.get_barrier_semaphore()

        def one(k, carry):
            sp, tp = self.target(k)
            pl.semaphore_signal(
                barrier, inc=1, device_id={"sp": sp, "tp": tp}, device_id_type=MESH
            )
            return carry

        lax.fori_loop(1, self.count, one, 0)
        pl.semaphore_wait(barrier, self.count - 1)

    def copy(self, k):
        source, dest, send, recv = self.refs
        sp, tp = self.target(k)
        return remote(
            source.at[sp * self.n_tp + tp],
            dest.at[self.me],
            send.at[k],
            recv.at[k],
            {"sp": sp, "tp": tp},
        )

    def start(self):
        def one(k, carry):
            self.copy(self.count - k).start()
            return carry

        lax.fori_loop(1, self.count, one, 0)
        self.own.start()

    def finish(self):
        def one(k, carry):
            self.copy(k).wait()
            return carry

        lax.fori_loop(1, self.count, one, 0)
        self.own.wait()


def exchange_semaphores(count):
    return [
        pltpu.SemaphoreType.DMA((count,)),
        pltpu.SemaphoreType.DMA((count,)),
        pltpu.SemaphoreType.DMA,
    ]


def layer_kernel(chunks, cap, sizes, *refs):
    groups = len(sizes)
    x_ref, cosine, sine = refs[:3]
    queries, key_ws, value_ws = (refs[3 + k * groups : 3 + (k + 1) * groups] for k in range(3))
    refs = refs[3 + 3 * groups :]
    facts_ref, gain_ref, residual_ref = refs[:3]
    hbm, out_ref, refs = refs[3:11], refs[11], refs[12:]
    heads_scratch, refs = refs[: 5 * groups], refs[5 * groups :]
    packed, mixes, refs = refs[0], refs[1 : 1 + groups], refs[1 + groups :]
    meta, factors, factor_out, stream, x_scr = refs[:5]
    blk, plane, gbuf, crow, chs, chin, fin = refs[5:12]
    bsent, bgot, sent, got = refs[12:16]
    local = refs[16:24]
    ow, on, sg, su, sd, eg, eu, ed = local
    smat, som, wcol, hg, hu, aout, ain, spread_act, shg, shu, sact, facc, squares = refs[24:37]
    refs = refs[37:]
    wsem, lsend, lrecv, psend_l, precv_l, msend, mrecv, fsend, frecv_f = refs[:9]
    psend, precv, csend, crecv, gsend, grecv, asend, arecv = refs[9:17]
    dsend, drecv, frecv, rsend, rrecv, bsend, brecv, esend, erecv, ysend = refs[17:27]
    z, tp = lax.axis_index("sp"), lax.axis_index("tp")
    group = lax.axis_index("grp")
    n_sp, n_tp = lax.axis_size("sp"), lax.axis_size("tp")
    count = n_sp * n_tp
    me = z * n_tp + tp
    rows, width = stream.shape
    tok = x_ref.shape[0]
    part = width // chunks
    hidden_width = eg.shape[0]
    way = 1 - 2 * (z // 2)
    f32, bf16 = jnp.float32, jnp.bfloat16

    def cols(q):
        return pl.ds(pl.multiple_of(q * part, part), part)

    def peer(d):
        return {"tp": flip(tp, d)}

    def dot(a, b):
        return jnp.dot(a, b, preferred_element_type=f32)

    def dot_nt(a, b):
        return lax.dot_general(a, b, (((1,), (1,)), ((), ())), preferred_element_type=f32)

    def dot_tn(a, b):
        return lax.dot_general(a, b, (((0,), (0,)), ((), ())), preferred_element_type=f32)

    def other(k):
        return {
            "sp": lax.rem(z + k // n_tp, n_sp),
            "tp": lax.rem(tp + lax.rem(k, n_tp), n_tp),
        }

    def others(step):
        def one(k, carry):
            step(k)
            return carry

        lax.fori_loop(1, count, one, 0)

    barrier = pltpu.get_barrier_semaphore()
    others(
        lambda k: pl.semaphore_signal(barrier, inc=1, device_id=other(k), device_id_type=MESH)
    )
    pl.semaphore_signal(barrier, inc=1, device_id={"grp": 1 - group}, device_id_type=MESH)
    landing = [ed.at[0] if k == 7 else local[k] for k in range(8)]
    loads = [pltpu.make_async_copy(a, b, wsem.at[k]) for k, (a, b) in enumerate(zip(hbm, landing))]
    for k in (7, 0, 1, 5, 6, 2, 3, 4):
        loads[k].start()
    pl.semaphore_wait(barrier, count)

    half = tok // 2
    mine = lax.rem(tp, 2) * half

    def latent_rows(block, start):
        return pl.ds(pl.multiple_of(block * tok + start, half), half)

    def latent_out(block, source=None):
        into = packed.at[latent_rows(block, mine)]
        source = into if source is None else source
        return remote(source, into, lsend.at[block], lrecv.at[block], {"sp": z + 1})

    def latent_over(block):
        at = packed.at[latent_rows(block, mine)]
        return remote(at, at, psend_l.at[block], precv_l.at[block], peer(1))

    def latent_here(block):
        at = packed.at[latent_rows(block, half - mine)]
        remote(at, at, psend_l.at[block], precv_l.at[block], peer(1)).wait_recv()

    @pl.when(z < n_sp - 1)
    def _():
        latent_out(z, x_ref.at[pl.ds(pl.multiple_of(mine, half), half)]).start()

    def fact_out(k):
        return remote(facts_ref, meta.at[me], msend.at[k], mrecv.at[me], other(k))

    def factor_send(k):
        return remote(factor_out, factors.at[me], fsend.at[k], frecv_f.at[me], other(k))

    others(lambda k: fact_out(k).start())
    meta[me] = facts_ref[...]

    def down_out(m, q):
        return remote(
            ed.at[0, :, cols(q)],
            ed.at[m, :, cols(q)],
            esend.at[m, q],
            erecv.at[m, q],
            peer(m),
        )

    def down_on(q):
        return remote(
            ed.at[2, :, cols(q)],
            ed.at[3, :, cols(q)],
            esend.at[3, q],
            erecv.at[3, q],
            peer(1),
        )

    def down_across(q):
        at = ed.at[2, :, cols(q)]
        return remote(at, at, ysend.at[q], erecv.at[2, q], {"grp": 1 - group})

    loads[7].wait()
    for i in range(chunks // 2):
        down_out(2, 2 * i + group).start()
    for q in range(chunks):
        down_out(1, q).start()

    packed[pl.ds(pl.multiple_of(z * tok, tok), tok)] = x_ref[...]
    attend_start(sizes, cosine, sine, queries, [w.shape[1] for w in key_ws], heads_scratch)
    attend_block(sizes, packed, z, z, key_ws, value_ws, heads_scratch)

    def earlier(k, carry):
        block = z - k
        remote(
            packed.at[latent_rows(block, mine)],
            packed.at[latent_rows(block, mine)],
            lsend.at[block],
            lrecv.at[block],
            peer(1),
        ).wait_recv()

        @pl.when(z < n_sp - 1)
        def _():
            latent_out(block).start()

        latent_over(block).start()
        latent_here(block)
        attend_block(sizes, packed, block, z, key_ws, value_ws, heads_scratch)
        return carry

    lax.fori_loop(1, z + 1, earlier, 0)
    attend_end(sizes, mixes, heads_scratch)

    def block_out(p, q, k, target, source=None):
        source = blk.at[p, :, cols(q)] if source is None else source
        return remote(source, blk.at[p, :, cols(q)], csend.at[k, q], crecv.at[p, q], target)

    def own_out(q, step):
        return block_out(z, q, (1 - step) // 2, {"sp": z + step}, x_scr.at[:, cols(q)])

    def gather_out(m, q):
        return remote(
            x_scr.at[:, cols(q)],
            plane.at[pl.ds(m * rows, rows), cols(q)],
            psend.at[m, q],
            precv.at[m, q],
            peer(m),
        )

    def gather_on(q):
        return remote(
            plane.at[pl.ds(2 * rows, rows), cols(q)],
            plane.at[pl.ds(3 * rows, rows), cols(q)],
            psend.at[3, q],
            precv.at[3, q],
            peer(1),
        )

    def fold_in(sends, gets, send_sem, recv_sem):
        def fold(d, q, mask):
            return remote(
                sends.at[d, :, cols(q)],
                gets.at[d, :, cols(q)],
                send_sem.at[d, q],
                recv_sem.at[d, q],
                peer(mask),
            )

        return fold

    first_fold = fold_in(bsent, bgot, bsend, brecv)
    fold = fold_in(sent, got, rsend, rrecv)

    def projected(d, q):
        start = pl.ds(pl.multiple_of(flip(tp, d) * rows, rows), rows)
        return dot(mixes[0][start, :], ow[:, cols(q)]) + dot(mixes[1][start, :], on[:, cols(q)])

    def b1(q):
        for d in (3, 1):
            bsent[d, :, cols(q)] = projected(d, q).astype(bf16)
            first_fold(d, q, 1).start()

    def b2(q):
        total = projected(2, q)
        first_fold(3, q, 1).wait_recv()
        bsent[2, :, cols(q)] = (total + bgot[3, :, cols(q)].astype(f32)).astype(bf16)
        first_fold(2, q, 2).start()

    def b3(q):
        total = projected(0, q) + residual_ref[:, cols(q)].astype(f32)
        first_fold(1, q, 1).wait_recv()
        total = total + bgot[1, :, cols(q)].astype(f32)
        first_fold(2, q, 2).wait_recv()
        total = (total + bgot[2, :, cols(q)].astype(f32)).astype(bf16)
        stream[:, cols(q)] = total
        total = total.astype(f32)
        squares[...] += jnp.sum(total * total, axis=1, keepdims=True)
        scaled = (total * gain_ref[:, cols(q)]).astype(bf16)
        x_scr[:, cols(q)] = scaled

        @pl.when(z < n_sp - 1)
        def _():
            own_out(q, 1).start()

        @pl.when(z > 0)
        def _():
            own_out(q, -1).start()

        gather_out(2, q).start()
        gather_out(1, q).start()
        plane[:rows, cols(q)] = scaled

        @pl.when(q < chunks // 2)
        def _():
            down_out(2, 2 * q + group).wait_recv()
            down_across(2 * q + group).start()

    def staged(*stages):
        def one(q, carry):
            for lag, stage in enumerate(stages):

                @pl.when((q >= lag) & (q < chunks + lag))
                def _():
                    stage(q - lag)

            return carry

        lax.fori_loop(0, chunks + len(stages) - 1, one, 0)

    loads[0].wait()
    loads[1].wait()
    squares[...] = jnp.zeros_like(squares)
    staged(b1, b2, b3)
    factor = lax.rsqrt(squares[...] * (1.0 / width) + EPS)
    i, j = grid((rows, factor_out.shape[1]))
    factor = jnp.sum(jnp.where(i == j, factor, 0.0), axis=0, keepdims=True)
    factor_out[...] = jnp.broadcast_to(factor, factor_out.shape)
    others(lambda k: factor_send(k).start())
    factors[me] = factor_out[...]

    hg[...] = jnp.zeros_like(hg)
    hu[...] = jnp.zeros_like(hu)
    shg[...] = jnp.zeros_like(shg)
    shu[...] = jnp.zeros_like(shu)
    som[...] = jnp.zeros_like(som)
    lanes = meta.shape[2]
    iota = lax.broadcasted_iota(jnp.int32, (cap, lanes), 0)

    def fact_wait(k):
        source = lax.rem(z + k // n_tp, n_sp) * n_tp + lax.rem(tp + lax.rem(k, n_tp), n_tp)
        remote(facts_ref, meta.at[source], msend.at[k], mrecv.at[source], peer(1)).wait_recv()

    others(fact_wait)

    def held(p, d):
        info = meta[p * n_tp + flip(tp, d)]
        slot = ((z * n_tp + tp) * cap + iota).astype(f32)
        return info, info[0:1, :] == slot, info[1:2, :] == slot

    for step in range(n_sp):
        p = lax.rem(z + step, n_sp)
        for d in range(n_tp):
            info = meta[p * n_tp + tp]
            slot = ((z * n_tp + flip(tp, d)) * cap + iota).astype(f32)
            hit = (info[0:1, :] == slot) | (info[1:2, :] == slot)
            smat[p, d * cap : (d + 1) * cap, :] = hit.astype(f32)[:, :rows].astype(bf16)
            info, first, second = held(p, d)
            weight = jnp.where(first, info[2:3, :], 0.0) + jnp.where(second, info[3:4, :], 0.0)
            wcol[p, d * cap : (d + 1) * cap, :] = jnp.sum(weight, axis=1, keepdims=True)
            if not step:
                hit = (first | second).astype(f32)[:, :rows].astype(bf16)
                som[d * cap : (d + 1) * cap, d * rows : (d + 1) * rows] = hit

    def piece(p, d, q):
        return p, pl.ds(d * cap, cap), cols(q)

    def spread_out(p, d, q):
        at = piece(p, d, q)
        return remote(gbuf.at[at], crow.at[at], gsend.at[p, d, q], grecv.at[p, d, q], peer(d))

    def c_unit(p, q, k=None, target=None):
        block_out(p, q, 0, peer(1)).wait_recv()
        if k is not None:
            block_out(p, q, k, target).start()
        picked = dot(smat[p], blk[p, :, cols(q)]).astype(bf16)
        gbuf[p, :, cols(q)] = picked
        crow[p, :cap, cols(q)] = picked[:cap]
        for d in (2, 3, 1):
            spread_out(p, d, q).start()

    def hidden(p, q):
        taken = crow[p, :, cols(q)]
        hg[p] += dot_nt(taken, eg[:, cols(q)])
        hu[p] += dot_nt(taken, eu[:, cols(q)])

    def h_unit(p, q):
        for d in (1, 2, 3):
            spread_out(p, d, q).wait_recv()
        hidden(p, q)

    def act_out(p, d):
        at = (p, pl.ds(d * cap, cap))
        return remote(aout.at[at], ain.at[at], asend.at[p, d], arecv.at[p, d], peer(d))

    def factor_of(p, d):
        source = p * n_tp + flip(tp, d)

        @pl.when(source != me)
        def _():
            remote(
                factor_out, factors.at[source], fsend.at[0], frecv_f.at[source], peer(1)
            ).wait_recv()

        return factors[source][0:1, :]

    def silu(gate):
        return gate / (1.0 + jnp.exp(-gate))

    def activate(p, values=None):
        for d in range(n_tp):
            at = pl.ds(d * cap, cap)
            value = factor_of(p, d) if values is None else values[d]
            _, first, second = held(p, d)
            scale = jnp.sum(jnp.where(first | second, value, 0.0), axis=1, keepdims=True)
            made = silu(hg[p, at, :] * scale) * (hu[p, at, :] * scale) * wcol[p, at, :]
            made = made.astype(bf16)
            if d:
                aout[p, at, :] = made
                act_out(p, d).start()
            else:
                ain[p, at, :] = made

    def mix_in(p):
        for d in range(n_tp):
            if d:
                act_out(p, d).wait_recv()
            at = pl.ds(d * cap, cap)
            spread_act[p, d] = dot_tn(smat[p, at, :], ain[p, at, :]).astype(bf16)

    def own_unit(q):
        gather_out(2, q).wait_recv()
        gather_on(q).start()
        gather_out(1, q).wait_recv()
        gather_on(q).wait_recv()
        full = plane[:, cols(q)]
        crow[z, :, cols(q)] = dot(som[...], full).astype(bf16)
        shg[...] += dot(full, sg[cols(q), :])
        shu[...] += dot(full, su[cols(q), :])
        hidden(z, q)

    def own_activate():
        values = [factor_of(z, d) for d in range(n_tp)]
        activate(z, values)
        i, j = grid((rows, lanes))
        for d in range(n_tp):
            at = pl.ds(d * rows, rows)
            scale = jnp.sum(jnp.where(i == j, values[d], 0.0), axis=1, keepdims=True)
            sact[at, :] = (silu(shg[at, :] * scale) * (shu[at, :] * scale)).astype(bf16)

    def outcome(p, q):
        total = dot(spread_act[p, 0], ed[0, :, cols(q)])
        for d in range(1, n_tp):
            total = total + dot(spread_act[p, d], ed[d, :, cols(q)])
        return total

    def down_relay(q):
        @pl.when(lax.rem(q, 2) != group)
        def _():
            down_out(2, q).wait_recv()

        down_on(q).start()

    def down_ready(q):
        down_out(1, q).wait_recv()
        down_on(q).wait_recv()

    def chain_out(p, q, last, step):
        into, sem = chin.at[p, :, cols(q)], drecv.at[p, q]
        if last:
            side = (1 - step) // 2
            into, sem = fin.at[side, :, cols(q)], frecv.at[side, q]
        return remote(chs.at[p, :, cols(q)], into, dsend.at[p, q], sem, {"sp": z + step})

    def d_unit(p, q, incoming, last, step):
        total = outcome(p, q)
        if incoming:
            chain_out(p, q, False, step).wait_recv()
            total = total + chin[p, :, cols(q)].astype(f32)
        chs[p, :, cols(q)] = total.astype(bf16)
        chain_out(p, q, last, step).start()

    def product(d, q):
        return dot(sact[d * rows : (d + 1) * rows, :], sd[:, cols(q)])

    def rs1(q):
        for d in (3, 1):
            sent[d, :, cols(q)] = product(d, q).astype(bf16)
            fold(d, q, 1).start()

    def rs2(q):
        total = product(2, q)
        fold(3, q, 1).wait_recv()
        sent[2, :, cols(q)] = (total + got[3, :, cols(q)].astype(f32)).astype(bf16)
        fold(2, q, 2).start()

    def base(q):
        total = product(0, q) + outcome(z, q) + stream[:, cols(q)].astype(f32)
        fold(1, q, 1).wait_recv()
        total = total + got[1, :, cols(q)].astype(f32)
        fold(2, q, 2).wait_recv()
        facc[:, cols(q)] = total + got[2, :, cols(q)].astype(f32)

    def arrive(side, q):
        at = fin.at[side, :, cols(q)]
        remote(at, at, dsend.at[0, q], frecv.at[side, q], peer(1)).wait_recv()
        return fin[side, :, cols(q)].astype(f32)

    def run(*steps):
        def each(q):
            for step in steps:
                step(q)

        return each

    def at_first(step):
        def each(q):
            @pl.when(q == 0)
            def _():
                step()

        return each

    def sends_done(copies):
        def one(q, carry):
            for copy in copies(q):
                copy.wait_send()
            return carry

        lax.fori_loop(0, chunks, one, 0)

    for k in (5, 6, 2, 3, 4):
        loads[k].wait()

    is_end = (z == 0) | (z == n_sp - 1)

    @pl.when(is_end)
    def _():
        p0, p1, p2 = z + way, z + 2 * way, z + 3 * way
        staged(run(lambda q: c_unit(p0, q), own_unit), lambda q: h_unit(p0, q))
        activate(p0)
        own_activate()
        staged(
            run(lambda q: c_unit(p1, q), down_relay),
            run(
                at_first(lambda: mix_in(p0)),
                lambda q: h_unit(p1, q),
                down_ready,
                lambda q: d_unit(p0, q, False, True, way),
            ),
        )
        activate(p1)
        staged(
            lambda q: c_unit(p2, q),
            run(
                at_first(lambda: mix_in(p1)),
                lambda q: h_unit(p2, q),
                lambda q: d_unit(p1, q, False, False, way),
            ),
        )
        activate(p2)
        staged(rs1)
        mix_in(p2)
        staged(run(lambda q: d_unit(p2, q, False, False, way), rs2))
        mix_in(z)
        staged(base)

        def last(q):
            out_ref[:, cols(q)] = (facc[:, cols(q)] + arrive((1 + way) // 2, q)).astype(bf16)

        staged(last)
        sends_done(
            lambda q: [own_out(q, way)]
            + [spread_out(p, d, q) for p in (p0, p1, p2) for d in (1, 2, 3)]
            + [chain_out(p, q, False, way) for p in (p0, p1, p2)]
        )

    @pl.when(jnp.logical_not(is_end))
    def _():
        s0, s1, s2 = z - way, z + way, z + 2 * way
        ahead, behind = {"sp": z + way}, {"sp": z - way}
        staged(
            run(
                lambda q: c_unit(s0, q, 2, ahead),
                lambda q: c_unit(s1, q, 3, behind),
                own_unit,
            ),
            run(lambda q: h_unit(s0, q), lambda q: h_unit(s1, q)),
        )
        activate(s0)
        activate(s1)
        own_activate()
        staged(
            run(lambda q: c_unit(s2, q, 4, behind), down_relay),
            run(lambda q: h_unit(s2, q), down_ready),
        )
        activate(s2)
        mix_in(s1)
        staged(run(rs1, lambda q: d_unit(s1, q, True, True, way)), rs2)
        mix_in(s2)
        mix_in(s0)
        mix_in(z)
        staged(
            run(
                lambda q: d_unit(s2, q, True, False, way),
                lambda q: d_unit(s0, q, True, True, -way),
            ),
            base,
        )

        def last(q):
            total = facc[:, cols(q)] + arrive(0, q) + arrive(1, q)
            out_ref[:, cols(q)] = total.astype(bf16)

        staged(last)
        sends_done(
            lambda q: [own_out(q, way), own_out(q, -way)]
            + [block_out(s0, q, 2, ahead), block_out(s1, q, 3, behind)]
            + [block_out(s2, q, 4, behind)]
            + [spread_out(p, d, q) for p in (s0, s1, s2) for d in (1, 2, 3)]
            + [chain_out(p, q, False, way) for p in (s0, s1, s2)]
        )

    sends_done(
        lambda q: [gather_out(2, q), gather_out(1, q), gather_on(q)]
        + [down_out(1, q), down_on(q)]
        + [f(d, q, 1) for f in (fold, first_fold) for d in (3, 1, 2)]
    )
    for i in range(chunks // 2):
        down_out(2, 2 * i + group).wait_send()
        down_across(2 * i + group).wait_send()
    for p in range(n_sp):
        for d in range(1, n_tp):
            act_out(p, d).wait_send()

    def finish(k):
        fact_out(k).wait_send()
        factor_send(k).wait_send()

    others(finish)

    def latents_done(block, carry):
        @pl.when(z < n_sp - 1)
        def _():
            latent_out(block).wait_send()

        @pl.when(block < z)
        def _():
            latent_over(block).wait_send()

        return carry

    lax.fori_loop(0, z + 1, latents_done, 0)


def layer(near, far, n_sp, n_tp, cap, sizes, chunks=4):
    groups = len(sizes)
    rows_packed, cosine = near[:2]
    key_ws, value_ws = (near[3 + k * groups : 3 + (k + 1) * groups] for k in (1, 2))
    residual = near[-1]
    facts = near[-3]
    tok, lanes = cosine.shape
    rows, width = residual.shape
    ow, on, sg, su, sd, eg, eu, ed = far
    slots = n_tp * cap
    hidden, share = eg.shape[0], sg.shape[1]
    bf16, f32 = jnp.bfloat16, jnp.float32
    count = n_sp * n_tp

    def sems(*shape):
        return pltpu.SemaphoreType.DMA(shape)

    def half(*shape):
        return pltpu.VMEM(shape, bf16)

    def full(*shape):
        return pltpu.VMEM(shape, f32)

    scratch = attend_scratch(tok, lanes, key_ws, value_ws, sizes)
    scratch += [half(n_sp * tok, rows_packed.shape[1])]
    scratch += [half(tok, w.shape[1]) for w in value_ws]
    scratch += [full(count, *facts.shape), full(count, *facts.shape), full(*facts.shape)]
    scratch += [half(rows, width), half(rows, width)]
    scratch += [half(n_sp, rows, width), half(n_tp * rows, width)]
    scratch += [half(n_sp, slots, width)] * 2
    scratch += [half(n_sp, rows, width)] * 2 + [half(2, rows, width)]
    scratch += [half(n_tp, rows, width)] * 4
    scratch += [half(*w.shape) for w in far[:-1]] + [half(n_tp, *ed.shape)]
    scratch += [half(n_sp, slots, rows), half(slots, n_tp * rows), full(n_sp, slots, 1)]
    scratch += [full(n_sp, slots, hidden)] * 2
    scratch += [half(n_sp, slots, hidden)] * 2
    scratch += [half(n_sp, n_tp, rows, hidden)]
    scratch += [full(n_tp * rows, share)] * 2 + [half(n_tp * rows, share)]
    scratch += [full(rows, width), full(rows, 1)]
    scratch += [sems(8)] + [sems(n_sp)] * 4
    scratch += [sems(count)] * 4
    scratch += [sems(n_tp, chunks)] * 2
    scratch += [sems(5, chunks), sems(n_sp, chunks)]
    scratch += [sems(n_sp, n_tp, chunks)] * 2
    scratch += [sems(n_sp, n_tp)] * 2
    scratch += [sems(n_sp, chunks), sems(n_sp, chunks), sems(2, chunks)]
    scratch += [sems(n_tp, chunks)] * 6 + [sems(chunks)]
    return pl.pallas_call(
        lambda *refs: layer_kernel(chunks, cap, sizes, *refs),
        out_shape=jax.ShapeDtypeStruct((rows, width), bf16),
        in_specs=[VMEM] * len(near) + [pl.BlockSpec(memory_space=pl.ANY)] * len(far),
        out_specs=VMEM,
        scratch_shapes=scratch,
        compiler_params=pltpu.CompilerParams(
            collective_id=4, has_side_effects=True, vmem_limit_bytes=60 << 20
        ),
    )(*near, *far)


def rms_scale(values, gain):
    return values * lax.rsqrt(jnp.mean(values * values, axis=-1, keepdims=True) + EPS) * gain


def body(
    latent,
    rope_key,
    wide_query,
    narrow_query,
    wide_key_weight,
    wide_value_weight,
    narrow_key_weight,
    narrow_value_weight,
    latent_norm_scale,
    out_wide,
    out_narrow,
    residual,
    ffn_gain,
    shared_gate,
    shared_up,
    shared_down,
    expert_gate,
    expert_up,
    expert_down,
    routes,
    route_weights,
):
    tok_dev = latent.shape[0]
    seq_index = lax.axis_index("sp")
    own_pos = seq_index * tok_dev + jnp.arange(tok_dev, dtype=jnp.int32)
    n_sp, n_tp = lax.axis_size("sp"), lax.axis_size("tp")
    normed_latent = rms_scale(latent.astype(jnp.float32), latent_norm_scale).astype(jnp.bfloat16)
    half = ROPE // 2
    lane = jnp.arange(ROPE + -ROPE % 128, dtype=jnp.int32)
    inverse = ROPE_BASE ** (-(lane % half).astype(jnp.float32) * 2.0 / ROPE)
    angles = own_pos.astype(jnp.float32)[:, None] * inverse[None, :]
    cosine, sine = jnp.cos(angles), jnp.sin(angles)
    row = jnp.arange(ROPE, dtype=jnp.int32)[:, None]
    same = (row == lane[None, :]).astype(jnp.bfloat16)
    cross = (row == lane[None, :] - half).astype(jnp.bfloat16) * (lane < ROPE)[None, :] - (
        (row == lane[None, :] + half) & (lane < half)[None, :]
    ).astype(jnp.bfloat16)
    turned_key = (
        jnp.dot(rope_key, same, preferred_element_type=jnp.float32) * cosine
        + jnp.dot(rope_key, cross.astype(jnp.bfloat16), preferred_element_type=jnp.float32) * sine
    ).astype(jnp.bfloat16)
    rows_here, top_count = routes.shape
    local_experts = expert_gate.shape[0]
    experts_all = local_experts * lax.axis_size(("sp", "tp"))
    capacity = max(2, 2 * top_count * rows_here // experts_all)
    flat_routes = routes.reshape(-1)
    assigned = flat_routes.shape[0]
    choose = (flat_routes[:, None] == jnp.arange(experts_all, dtype=jnp.int32)[None, :]).astype(
        jnp.float32
    )
    lower_mask = (jnp.arange(assigned)[:, None] > jnp.arange(assigned)[None, :]).astype(jnp.float32)
    earlier = jnp.dot(lower_mask, choose, precision=lax.Precision.HIGHEST)
    slots = jnp.sum(earlier * choose, axis=1).astype(jnp.int32)
    target = flat_routes * capacity + slots
    by_choice = target.reshape(rows_here, top_count)
    planes = n_sp == 4 and n_tp == 4 and local_experts == 1 and capacity % 16 == 0
    fused = planes and top_count == 2 and rows_here <= 128 and lax.axis_size("grp") == 2
    rows_packed = jnp.concatenate([normed_latent, turned_key], axis=1)
    queries = (wide_query, narrow_query)
    key_ws = (wide_key_weight, narrow_key_weight)
    value_ws = (wide_value_weight, narrow_value_weight)
    sizes = (WIDE_HEAD_SIZE, NARROW_HEAD_SIZE)
    if fused:
        spare = (-rows_here) % 128
        facts = jnp.concatenate([by_choice.astype(jnp.float32).T, route_weights.T], axis=0)
        facts = jnp.pad(facts, ((0, 4), (0, spare)), constant_values=-1.0)
        near = (rows_packed, cosine, sine, *queries, *key_ws, *value_ws)
        near += (facts, ffn_gain[None, :], residual)
        far = (out_wide, out_narrow, shared_gate, shared_up, shared_down)
        far += (expert_gate[0].T, expert_up[0].T, expert_down[0])
        return layer(near, far, n_sp, n_tp, capacity, sizes)
    packed = spread(rows_packed, n_sp, n_tp)
    wide_mix, narrow_mix = attend(packed, cosine, sine, queries, key_ws, value_ws, sizes)
    (projected,) = dot_scatter((wide_mix, narrow_mix), (out_wide, out_narrow), n_tp, 2)
    stream = (residual.astype(jnp.float32) + projected).astype(jnp.bfloat16)
    normed = rms_scale(stream.astype(jnp.float32), ffn_gain).astype(jnp.bfloat16)
    model_width = normed.shape[1]
    send_map = jnp.any(
        target.reshape(rows_here, top_count)[None, :, :]
        == jnp.arange(experts_all * capacity, dtype=jnp.int32)[:, None, None],
        axis=2,
    ).astype(jnp.bfloat16)
    outgoing = jnp.dot(send_map, normed, preferred_element_type=jnp.float32).astype(jnp.bfloat16)
    devices = n_sp * n_tp
    outgoing = outgoing.reshape(devices, local_experts * capacity, model_width)
    piece, incoming = gather_rows(normed, outgoing, n_tp)
    sources = devices
    incoming = incoming.reshape(experts_all, capacity, model_width)
    grouped = incoming.reshape(sources, local_experts, incoming.shape[1], model_width)
    gate_part = jnp.einsum(
        "sxcd,xdf->sxcf", grouped, expert_gate, preferred_element_type=jnp.float32
    )
    up_part = jnp.einsum("sxcd,xdf->sxcf", grouped, expert_up, preferred_element_type=jnp.float32)
    active = (jax.nn.silu(gate_part) * up_part).astype(jnp.bfloat16)
    finished = jnp.einsum(
        "sxcf,xfd->sxcd", active, expert_down, preferred_element_type=jnp.float32
    ).astype(jnp.bfloat16)
    gate_part = jnp.dot(piece, shared_gate, preferred_element_type=jnp.float32)
    up_part = jnp.dot(piece, shared_up, preferred_element_type=jnp.float32)
    active = (jax.nn.silu(gate_part) * up_part).astype(jnp.bfloat16)
    shared, returned = dot_scatter(
        (active,), (shared_down,), n_tp, 3, finished.reshape(outgoing.shape)
    )
    slot_rows = returned.reshape(experts_all * capacity, model_width)
    routed = jnp.zeros((rows_here, model_width), jnp.float32)
    for choice in range(top_count):
        hot = by_choice[:, choice : choice + 1] == jnp.arange(experts_all * capacity)[None, :]
        picked = jnp.dot(
            hot.astype(jnp.bfloat16), slot_rows, preferred_element_type=jnp.float32
        )
        routed = routed + picked * route_weights[:, choice : choice + 1]
    return (stream.astype(jnp.float32) + shared + routed).astype(jnp.bfloat16)


def solution(mesh):
    placed = (
        P(("grp", "sp"), None),
        P(("grp", "sp"), None),
        P(("grp", "sp"), "tp"),
        P(("grp", "sp"), "tp"),
        P(None, "tp"),
        P(None, "tp"),
        P(None, "tp"),
        P(None, "tp"),
        P(),
        P("tp", None),
        P("tp", None),
        P(("grp", "sp", "tp"), None),
        P(),
        P(None, "tp"),
        P(None, "tp"),
        P("tp", None),
        P(("sp", "tp"), None, None),
        P(("sp", "tp"), None, None),
        P(("sp", "tp"), None, None),
        P(("grp", "sp", "tp"), None),
        P(("grp", "sp", "tp"), None),
    )
    return jax.shard_map(
        body, mesh=mesh, in_specs=placed, out_specs=P(("grp", "sp", "tp"), None), check_vma=False
    )
```

```python
import jax
import jax.numpy as jnp
import numpy as np
from jax import lax
from jax.experimental import pallas as pl
from jax.experimental.pallas import tpu as pltpu
from jax.sharding import PartitionSpec as P

ROPE = 64
WIDE_HEAD_SIZE = 128
NARROW_HEAD_SIZE = 64
EPS = 1e-06
ROPE_BASE = 10000.0
NEG_FILL = -1e30


MESH = pl.DeviceIdType.MESH
VMEM = pl.BlockSpec(memory_space=pltpu.VMEM)


def flip(index, bits):
    mask = 1
    while mask <= bits:
        if bits & mask:
            index = index + mask - 2 * mask * ((index // mask) % 2)
        mask *= 2
    return index


def masks_of(count):
    return [1 << k for k in range(count.bit_length() - 1)]


def low_bit(number):
    return number & -number


def greet(partners):
    barrier = pltpu.get_barrier_semaphore()
    for partner in partners:
        pl.semaphore_signal(barrier, inc=1, device_id=partner, device_id_type=MESH)
    pl.semaphore_wait(barrier, len(partners))


def doubling_order(count):
    return sorted(range(count), key=lambda d: (bin(d).count("1"), -d))


def remote(src, dst, send_sem, recv_sem, target):
    return pltpu.make_async_remote_copy(
        src_ref=src,
        dst_ref=dst,
        send_sem=send_sem,
        recv_sem=recv_sem,
        device_id=target,
        device_id_type=MESH,
    )


def spread_kernel(n_sp, n_tp, x_ref, out_ref, z_send, z_recv, t_send, t_recv, own_sem):
    sp, tp = lax.axis_index("sp"), lax.axis_index("tp")
    tok = x_ref.shape[0]
    part = tok // n_tp
    targets = [{"sp": lax.rem(sp + r, n_sp)} for r in range(1, n_sp)]
    greet(targets + [{"tp": flip(tp, m)} for m in masks_of(n_tp)])

    def rows(block, member):
        return pl.ds(pl.multiple_of(block * tok + member * part, part), part)

    own = pltpu.make_async_copy(
        x_ref, out_ref.at[pl.ds(pl.multiple_of(sp * tok, tok), tok)], own_sem
    )
    sends = []
    for r in range(1, n_sp):
        copy = remote(
            x_ref.at[pl.ds(pl.multiple_of(tp * part, part), part)],
            out_ref.at[rows(sp, tp)],
            z_send.at[r],
            z_recv.at[r],
            targets[r - 1],
        )
        copy.start()
        sends.append(copy)
    own.start()

    def piece(r, d):
        return out_ref.at[rows(lax.rem(sp + n_sp - r, n_sp), flip(tp, d))]

    for d in doubling_order(n_tp):
        for r in range(1, n_sp):
            block = piece(r, d)
            if d == 0:
                sends[r - 1].wait_recv()
            else:
                remote(
                    block, block, t_send.at[r, d], t_recv.at[r, d], {"tp": flip(tp, low_bit(d))}
                ).wait_recv()
            for mask in reversed(masks_of(low_bit(d) if d else n_tp)):
                copy = remote(
                    block,
                    block,
                    t_send.at[r, d + mask],
                    t_recv.at[r, d + mask],
                    {"tp": flip(tp, mask)},
                )
                copy.start()
                sends.append(copy)
    for copy in sends:
        copy.wait_send()
    own.wait()


def spread(x, n_sp, n_tp):
    tok, width = x.shape
    return pl.pallas_call(
        lambda *refs: spread_kernel(n_sp, n_tp, *refs),
        out_shape=jax.ShapeDtypeStruct((n_sp * tok, width), x.dtype),
        in_specs=[VMEM],
        out_specs=VMEM,
        scratch_shapes=[
            pltpu.SemaphoreType.DMA((n_sp,)),
            pltpu.SemaphoreType.DMA((n_sp,)),
            pltpu.SemaphoreType.DMA((n_sp, n_tp)),
            pltpu.SemaphoreType.DMA((n_sp, n_tp)),
            pltpu.SemaphoreType.DMA,
        ],
        compiler_params=pltpu.CompilerParams(collective_id=0, has_side_effects=True),
        cost_estimate=pl.CostEstimate(flops=0, bytes_accessed=30_000_000, transcendentals=0),
    )(x)


def gather_kernel(
    n_tp, pieces, x_ref, blocks_ref, out_ref, moved_ref, send, recv, own_sem, *semaphores
):
    exchange = Exchange(blocks_ref, moved_ref, *semaphores)
    tp = lax.axis_index("tp")
    rows, width = x_ref.shape
    part = width // pieces
    exchange.greet()

    def block(d, c):
        start = pl.multiple_of(flip(tp, d) * rows, rows)
        return out_ref.at[pl.ds(start, rows), pl.ds(c * part, part)]

    own = pltpu.make_async_copy(
        x_ref, out_ref.at[pl.ds(pl.multiple_of(tp * rows, rows), rows)], own_sem
    )
    sends = []
    for d in doubling_order(n_tp):
        for c in range(pieces):
            source = x_ref.at[:, pl.ds(c * part, part)] if d == 0 else block(d, c)
            if d:
                remote(
                    source, source, send.at[d, c], recv.at[d, c], {"tp": flip(tp, low_bit(d))}
                ).wait_recv()
            for mask in reversed(masks_of(low_bit(d) if d else n_tp)):
                copy = remote(
                    source,
                    block(d, c),
                    send.at[d + mask, c],
                    recv.at[d + mask, c],
                    {"tp": flip(tp, mask)},
                )
                copy.start()
                sends.append(copy)
        if d == 0:
            exchange.start()
            own.start()
    for copy in sends:
        copy.wait_send()
    own.wait()
    exchange.finish()


def gather_rows(x, blocks, n_tp, pieces=2):
    rows, width = x.shape
    return pl.pallas_call(
        lambda *refs: gather_kernel(n_tp, pieces, *refs),
        out_shape=[
            jax.ShapeDtypeStruct((n_tp * rows, width), x.dtype),
            jax.ShapeDtypeStruct(blocks.shape, blocks.dtype),
        ],
        in_specs=[VMEM] * 2,
        out_specs=[VMEM] * 2,
        scratch_shapes=[
            pltpu.SemaphoreType.DMA((n_tp, pieces)),
            pltpu.SemaphoreType.DMA((n_tp, pieces)),
            pltpu.SemaphoreType.DMA,
        ]
        + exchange_semaphores(blocks.shape[0]),
        compiler_params=pltpu.CompilerParams(collective_id=1, has_side_effects=True),
        cost_estimate=pl.CostEstimate(flops=0, bytes_accessed=40_000_000, transcendentals=0),
    )(x, blocks)


def scatter_kernel(n_tp, pieces, pairs, moving, *refs):
    lefts, rights = refs[:pairs], refs[pairs : 2 * pairs]
    refs = refs[2 * pairs :]
    exchange = None
    if moving:
        blocks_ref, out_ref, moved_ref, sent, got, send, recv = refs[:7]
        exchange = Exchange(blocks_ref, moved_ref, *refs[7:])
    else:
        out_ref, sent, got, send, recv = refs
    tp = lax.axis_index("tp")
    rows, width = out_ref.shape
    part = width // pieces
    if moving:
        exchange.greet()
        exchange.start()
    else:
        greet([{"tp": flip(tp, m)} for m in masks_of(n_tp)])
    copies = {}

    def product(d, c):
        start = pl.multiple_of(flip(tp, d) * rows, rows)
        total = None
        for left, right in zip(lefts, rights):
            term = jnp.dot(
                left[pl.ds(start, rows), :],
                right[:, pl.ds(c * part, part)],
                preferred_element_type=jnp.float32,
            )
            total = term if total is None else total + term
        return total

    def summed(d, c, below):
        total = product(d, c)
        if below > 1:
            total = total.astype(jnp.bfloat16).astype(jnp.float32)
        for mask in masks_of(below):
            copies[d + mask, c].wait_recv()
            total = total + got[d + mask, :, pl.ds(c * part, part)].astype(jnp.float32)
        return total

    def pass_on(mask, c):
        for d in range(mask, n_tp, 2 * mask):
            sent[d, :, pl.ds(c * part, part)] = summed(d, c, mask).astype(jnp.bfloat16)
            copies[d, c] = remote(
                sent.at[d, :, pl.ds(c * part, part)],
                got.at[d, :, pl.ds(c * part, part)],
                send.at[d, c],
                recv.at[d, c],
                {"tp": flip(tp, mask)},
            )
            copies[d, c].start()

    masks = masks_of(n_tp)
    for step in range(pieces + len(masks) - 1):
        for stage, mask in enumerate(masks):
            if 0 <= step - stage < pieces:
                pass_on(mask, step - stage)
    for c in range(pieces):
        out_ref[:, pl.ds(c * part, part)] = summed(0, c, n_tp)
    for copy in copies.values():
        copy.wait_send()
    if moving:
        exchange.finish()


def dot_scatter(lefts, rights, n_tp, collective, blocks=None, pieces=4):
    rows, width = lefts[0].shape[0] // n_tp, rights[0].shape[1]
    pairs, moving = len(lefts), blocks is not None
    shapes = [jax.ShapeDtypeStruct((rows, width), jnp.float32)]
    operands = (*lefts, *rights)
    scratch = [
        pltpu.VMEM((n_tp, rows, width), jnp.bfloat16),
        pltpu.VMEM((n_tp, rows, width), jnp.bfloat16),
        pltpu.SemaphoreType.DMA((n_tp, pieces)),
        pltpu.SemaphoreType.DMA((n_tp, pieces)),
    ]
    if moving:
        shapes.append(jax.ShapeDtypeStruct(blocks.shape, blocks.dtype))
        operands += (blocks,)
        scratch += exchange_semaphores(blocks.shape[0])
    return pl.pallas_call(
        lambda *refs: scatter_kernel(n_tp, pieces, pairs, moving, *refs),
        out_shape=shapes,
        in_specs=[VMEM] * len(operands),
        out_specs=[VMEM] * len(shapes),
        scratch_shapes=scratch,
        compiler_params=pltpu.CompilerParams(collective_id=collective, has_side_effects=True),
        cost_estimate=pl.CostEstimate(flops=0, bytes_accessed=40_000_000, transcendentals=0),
    )(*operands)


def grid(shape):
    return lax.broadcasted_iota(jnp.int32, shape, 0), lax.broadcasted_iota(jnp.int32, shape, 1)


def attend_start(sizes, cosine, sine, queries, widths, scratch):
    half = ROPE // 2
    lanes = cosine.shape[1]
    for g, size in enumerate(sizes):
        plain, turned, peak, total, mixed = scratch[5 * g : 5 * g + 5]
        query = queries[g][...]
        width = query.shape[1]
        for h in range(plain.shape[0]):
            i, j = grid((width, widths[g]))
            select = (i == j + h * ROPE) & (j >= h * size) & (j < (h + 1) * size)
            plain[h] = jnp.dot(
                query, select.astype(jnp.bfloat16), preferred_element_type=jnp.float32
            ).astype(jnp.bfloat16)
            i, j = grid((width, lanes))
            base = h * (size + ROPE) + size
            same = ((i == j + base) & (j < ROPE)).astype(jnp.float32)
            upper = ((i == j + base + half) & (j < half)).astype(jnp.float32)
            lower = ((i == j + base - half) & (j >= half) & (j < ROPE)).astype(jnp.float32)
            straight = jnp.dot(
                query, same.astype(jnp.bfloat16), preferred_element_type=jnp.float32
            )
            crossed = jnp.dot(
                query, (lower - upper).astype(jnp.bfloat16), preferred_element_type=jnp.float32
            )
            turned[h] = (straight * cosine[...] + crossed * sine[...]).astype(jnp.bfloat16)
        peak[...] = jnp.full_like(peak, NEG_FILL)
        total[...] = jnp.zeros_like(total)
        mixed[...] = jnp.zeros_like(mixed)


def attend_block(sizes, packed, index, sp, key_ws, value_ws, scratch):
    latent_width = key_ws[0].shape[0]
    tok = scratch[0].shape[1]
    start = pl.ds(pl.multiple_of(index * tok, tok), tok)
    latent = packed[start, :latent_width]
    turned_rows = packed[start, latent_width:]
    i, j = grid((tok, tok))
    visible = index * tok + j <= sp * tok + i
    across = (((1,), (1,)), ((), ()))
    for g, size in enumerate(sizes):
        plain, turned, peak, total, mixed = scratch[5 * g : 5 * g + 5]
        factor = (size + ROPE) ** (-0.5)
        keys = jnp.dot(latent, key_ws[g][...], preferred_element_type=jnp.float32)
        keys = keys.astype(jnp.bfloat16)
        values = jnp.dot(latent, value_ws[g][...], preferred_element_type=jnp.float32)
        values = values.astype(jnp.bfloat16)
        for h in range(plain.shape[0]):
            scores = lax.dot_general(
                plain[h], keys, across, preferred_element_type=jnp.float32
            ) + lax.dot_general(
                turned[h], turned_rows, across, preferred_element_type=jnp.float32
            )
            scores = jnp.where(visible, scores * factor, NEG_FILL)
            old = peak[h]
            new = jnp.maximum(old, jnp.max(scores, axis=1, keepdims=True))
            probs = jnp.where(visible, jnp.exp(scores - new), 0.0)
            fading = jnp.exp(old - new)
            peak[h] = new
            total[h] = total[h] * fading + jnp.sum(probs, axis=1, keepdims=True)
            mixed[h] = mixed[h] * fading + jnp.dot(
                probs.astype(jnp.bfloat16), values, preferred_element_type=jnp.float32
            )


def attend_end(sizes, outs, scratch):
    for g, size in enumerate(sizes):
        plain, turned, peak, total, mixed = scratch[5 * g : 5 * g + 5]
        i, j = grid(outs[g].shape)
        result = jnp.zeros(outs[g].shape, jnp.float32)
        for h in range(plain.shape[0]):
            own = (j >= h * size) & (j < (h + 1) * size)
            result = jnp.where(own, mixed[h] / total[h], result)
        outs[g][...] = result.astype(jnp.bfloat16)


def attend_kernel(sizes, packed, cosine, sine, *refs):
    groups = len(sizes)
    queries, key_ws, value_ws = refs[:groups], refs[groups : 2 * groups], refs[2 * groups : 3 * groups]
    outs = refs[3 * groups : 4 * groups]
    scratch = refs[4 * groups :]
    sp = lax.axis_index("sp")
    attend_start(sizes, cosine, sine, queries, [w.shape[1] for w in key_ws], scratch)

    def one_block(index, carry):
        attend_block(sizes, packed, index, sp, key_ws, value_ws, scratch)
        return carry

    lax.fori_loop(0, sp + 1, one_block, 0)
    attend_end(sizes, outs, scratch)


def attend_scratch(tok, lanes, key_ws, value_ws, sizes):
    scratch = []
    for g, size in enumerate(sizes):
        heads = value_ws[g].shape[1] // size
        scratch += [
            pltpu.VMEM((heads, tok, key_ws[g].shape[1]), jnp.bfloat16),
            pltpu.VMEM((heads, tok, lanes), jnp.bfloat16),
            pltpu.VMEM((heads, tok, 1), jnp.float32),
            pltpu.VMEM((heads, tok, 1), jnp.float32),
            pltpu.VMEM((heads, tok, value_ws[g].shape[1]), jnp.float32),
        ]
    return scratch


def attend(packed, cosine, sine, queries, key_ws, value_ws, sizes):
    tok, lanes = cosine.shape
    scratch = attend_scratch(tok, lanes, key_ws, value_ws, sizes)
    return pl.pallas_call(
        lambda *refs: attend_kernel(sizes, *refs),
        out_shape=[jax.ShapeDtypeStruct((tok, w.shape[1]), jnp.bfloat16) for w in value_ws],
        in_specs=[VMEM] * (3 + 3 * len(sizes)),
        out_specs=[VMEM] * len(sizes),
        scratch_shapes=scratch,
    )(packed, cosine, sine, *queries, *key_ws, *value_ws)


class Exchange:
    def __init__(self, source, dest, send, recv, own_sem):
        self.refs = source, dest, send, recv
        self.sp, self.tp = lax.axis_index("sp"), lax.axis_index("tp")
        self.n_sp, self.n_tp = lax.axis_size("sp"), lax.axis_size("tp")
        self.count = self.n_sp * self.n_tp
        self.me = self.sp * self.n_tp + self.tp
        self.own = pltpu.make_async_copy(source.at[self.me], dest.at[self.me], own_sem)

    def target(self, k):
        return (
            lax.rem(self.sp + k // self.n_tp, self.n_sp),
            lax.rem(self.tp + lax.rem(k, self.n_tp), self.n_tp),
        )

    def greet(self):
        barrier = pltpu.get_barrier_semaphore()

        def one(k, carry):
            sp, tp = self.target(k)
            pl.semaphore_signal(
                barrier, inc=1, device_id={"sp": sp, "tp": tp}, device_id_type=MESH
            )
            return carry

        lax.fori_loop(1, self.count, one, 0)
        pl.semaphore_wait(barrier, self.count - 1)

    def copy(self, k):
        source, dest, send, recv = self.refs
        sp, tp = self.target(k)
        return remote(
            source.at[sp * self.n_tp + tp],
            dest.at[self.me],
            send.at[k],
            recv.at[k],
            {"sp": sp, "tp": tp},
        )

    def start(self):
        def one(k, carry):
            self.copy(self.count - k).start()
            return carry

        lax.fori_loop(1, self.count, one, 0)
        self.own.start()

    def finish(self):
        def one(k, carry):
            self.copy(k).wait()
            return carry

        lax.fori_loop(1, self.count, one, 0)
        self.own.wait()


def exchange_semaphores(count):
    return [
        pltpu.SemaphoreType.DMA((count,)),
        pltpu.SemaphoreType.DMA((count,)),
        pltpu.SemaphoreType.DMA,
    ]


def turn(straight, crossed, cosine, sine):
    return (straight * cosine + crossed * sine).astype(jnp.bfloat16)


def turn_picks(height, lanes, base):
    half = ROPE // 2
    i, j = grid((height, lanes))
    same = ((i == j + base) & (j < ROPE)).astype(jnp.float32)
    upper = ((i == j + base + half) & (j < half)).astype(jnp.float32)
    lower = ((i == j + base - half) & (j >= half) & (j < ROPE)).astype(jnp.float32)
    return same.astype(jnp.bfloat16), (lower - upper).astype(jnp.bfloat16)


class Heads:
    def __init__(self, sizes, widths, refs):
        self.sizes, self.widths = sizes, widths
        self.joined, self.peak, self.total, self.mixed, self.turned_ws = refs
        self.list = []
        row = 0
        for g, size in enumerate(sizes):
            for h in range(widths[g] // size):
                self.list.append((g, h, size, row))
                row += size

    def start(self, queries, value_ws, cosine, sine):
        lanes = cosine.shape[1]
        cosine, sine = cosine[...], sine[...]
        for n, (g, h, size, row) in enumerate(self.list):
            query = queries[g][...]
            i, j = grid((query.shape[1], lanes))
            base = h * (size + ROPE)
            start = h * size % lanes
            select = (i == j - start + base) & (j >= start) & (j < start + size)
            self.joined[n, :, :lanes] = jnp.dot(
                query, select.astype(jnp.bfloat16), preferred_element_type=jnp.float32
            ).astype(jnp.bfloat16)
            same, cross = turn_picks(query.shape[1], lanes, base + size)
            straight = jnp.dot(query, same, preferred_element_type=jnp.float32)
            crossed = jnp.dot(query, cross, preferred_element_type=jnp.float32)
            self.joined[n, :, lanes:] = turn(straight, crossed, cosine, sine)
        row = 0
        for weight in value_ws:
            self.turned_ws[row : row + weight.shape[1], :] = weight[...].T
            row += weight.shape[1]
        self.peak[...] = jnp.full_like(self.peak, NEG_FILL)
        self.total[...] = jnp.zeros_like(self.total)
        self.mixed[...] = jnp.zeros_like(self.mixed)

    def block(self, latent, turned_rows, key_ws, diagonal):
        lanes = turned_rows.shape[1]
        across = (((1,), (1,)), ((), ()))
        bf16, f32 = jnp.bfloat16, jnp.float32
        keys = [jnp.dot(latent, w[...], preferred_element_type=f32).astype(bf16) for w in key_ws]
        values = lax.dot_general(
            self.turned_ws[...], latent, across, preferred_element_type=f32
        ).astype(bf16)
        for n, (g, h, size, row) in enumerate(self.list):
            scale = (size + ROPE) ** (-0.5) * 1.4426950408889634
            start = h * size // lanes * lanes
            joined = jnp.concatenate([keys[g][:, start : start + lanes], turned_rows], axis=1)
            scores = lax.dot_general(joined, self.joined[n], across, preferred_element_type=f32)
            if diagonal:
                i, j = grid(scores.shape)
                scores = jnp.where(i <= j, scores, NEG_FILL)
            old = self.peak[n : n + 1, :]
            new = jnp.maximum(old, jnp.max(scores, axis=0, keepdims=True))
            probs = jnp.exp2((scores - new) * scale)
            fading = jnp.exp2((old - new) * scale)
            self.peak[n : n + 1, :] = new
            self.total[n : n + 1, :] = self.total[n : n + 1, :] * fading + jnp.sum(
                probs, axis=0, keepdims=True
            )
            at = slice(row, row + size)
            self.mixed[at, :] = self.mixed[at, :] * fading + jnp.dot(
                values[at, :], probs.astype(bf16), preferred_element_type=f32
            )

    def end(self, outs):
        for n, (g, h, size, row) in enumerate(self.list):
            at = slice(row, row + size)
            self.mixed[at, :] = self.mixed[at, :] / self.total[n : n + 1, :]
        row = 0
        for out in outs:
            out[...] = self.mixed[row : row + out.shape[1], :].T.astype(jnp.bfloat16)
            row += out.shape[1]


def layer_kernel(chunks, cap, sizes, *refs):
    groups = len(sizes)
    latent_ref, rope_ref, latent_gain = refs[:3]
    queries, key_ws, value_ws = (refs[3 + k * groups : 3 + (k + 1) * groups] for k in range(3))
    refs = refs[3 + 3 * groups :]
    routes_ref, weights_ref, gain_ref, residual_ref = refs[:4]
    hbm, tables, out_ref, refs = refs[4:12], refs[12:14], refs[14], refs[15:]
    heads = Heads(sizes, [w.shape[1] for w in value_ws], refs[:5])
    cosine, sine, facts_ref, refs = refs[5], refs[6], refs[7], refs[8:]
    packed, mixes, refs = refs[0], refs[1 : 1 + groups], refs[1 + groups :]
    meta, factors, factor_out, stream, x_scr = refs[:5]
    blk, plane, gbuf, crow, chs, chin, fin = refs[5:12]
    bsent, bgot, sent, got = refs[12:16]
    local = refs[16:24]
    ow, on, sg, su, sd, eg, eu, ed = local
    smat, som, wcol, hg, hu, aout, ain, spread_act, shg, shu, sact, facc, squares = refs[24:37]
    refs = refs[37:]
    wsem, lsend, lrecv, psend_l, precv_l, msend, mrecv, fsend, frecv_f = refs[:9]
    psend, precv, csend, crecv, gsend, grecv, asend, arecv = refs[9:17]
    dsend, drecv, frecv, rsend, rrecv, bsend, brecv, esend, erecv, ysend = refs[17:27]
    z, tp = lax.axis_index("sp"), lax.axis_index("tp")
    group = lax.axis_index("grp")
    n_sp, n_tp = lax.axis_size("sp"), lax.axis_size("tp")
    count = n_sp * n_tp
    me = z * n_tp + tp
    rows, width = stream.shape
    tok = latent_ref.shape[0]
    latent_width = latent_ref.shape[1]
    part = width // chunks
    hidden_width = eg.shape[0]
    way = 1 - 2 * (z // 2)
    f32, bf16 = jnp.float32, jnp.bfloat16

    def cols(q):
        return pl.ds(pl.multiple_of(q * part, part), part)

    def peer(d):
        return {"tp": flip(tp, d)}

    def dot(a, b):
        return jnp.dot(a, b, preferred_element_type=f32)

    def dot_nt(a, b):
        return lax.dot_general(a, b, (((1,), (1,)), ((), ())), preferred_element_type=f32)

    def dot_tn(a, b):
        return lax.dot_general(a, b, (((0,), (0,)), ((), ())), preferred_element_type=f32)

    def other(k):
        return {
            "sp": lax.rem(z + k // n_tp, n_sp),
            "tp": lax.rem(tp + lax.rem(k, n_tp), n_tp),
        }

    def others(step):
        def one(k, carry):
            step(k)
            return carry

        lax.fori_loop(1, count, one, 0)

    barrier = pltpu.get_barrier_semaphore()
    others(
        lambda k: pl.semaphore_signal(barrier, inc=1, device_id=other(k), device_id_type=MESH)
    )
    pl.semaphore_signal(barrier, inc=1, device_id={"grp": 1 - group}, device_id_type=MESH)
    landing = [ed.at[0] if k == 7 else local[k] for k in range(8)]
    loads = [pltpu.make_async_copy(a, b, wsem.at[k]) for k, (a, b) in enumerate(zip(hbm, landing))]
    own_rows = pl.ds(pl.multiple_of(z * tok, tok), tok)
    tables = [
        pltpu.make_async_copy(a.at[own_rows], b, wsem.at[8 + k])
        for k, (a, b) in enumerate(zip(tables, (cosine, sine)))
    ]
    for table in tables:
        table.start()
    for k in (7, 0, 1, 5, 6, 2, 3, 4):
        loads[k].start()

    latent = latent_ref[...].astype(f32)
    latent = rms_scale(latent, latent_gain[...])
    packed[own_rows, :latent_width] = latent.astype(bf16)
    firsts = routes_ref[...].astype(f32)
    facts_ref[...] = jnp.full_like(facts_ref, -1.0)
    i, j = grid((rows, rows))
    named = [firsts[k : k + 1, :] for k in range(2)]
    columns = [
        jnp.sum(jnp.where(i == j, name, 0.0), axis=1, keepdims=True) for name in named
    ]
    for k in range(2):
        before = [((column == named[k]) & (i < j)).astype(f32) for column in columns]
        slot = jnp.sum(before[0] + before[1], axis=0, keepdims=True)
        facts_ref[k : k + 1, :rows] = named[k] * cap + slot
    facts_ref[2:4, :rows] = weights_ref[...]
    same, cross = turn_picks(rope_ref.shape[0], cosine.shape[1], 0)
    straight, crossed = dot_tn(rope_ref[...], same), dot_tn(rope_ref[...], cross)
    for table in tables:
        table.wait()
    packed[own_rows, latent_width:] = turn(straight, crossed, cosine[...], sine[...])
    pl.semaphore_wait(barrier, count)

    half = tok // 2
    mine = lax.rem(tp, 2) * half

    def latent_rows(block, start):
        return pl.ds(pl.multiple_of(block * tok + start, half), half)

    def latent_out(block):
        into = packed.at[latent_rows(block, mine)]
        return remote(into, into, lsend.at[block], lrecv.at[block], {"sp": z + 1})

    def latent_over(block):
        at = packed.at[latent_rows(block, mine)]
        return remote(at, at, psend_l.at[block], precv_l.at[block], peer(1))

    def latent_here(block):
        at = packed.at[latent_rows(block, half - mine)]
        remote(at, at, psend_l.at[block], precv_l.at[block], peer(1)).wait_recv()

    @pl.when(z < n_sp - 1)
    def _():
        latent_out(z).start()

    def fact_out(k):
        return remote(facts_ref, meta.at[me], msend.at[k], mrecv.at[me], other(k))

    def factor_send(k):
        return remote(factor_out, factors.at[me], fsend.at[k], frecv_f.at[me], other(k))

    others(lambda k: fact_out(k).start())
    meta[me] = facts_ref[...]

    def down_out(m, q):
        return remote(
            ed.at[0, :, cols(q)],
            ed.at[m, :, cols(q)],
            esend.at[m, q],
            erecv.at[m, q],
            peer(m),
        )

    def down_on(q):
        return remote(
            ed.at[2, :, cols(q)],
            ed.at[3, :, cols(q)],
            esend.at[3, q],
            erecv.at[3, q],
            peer(1),
        )

    def down_across(q):
        at = ed.at[2, :, cols(q)]
        return remote(at, at, ysend.at[q], erecv.at[2, q], {"grp": 1 - group})

    loads[7].wait()
    for i in range(chunks // 2):
        down_out(2, 2 * i + group).start()
    for q in range(chunks):
        down_out(1, q).start()

    heads.start(queries, value_ws, cosine, sine)

    def attend_rows(block, diagonal):
        at = pl.ds(pl.multiple_of(block * tok, tok), tok)
        heads.block(packed[at, :latent_width], packed[at, latent_width:], key_ws, diagonal)

    attend_rows(z, True)

    def earlier(k, carry):
        block = z - k
        remote(
            packed.at[latent_rows(block, mine)],
            packed.at[latent_rows(block, mine)],
            lsend.at[block],
            lrecv.at[block],
            peer(1),
        ).wait_recv()

        @pl.when(z < n_sp - 1)
        def _():
            latent_out(block).start()

        latent_over(block).start()
        latent_here(block)
        attend_rows(block, False)
        return carry

    lax.fori_loop(1, z + 1, earlier, 0)
    heads.end(mixes)

    def block_out(p, q, k, target, source=None):
        source = blk.at[p, :, cols(q)] if source is None else source
        return remote(source, blk.at[p, :, cols(q)], csend.at[k, q], crecv.at[p, q], target)

    def own_out(q, step):
        return block_out(z, q, (1 - step) // 2, {"sp": z + step}, x_scr.at[:, cols(q)])

    def gather_out(m, q):
        return remote(
            x_scr.at[:, cols(q)],
            plane.at[pl.ds(m * rows, rows), cols(q)],
            psend.at[m, q],
            precv.at[m, q],
            peer(m),
        )

    def gather_on(q):
        return remote(
            plane.at[pl.ds(2 * rows, rows), cols(q)],
            plane.at[pl.ds(3 * rows, rows), cols(q)],
            psend.at[3, q],
            precv.at[3, q],
            peer(1),
        )

    def fold_in(sends, gets, send_sem, recv_sem):
        def fold(d, q, mask):
            return remote(
                sends.at[d, :, cols(q)],
                gets.at[d, :, cols(q)],
                send_sem.at[d, q],
                recv_sem.at[d, q],
                peer(mask),
            )

        return fold

    first_fold = fold_in(bsent, bgot, bsend, brecv)
    fold = fold_in(sent, got, rsend, rrecv)

    def projected(d, q):
        start = pl.ds(pl.multiple_of(flip(tp, d) * rows, rows), rows)
        return dot(mixes[0][start, :], ow[:, cols(q)]) + dot(mixes[1][start, :], on[:, cols(q)])

    def b1(q):
        for d in (3, 1):
            bsent[d, :, cols(q)] = projected(d, q).astype(bf16)
            first_fold(d, q, 1).start()

    def b2(q):
        total = projected(2, q)
        first_fold(3, q, 1).wait_recv()
        bsent[2, :, cols(q)] = (total + bgot[3, :, cols(q)].astype(f32)).astype(bf16)
        first_fold(2, q, 2).start()

    def b3(q):
        total = projected(0, q) + residual_ref[:, cols(q)].astype(f32)
        first_fold(1, q, 1).wait_recv()
        total = total + bgot[1, :, cols(q)].astype(f32)
        first_fold(2, q, 2).wait_recv()
        total = (total + bgot[2, :, cols(q)].astype(f32)).astype(bf16)
        stream[:, cols(q)] = total
        total = total.astype(f32)
        squares[...] += jnp.sum(total * total, axis=1, keepdims=True)
        scaled = (total * gain_ref[:, cols(q)]).astype(bf16)
        x_scr[:, cols(q)] = scaled

        @pl.when(z < n_sp - 1)
        def _():
            own_out(q, 1).start()

        @pl.when(z > 0)
        def _():
            own_out(q, -1).start()

        plane[:rows, cols(q)] = scaled

        @pl.when(q < chunks // 2)
        def _():
            down_out(2, 2 * q + group).wait_recv()
            down_across(2 * q + group).start()

    def staged(*stages):
        def one(q, carry):
            for lag, stage in enumerate(stages):

                @pl.when((q >= lag) & (q < chunks + lag))
                def _():
                    stage(q - lag)

            return carry

        lax.fori_loop(0, chunks + len(stages) - 1, one, 0)

    hg[...] = jnp.zeros_like(hg)
    hu[...] = jnp.zeros_like(hu)
    shg[...] = jnp.zeros_like(shg)
    shu[...] = jnp.zeros_like(shu)
    som[...] = jnp.zeros_like(som)
    lanes = meta.shape[2]
    iota = lax.broadcasted_iota(jnp.int32, (cap, lanes), 0)

    def fact_wait(k):
        source = lax.rem(z + k // n_tp, n_sp) * n_tp + lax.rem(tp + lax.rem(k, n_tp), n_tp)
        remote(facts_ref, meta.at[source], msend.at[k], mrecv.at[source], peer(1)).wait_recv()

    others(fact_wait)

    def held(p, d):
        info = meta[p * n_tp + flip(tp, d)]
        slot = ((z * n_tp + tp) * cap + iota).astype(f32)
        return info, info[0:1, :] == slot, info[1:2, :] == slot

    for step in range(n_sp):
        p = lax.rem(z + step, n_sp)
        for d in range(n_tp):
            info = meta[p * n_tp + tp]
            slot = ((z * n_tp + flip(tp, d)) * cap + iota).astype(f32)
            hit = (info[0:1, :] == slot) | (info[1:2, :] == slot)
            smat[p, d * cap : (d + 1) * cap, :] = hit.astype(f32)[:, :rows].astype(bf16)
            info, first, second = held(p, d)
            weight = jnp.where(first, info[2:3, :], 0.0) + jnp.where(second, info[3:4, :], 0.0)
            wcol[p, d * cap : (d + 1) * cap, :] = jnp.sum(weight, axis=1, keepdims=True)
            if not step:
                hit = (first | second).astype(f32)[:, :rows].astype(bf16)
                som[d * cap : (d + 1) * cap, d * rows : (d + 1) * rows] = hit

    def piece(p, d, q):
        return p, pl.ds(d * cap, cap), cols(q)

    def spread_out(p, d, q):
        at = piece(p, d, q)
        return remote(gbuf.at[at], crow.at[at], gsend.at[p, d, q], grecv.at[p, d, q], peer(d))

    def c_unit(p, q, k=None, target=None):
        block_out(p, q, 0, peer(1)).wait_recv()
        if k is not None:
            block_out(p, q, k, target).start()
        picked = dot(smat[p], blk[p, :, cols(q)]).astype(bf16)
        gbuf[p, :, cols(q)] = picked
        crow[p, :cap, cols(q)] = picked[:cap]
        for d in (2, 3, 1):
            spread_out(p, d, q).start()

    def hidden(p, q):
        taken = crow[p, :, cols(q)]
        hg[p] += dot_nt(taken, eg[:, cols(q)])
        hu[p] += dot_nt(taken, eu[:, cols(q)])

    def h_unit(p, q):
        for d in (1, 2, 3):
            spread_out(p, d, q).wait_recv()
        hidden(p, q)

    def act_out(p, d):
        at = (p, pl.ds(d * cap, cap))
        return remote(aout.at[at], ain.at[at], asend.at[p, d], arecv.at[p, d], peer(d))

    def factor_of(p, d):
        source = p * n_tp + flip(tp, d)

        @pl.when(source != me)
        def _():
            remote(
                factor_out, factors.at[source], fsend.at[0], frecv_f.at[source], peer(1)
            ).wait_recv()

        return factors[source][0:1, :]

    def silu(gate):
        return gate / (1.0 + jnp.exp(-gate))

    def activate(p, values=None):
        for d in range(n_tp):
            at = pl.ds(d * cap, cap)
            value = factor_of(p, d) if values is None else values[d]
            _, first, second = held(p, d)
            scale = jnp.sum(jnp.where(first | second, value, 0.0), axis=1, keepdims=True)
            made = silu(hg[p, at, :] * scale) * (hu[p, at, :] * scale) * wcol[p, at, :]
            made = made.astype(bf16)
            if d:
                aout[p, at, :] = made
                act_out(p, d).start()
            else:
                ain[p, at, :] = made

    def mix_in(p):
        for d in range(n_tp):
            if d:
                act_out(p, d).wait_recv()
            at = pl.ds(d * cap, cap)
            spread_act[p, d] = dot_tn(smat[p, at, :], ain[p, at, :]).astype(bf16)

    def own_spread(q):
        gather_out(2, q).start()
        gather_out(1, q).start()

    def own_unit(q):
        gather_out(2, q).wait_recv()
        gather_on(q).start()
        gather_out(1, q).wait_recv()
        gather_on(q).wait_recv()
        full = plane[:, cols(q)]
        crow[z, :, cols(q)] = dot(som[...], full).astype(bf16)
        shg[...] += dot(full, sg[cols(q), :])
        shu[...] += dot(full, su[cols(q), :])
        hidden(z, q)

    def own_activate():
        values = [factor_of(z, d) for d in range(n_tp)]
        activate(z, values)
        i, j = grid((rows, lanes))
        for d in range(n_tp):
            at = pl.ds(d * rows, rows)
            scale = jnp.sum(jnp.where(i == j, values[d], 0.0), axis=1, keepdims=True)
            sact[at, :] = (silu(shg[at, :] * scale) * (shu[at, :] * scale)).astype(bf16)

    def outcome(p, q):
        total = dot(spread_act[p, 0], ed[0, :, cols(q)])
        for d in range(1, n_tp):
            total = total + dot(spread_act[p, d], ed[d, :, cols(q)])
        return total

    def down_relay(q):
        @pl.when(lax.rem(q, 2) != group)
        def _():
            down_out(2, q).wait_recv()

        down_on(q).start()

    def down_ready(q):
        down_out(1, q).wait_recv()
        down_on(q).wait_recv()

    def chain_out(p, q, last, step):
        into, sem = chin.at[p, :, cols(q)], drecv.at[p, q]
        if last:
            side = (1 - step) // 2
            into, sem = fin.at[side, :, cols(q)], frecv.at[side, q]
        return remote(chs.at[p, :, cols(q)], into, dsend.at[p, q], sem, {"sp": z + step})

    def d_unit(p, q, incoming, last, step):
        total = outcome(p, q)
        if incoming:
            chain_out(p, q, False, step).wait_recv()
            total = total + chin[p, :, cols(q)].astype(f32)
        chs[p, :, cols(q)] = total.astype(bf16)
        chain_out(p, q, last, step).start()

    def product(d, q):
        return dot(sact[d * rows : (d + 1) * rows, :], sd[:, cols(q)])

    def rs1(q):
        for d in (3, 1):
            sent[d, :, cols(q)] = product(d, q).astype(bf16)
            fold(d, q, 1).start()

    def rs2(q):
        total = product(2, q)
        fold(3, q, 1).wait_recv()
        sent[2, :, cols(q)] = (total + got[3, :, cols(q)].astype(f32)).astype(bf16)
        fold(2, q, 2).start()

    def base(q):
        total = product(0, q) + outcome(z, q) + stream[:, cols(q)].astype(f32)
        fold(1, q, 1).wait_recv()
        total = total + got[1, :, cols(q)].astype(f32)
        fold(2, q, 2).wait_recv()
        facc[:, cols(q)] = total + got[2, :, cols(q)].astype(f32)

    def arrive(side, q):
        at = fin.at[side, :, cols(q)]
        remote(at, at, dsend.at[0, q], frecv.at[side, q], peer(1)).wait_recv()
        return fin[side, :, cols(q)].astype(f32)

    def run(*steps):
        def each(q):
            for step in steps:
                step(q)

        return each

    def at_first(step):
        def each(q):
            @pl.when(q == 0)
            def _():
                step()

        return each

    def at_odd(first):
        def each(q):
            @pl.when(lax.rem(q, 2) == 1)
            def _():
                own_spread(first + q // 2)

        return each

    def sends_done(copies):
        def one(q, carry):
            for copy in copies(q):
                copy.wait_send()
            return carry

        lax.fori_loop(0, chunks, one, 0)

    loads[0].wait()
    loads[1].wait()
    squares[...] = jnp.zeros_like(squares)
    is_end = (z == 0) | (z == n_sp - 1)
    ahead, behind = {"sp": z + way}, {"sp": z - way}

    def c_first(q):
        @pl.when(is_end)
        def _():
            c_unit(z + way, q)

        @pl.when(jnp.logical_not(is_end))
        def _():
            c_unit(z - way, q, 2, ahead)
            c_unit(z + way, q, 3, behind)

    def h_first(q):
        @pl.when(is_end)
        def _():
            h_unit(z + way, q)

        @pl.when(jnp.logical_not(is_end))
        def _():
            h_unit(z - way, q)
            h_unit(z + way, q)

    for k in (5, 6):
        loads[k].wait()
    staged(b1, b2, b3, c_first, h_first)
    factor = lax.rsqrt(squares[...] * (1.0 / width) + EPS)
    i, j = grid((rows, factor_out.shape[1]))
    factor = jnp.sum(jnp.where(i == j, factor, 0.0), axis=0, keepdims=True)
    factor_out[...] = jnp.broadcast_to(factor, factor_out.shape)
    others(lambda k: factor_send(k).start())
    factors[me] = factor_out[...]

    for k in (2, 3, 4):
        loads[k].wait()

    @pl.when(is_end)
    def _():
        p0, p1, p2 = z + way, z + 2 * way, z + 3 * way
        activate(p0)
        staged(
            run(lambda q: c_unit(p1, q), down_relay, at_odd(0)),
            run(
                at_first(lambda: mix_in(p0)),
                down_ready,
                lambda q: d_unit(p0, q, False, True, way),
                lambda q: h_unit(p1, q),
            ),
        )
        activate(p1)
        staged(
            run(lambda q: c_unit(p2, q), at_odd(chunks // 2)),
            run(
                at_first(lambda: mix_in(p1)),
                lambda q: d_unit(p1, q, False, False, way),
                lambda q: h_unit(p2, q),
            ),
        )
        activate(p2)
        mix_in(p2)
        staged(lambda q: d_unit(p2, q, False, False, way))
        staged(own_unit)
        own_activate()
        staged(rs1, rs2)
        mix_in(z)
        staged(base)

        def last(q):
            out_ref[:, cols(q)] = (facc[:, cols(q)] + arrive((1 + way) // 2, q)).astype(bf16)

        staged(last)
        sends_done(
            lambda q: [own_out(q, way)]
            + [spread_out(p, d, q) for p in (p0, p1, p2) for d in (1, 2, 3)]
            + [chain_out(p, q, False, way) for p in (p0, p1, p2)]
        )

    @pl.when(jnp.logical_not(is_end))
    def _():
        s0, s1, s2 = z - way, z + way, z + 2 * way
        activate(s0)
        activate(s1)
        staged(
            run(lambda q: c_unit(s2, q, 4, behind), down_relay),
            run(lambda q: h_unit(s2, q), down_ready),
        )
        staged(own_spread)
        activate(s2)
        mix_in(s1)
        staged(run(own_unit, lambda q: d_unit(s1, q, True, True, way)))
        own_activate()
        mix_in(s2)
        mix_in(s0)
        staged(rs1, rs2)
        mix_in(z)
        staged(
            run(
                lambda q: d_unit(s2, q, True, False, way),
                lambda q: d_unit(s0, q, True, True, -way),
                base,
            ),
        )

        def last(q):
            total = facc[:, cols(q)] + arrive(0, q) + arrive(1, q)
            out_ref[:, cols(q)] = total.astype(bf16)

        staged(last)
        sends_done(
            lambda q: [own_out(q, way), own_out(q, -way)]
            + [block_out(s0, q, 2, ahead), block_out(s1, q, 3, behind)]
            + [block_out(s2, q, 4, behind)]
            + [spread_out(p, d, q) for p in (s0, s1, s2) for d in (1, 2, 3)]
            + [chain_out(p, q, False, way) for p in (s0, s1, s2)]
        )

    sends_done(
        lambda q: [gather_out(2, q), gather_out(1, q), gather_on(q)]
        + [down_out(1, q), down_on(q)]
        + [f(d, q, 1) for f in (fold, first_fold) for d in (3, 1, 2)]
    )
    for i in range(chunks // 2):
        down_out(2, 2 * i + group).wait_send()
        down_across(2 * i + group).wait_send()
    for p in range(n_sp):
        for d in range(1, n_tp):
            act_out(p, d).wait_send()

    def finish(k):
        fact_out(k).wait_send()
        factor_send(k).wait_send()

    others(finish)

    def latents_done(block, carry):
        @pl.when(z < n_sp - 1)
        def _():
            latent_out(block).wait_send()

        @pl.when(block < z)
        def _():
            latent_over(block).wait_send()

        return carry

    lax.fori_loop(0, z + 1, latents_done, 0)


def rotary_tables(tokens, lanes):
    half = ROPE // 2
    lane = np.arange(lanes) % half
    inverse = np.float32(ROPE_BASE) ** (-lane.astype(np.float32) * np.float32(2.0 / ROPE))
    angles = np.arange(tokens, dtype=np.float32)[:, None] * inverse.astype(np.float32)[None, :]
    return jnp.asarray(np.cos(angles)), jnp.asarray(np.sin(angles))


def layer(near, far, n_sp, n_tp, cap, sizes, chunks=4):
    groups = len(sizes)
    tok, latent_width = near[0].shape
    key_ws, value_ws = (near[3 + k * groups : 3 + (k + 1) * groups] for k in (1, 2))
    residual = near[-1]
    lanes = ROPE + -ROPE % 128
    tables = rotary_tables(n_sp * tok, lanes)
    rows, width = residual.shape
    ow, on, sg, su, sd, eg, eu, ed = far
    slots = n_tp * cap
    hidden, share = eg.shape[0], sg.shape[1]
    bf16, f32 = jnp.bfloat16, jnp.float32
    count = n_sp * n_tp

    def sems(*shape):
        return pltpu.SemaphoreType.DMA(shape)

    def half(*shape):
        return pltpu.VMEM(shape, bf16)

    def full(*shape):
        return pltpu.VMEM(shape, f32)

    depth = sum(w.shape[1] for w in value_ws)
    number = sum(w.shape[1] // size for w, size in zip(value_ws, sizes))
    fact_shape = (8, rows + -rows % 128)
    scratch = [half(number, tok, 2 * lanes), full(-(-number // 8) * 8, tok)]
    scratch += [full(-(-number // 8) * 8, tok), full(depth, tok), half(depth, latent_width)]
    scratch += [full(tok, lanes), full(tok, lanes), full(*fact_shape)]
    scratch += [half(n_sp * tok, latent_width + lanes)]
    scratch += [half(tok, w.shape[1]) for w in value_ws]
    scratch += [full(count, *fact_shape), full(count, *fact_shape), full(*fact_shape)]
    scratch += [half(rows, width), half(rows, width)]
    scratch += [half(n_sp, rows, width), half(n_tp * rows, width)]
    scratch += [half(n_sp, slots, width)] * 2
    scratch += [half(n_sp, rows, width)] * 2 + [half(2, rows, width)]
    scratch += [half(n_tp, rows, width)] * 4
    scratch += [half(*w.shape) for w in far[:-1]] + [half(n_tp, *ed.shape)]
    scratch += [half(n_sp, slots, rows), half(slots, n_tp * rows), full(n_sp, slots, 1)]
    scratch += [full(n_sp, slots, hidden)] * 2
    scratch += [half(n_sp, slots, hidden)] * 2
    scratch += [half(n_sp, n_tp, rows, hidden)]
    scratch += [full(n_tp * rows, share)] * 2 + [half(n_tp * rows, share)]
    scratch += [full(rows, width), full(rows, 1)]
    scratch += [sems(10)] + [sems(n_sp)] * 4
    scratch += [sems(count)] * 4
    scratch += [sems(n_tp, chunks)] * 2
    scratch += [sems(5, chunks), sems(n_sp, chunks)]
    scratch += [sems(n_sp, n_tp, chunks)] * 2
    scratch += [sems(n_sp, n_tp)] * 2
    scratch += [sems(n_sp, chunks), sems(n_sp, chunks), sems(2, chunks)]
    scratch += [sems(n_tp, chunks)] * 6 + [sems(chunks)]
    return pl.pallas_call(
        lambda *refs: layer_kernel(chunks, cap, sizes, *refs),
        out_shape=jax.ShapeDtypeStruct((rows, width), bf16),
        in_specs=[VMEM] * len(near) + [pl.BlockSpec(memory_space=pl.ANY)] * (len(far) + 2),
        out_specs=VMEM,
        scratch_shapes=scratch,
        compiler_params=pltpu.CompilerParams(
            collective_id=4, has_side_effects=True, vmem_limit_bytes=60 << 20
        ),
    )(*near, *far, *tables)


def rms_scale(values, gain):
    return values * lax.rsqrt(jnp.mean(values * values, axis=-1, keepdims=True) + EPS) * gain


def body(
    latent,
    rope_key,
    wide_query,
    narrow_query,
    wide_key_weight,
    wide_value_weight,
    narrow_key_weight,
    narrow_value_weight,
    latent_norm_scale,
    out_wide,
    out_narrow,
    residual,
    ffn_gain,
    shared_gate,
    shared_up,
    shared_down,
    expert_gate,
    expert_up,
    expert_down,
    routes,
    route_weights,
):
    tok_dev = latent.shape[0]
    seq_index = lax.axis_index("sp")
    own_pos = seq_index * tok_dev + jnp.arange(tok_dev, dtype=jnp.int32)
    n_sp, n_tp = lax.axis_size("sp"), lax.axis_size("tp")
    rows_here, top_count = routes.shape
    local_experts = expert_gate.shape[0]
    experts_all = local_experts * lax.axis_size(("sp", "tp"))
    capacity = max(2, 2 * top_count * rows_here // experts_all)
    queries = (wide_query, narrow_query)
    key_ws = (wide_key_weight, narrow_key_weight)
    value_ws = (wide_value_weight, narrow_value_weight)
    sizes = (WIDE_HEAD_SIZE, NARROW_HEAD_SIZE)
    planes = n_sp == 4 and n_tp == 4 and local_experts == 1 and capacity % 16 == 0
    if planes and top_count == 2 and rows_here <= 128 and lax.axis_size("grp") == 2:
        near = (latent, rope_key.T, latent_norm_scale[None, :], *queries, *key_ws, *value_ws)
        near += (routes.T, route_weights.T, ffn_gain[None, :], residual)
        far = (out_wide, out_narrow, shared_gate, shared_up, shared_down)
        far += (expert_gate[0].T, expert_up[0].T, expert_down[0])
        return layer(near, far, n_sp, n_tp, capacity, sizes)
    normed_latent = rms_scale(latent.astype(jnp.float32), latent_norm_scale).astype(jnp.bfloat16)
    half = ROPE // 2
    lane = jnp.arange(ROPE + -ROPE % 128, dtype=jnp.int32)
    inverse = ROPE_BASE ** (-(lane % half).astype(jnp.float32) * 2.0 / ROPE)
    angles = own_pos.astype(jnp.float32)[:, None] * inverse[None, :]
    cosine, sine = jnp.cos(angles), jnp.sin(angles)
    row = jnp.arange(ROPE, dtype=jnp.int32)[:, None]
    same = (row == lane[None, :]).astype(jnp.bfloat16)
    cross = (row == lane[None, :] - half).astype(jnp.bfloat16) * (lane < ROPE)[None, :] - (
        (row == lane[None, :] + half) & (lane < half)[None, :]
    ).astype(jnp.bfloat16)
    turned_key = (
        jnp.dot(rope_key, same, preferred_element_type=jnp.float32) * cosine
        + jnp.dot(rope_key, cross.astype(jnp.bfloat16), preferred_element_type=jnp.float32) * sine
    ).astype(jnp.bfloat16)
    flat_routes = routes.reshape(-1)
    assigned = flat_routes.shape[0]
    choose = (flat_routes[:, None] == jnp.arange(experts_all, dtype=jnp.int32)[None, :]).astype(
        jnp.float32
    )
    lower_mask = (jnp.arange(assigned)[:, None] > jnp.arange(assigned)[None, :]).astype(jnp.float32)
    earlier = jnp.dot(lower_mask, choose, precision=lax.Precision.HIGHEST)
    slots = jnp.sum(earlier * choose, axis=1).astype(jnp.int32)
    target = flat_routes * capacity + slots
    by_choice = target.reshape(rows_here, top_count)
    rows_packed = jnp.concatenate([normed_latent, turned_key], axis=1)
    packed = spread(rows_packed, n_sp, n_tp)
    wide_mix, narrow_mix = attend(packed, cosine, sine, queries, key_ws, value_ws, sizes)
    (projected,) = dot_scatter((wide_mix, narrow_mix), (out_wide, out_narrow), n_tp, 2)
    stream = (residual.astype(jnp.float32) + projected).astype(jnp.bfloat16)
    normed = rms_scale(stream.astype(jnp.float32), ffn_gain).astype(jnp.bfloat16)
    model_width = normed.shape[1]
    send_map = jnp.any(
        target.reshape(rows_here, top_count)[None, :, :]
        == jnp.arange(experts_all * capacity, dtype=jnp.int32)[:, None, None],
        axis=2,
    ).astype(jnp.bfloat16)
    outgoing = jnp.dot(send_map, normed, preferred_element_type=jnp.float32).astype(jnp.bfloat16)
    devices = n_sp * n_tp
    outgoing = outgoing.reshape(devices, local_experts * capacity, model_width)
    piece, incoming = gather_rows(normed, outgoing, n_tp)
    sources = devices
    incoming = incoming.reshape(experts_all, capacity, model_width)
    grouped = incoming.reshape(sources, local_experts, incoming.shape[1], model_width)
    gate_part = jnp.einsum(
        "sxcd,xdf->sxcf", grouped, expert_gate, preferred_element_type=jnp.float32
    )
    up_part = jnp.einsum("sxcd,xdf->sxcf", grouped, expert_up, preferred_element_type=jnp.float32)
    active = (jax.nn.silu(gate_part) * up_part).astype(jnp.bfloat16)
    finished = jnp.einsum(
        "sxcf,xfd->sxcd", active, expert_down, preferred_element_type=jnp.float32
    ).astype(jnp.bfloat16)
    gate_part = jnp.dot(piece, shared_gate, preferred_element_type=jnp.float32)
    up_part = jnp.dot(piece, shared_up, preferred_element_type=jnp.float32)
    active = (jax.nn.silu(gate_part) * up_part).astype(jnp.bfloat16)
    shared, returned = dot_scatter(
        (active,), (shared_down,), n_tp, 3, finished.reshape(outgoing.shape)
    )
    slot_rows = returned.reshape(experts_all * capacity, model_width)
    routed = jnp.zeros((rows_here, model_width), jnp.float32)
    for choice in range(top_count):
        hot = by_choice[:, choice : choice + 1] == jnp.arange(experts_all * capacity)[None, :]
        picked = jnp.dot(
            hot.astype(jnp.bfloat16), slot_rows, preferred_element_type=jnp.float32
        )
        routed = routed + picked * route_weights[:, choice : choice + 1]
    return (stream.astype(jnp.float32) + shared + routed).astype(jnp.bfloat16)


def solution(mesh):
    placed = (
        P(("grp", "sp"), None),
        P(("grp", "sp"), None),
        P(("grp", "sp"), "tp"),
        P(("grp", "sp"), "tp"),
        P(None, "tp"),
        P(None, "tp"),
        P(None, "tp"),
        P(None, "tp"),
        P(),
        P("tp", None),
        P("tp", None),
        P(("grp", "sp", "tp"), None),
        P(),
        P(None, "tp"),
        P(None, "tp"),
        P("tp", None),
        P(("sp", "tp"), None, None),
        P(("sp", "tp"), None, None),
        P(("sp", "tp"), None, None),
        P(("grp", "sp", "tp"), None),
        P(("grp", "sp", "tp"), None),
    )
    return jax.shard_map(
        body, mesh=mesh, in_specs=placed, out_specs=P(("grp", "sp", "tp"), None), check_vma=False
    )
```

```python
import jax
import jax.numpy as jnp
import numpy as np
from jax import lax
from jax.experimental import pallas as pl
from jax.experimental.pallas import tpu as pltpu
from jax.sharding import PartitionSpec as P

ROPE = 64
WIDE_HEAD_SIZE = 128
NARROW_HEAD_SIZE = 64
EPS = 1e-06
ROPE_BASE = 10000.0
NEG_FILL = -1e30


MESH = pl.DeviceIdType.MESH
VMEM = pl.BlockSpec(memory_space=pltpu.VMEM)


def flip(index, bits):
    mask = 1
    while mask <= bits:
        if bits & mask:
            index = index + mask - 2 * mask * ((index // mask) % 2)
        mask *= 2
    return index


def masks_of(count):
    return [1 << k for k in range(count.bit_length() - 1)]


def low_bit(number):
    return number & -number


def greet(partners):
    barrier = pltpu.get_barrier_semaphore()
    for partner in partners:
        pl.semaphore_signal(barrier, inc=1, device_id=partner, device_id_type=MESH)
    pl.semaphore_wait(barrier, len(partners))


def doubling_order(count):
    return sorted(range(count), key=lambda d: (bin(d).count("1"), -d))


def remote(src, dst, send_sem, recv_sem, target):
    return pltpu.make_async_remote_copy(
        src_ref=src,
        dst_ref=dst,
        send_sem=send_sem,
        recv_sem=recv_sem,
        device_id=target,
        device_id_type=MESH,
    )


def spread_kernel(n_sp, n_tp, x_ref, out_ref, z_send, z_recv, t_send, t_recv, own_sem):
    sp, tp = lax.axis_index("sp"), lax.axis_index("tp")
    tok = x_ref.shape[0]
    part = tok // n_tp
    targets = [{"sp": lax.rem(sp + r, n_sp)} for r in range(1, n_sp)]
    greet(targets + [{"tp": flip(tp, m)} for m in masks_of(n_tp)])

    def rows(block, member):
        return pl.ds(pl.multiple_of(block * tok + member * part, part), part)

    own = pltpu.make_async_copy(
        x_ref, out_ref.at[pl.ds(pl.multiple_of(sp * tok, tok), tok)], own_sem
    )
    sends = []
    for r in range(1, n_sp):
        copy = remote(
            x_ref.at[pl.ds(pl.multiple_of(tp * part, part), part)],
            out_ref.at[rows(sp, tp)],
            z_send.at[r],
            z_recv.at[r],
            targets[r - 1],
        )
        copy.start()
        sends.append(copy)
    own.start()

    def piece(r, d):
        return out_ref.at[rows(lax.rem(sp + n_sp - r, n_sp), flip(tp, d))]

    for d in doubling_order(n_tp):
        for r in range(1, n_sp):
            block = piece(r, d)
            if d == 0:
                sends[r - 1].wait_recv()
            else:
                remote(
                    block, block, t_send.at[r, d], t_recv.at[r, d], {"tp": flip(tp, low_bit(d))}
                ).wait_recv()
            for mask in reversed(masks_of(low_bit(d) if d else n_tp)):
                copy = remote(
                    block,
                    block,
                    t_send.at[r, d + mask],
                    t_recv.at[r, d + mask],
                    {"tp": flip(tp, mask)},
                )
                copy.start()
                sends.append(copy)
    for copy in sends:
        copy.wait_send()
    own.wait()


def spread(x, n_sp, n_tp):
    tok, width = x.shape
    return pl.pallas_call(
        lambda *refs: spread_kernel(n_sp, n_tp, *refs),
        out_shape=jax.ShapeDtypeStruct((n_sp * tok, width), x.dtype),
        in_specs=[VMEM],
        out_specs=VMEM,
        scratch_shapes=[
            pltpu.SemaphoreType.DMA((n_sp,)),
            pltpu.SemaphoreType.DMA((n_sp,)),
            pltpu.SemaphoreType.DMA((n_sp, n_tp)),
            pltpu.SemaphoreType.DMA((n_sp, n_tp)),
            pltpu.SemaphoreType.DMA,
        ],
        compiler_params=pltpu.CompilerParams(collective_id=0, has_side_effects=True),
        cost_estimate=pl.CostEstimate(flops=0, bytes_accessed=30_000_000, transcendentals=0),
    )(x)


def gather_kernel(
    n_tp, pieces, x_ref, blocks_ref, out_ref, moved_ref, send, recv, own_sem, *semaphores
):
    exchange = Exchange(blocks_ref, moved_ref, *semaphores)
    tp = lax.axis_index("tp")
    rows, width = x_ref.shape
    part = width // pieces
    exchange.greet()

    def block(d, c):
        start = pl.multiple_of(flip(tp, d) * rows, rows)
        return out_ref.at[pl.ds(start, rows), pl.ds(c * part, part)]

    own = pltpu.make_async_copy(
        x_ref, out_ref.at[pl.ds(pl.multiple_of(tp * rows, rows), rows)], own_sem
    )
    sends = []
    for d in doubling_order(n_tp):
        for c in range(pieces):
            source = x_ref.at[:, pl.ds(c * part, part)] if d == 0 else block(d, c)
            if d:
                remote(
                    source, source, send.at[d, c], recv.at[d, c], {"tp": flip(tp, low_bit(d))}
                ).wait_recv()
            for mask in reversed(masks_of(low_bit(d) if d else n_tp)):
                copy = remote(
                    source,
                    block(d, c),
                    send.at[d + mask, c],
                    recv.at[d + mask, c],
                    {"tp": flip(tp, mask)},
                )
                copy.start()
                sends.append(copy)
        if d == 0:
            exchange.start()
            own.start()
    for copy in sends:
        copy.wait_send()
    own.wait()
    exchange.finish()


def gather_rows(x, blocks, n_tp, pieces=2):
    rows, width = x.shape
    return pl.pallas_call(
        lambda *refs: gather_kernel(n_tp, pieces, *refs),
        out_shape=[
            jax.ShapeDtypeStruct((n_tp * rows, width), x.dtype),
            jax.ShapeDtypeStruct(blocks.shape, blocks.dtype),
        ],
        in_specs=[VMEM] * 2,
        out_specs=[VMEM] * 2,
        scratch_shapes=[
            pltpu.SemaphoreType.DMA((n_tp, pieces)),
            pltpu.SemaphoreType.DMA((n_tp, pieces)),
            pltpu.SemaphoreType.DMA,
        ]
        + exchange_semaphores(blocks.shape[0]),
        compiler_params=pltpu.CompilerParams(collective_id=1, has_side_effects=True),
        cost_estimate=pl.CostEstimate(flops=0, bytes_accessed=40_000_000, transcendentals=0),
    )(x, blocks)


def scatter_kernel(n_tp, pieces, pairs, moving, *refs):
    lefts, rights = refs[:pairs], refs[pairs : 2 * pairs]
    refs = refs[2 * pairs :]
    exchange = None
    if moving:
        blocks_ref, out_ref, moved_ref, sent, got, send, recv = refs[:7]
        exchange = Exchange(blocks_ref, moved_ref, *refs[7:])
    else:
        out_ref, sent, got, send, recv = refs
    tp = lax.axis_index("tp")
    rows, width = out_ref.shape
    part = width // pieces
    if moving:
        exchange.greet()
        exchange.start()
    else:
        greet([{"tp": flip(tp, m)} for m in masks_of(n_tp)])
    copies = {}

    def product(d, c):
        start = pl.multiple_of(flip(tp, d) * rows, rows)
        total = None
        for left, right in zip(lefts, rights):
            term = jnp.dot(
                left[pl.ds(start, rows), :],
                right[:, pl.ds(c * part, part)],
                preferred_element_type=jnp.float32,
            )
            total = term if total is None else total + term
        return total

    def summed(d, c, below):
        total = product(d, c)
        if below > 1:
            total = total.astype(jnp.bfloat16).astype(jnp.float32)
        for mask in masks_of(below):
            copies[d + mask, c].wait_recv()
            total = total + got[d + mask, :, pl.ds(c * part, part)].astype(jnp.float32)
        return total

    def pass_on(mask, c):
        for d in range(mask, n_tp, 2 * mask):
            sent[d, :, pl.ds(c * part, part)] = summed(d, c, mask).astype(jnp.bfloat16)
            copies[d, c] = remote(
                sent.at[d, :, pl.ds(c * part, part)],
                got.at[d, :, pl.ds(c * part, part)],
                send.at[d, c],
                recv.at[d, c],
                {"tp": flip(tp, mask)},
            )
            copies[d, c].start()

    masks = masks_of(n_tp)
    for step in range(pieces + len(masks) - 1):
        for stage, mask in enumerate(masks):
            if 0 <= step - stage < pieces:
                pass_on(mask, step - stage)
    for c in range(pieces):
        out_ref[:, pl.ds(c * part, part)] = summed(0, c, n_tp)
    for copy in copies.values():
        copy.wait_send()
    if moving:
        exchange.finish()


def dot_scatter(lefts, rights, n_tp, collective, blocks=None, pieces=4):
    rows, width = lefts[0].shape[0] // n_tp, rights[0].shape[1]
    pairs, moving = len(lefts), blocks is not None
    shapes = [jax.ShapeDtypeStruct((rows, width), jnp.float32)]
    operands = (*lefts, *rights)
    scratch = [
        pltpu.VMEM((n_tp, rows, width), jnp.bfloat16),
        pltpu.VMEM((n_tp, rows, width), jnp.bfloat16),
        pltpu.SemaphoreType.DMA((n_tp, pieces)),
        pltpu.SemaphoreType.DMA((n_tp, pieces)),
    ]
    if moving:
        shapes.append(jax.ShapeDtypeStruct(blocks.shape, blocks.dtype))
        operands += (blocks,)
        scratch += exchange_semaphores(blocks.shape[0])
    return pl.pallas_call(
        lambda *refs: scatter_kernel(n_tp, pieces, pairs, moving, *refs),
        out_shape=shapes,
        in_specs=[VMEM] * len(operands),
        out_specs=[VMEM] * len(shapes),
        scratch_shapes=scratch,
        compiler_params=pltpu.CompilerParams(collective_id=collective, has_side_effects=True),
        cost_estimate=pl.CostEstimate(flops=0, bytes_accessed=40_000_000, transcendentals=0),
    )(*operands)


def grid(shape):
    return lax.broadcasted_iota(jnp.int32, shape, 0), lax.broadcasted_iota(jnp.int32, shape, 1)


def attend_start(sizes, cosine, sine, queries, widths, scratch):
    half = ROPE // 2
    lanes = cosine.shape[1]
    for g, size in enumerate(sizes):
        plain, turned, peak, total, mixed = scratch[5 * g : 5 * g + 5]
        query = queries[g][...]
        width = query.shape[1]
        for h in range(plain.shape[0]):
            i, j = grid((width, widths[g]))
            select = (i == j + h * ROPE) & (j >= h * size) & (j < (h + 1) * size)
            plain[h] = jnp.dot(
                query, select.astype(jnp.bfloat16), preferred_element_type=jnp.float32
            ).astype(jnp.bfloat16)
            i, j = grid((width, lanes))
            base = h * (size + ROPE) + size
            same = ((i == j + base) & (j < ROPE)).astype(jnp.float32)
            upper = ((i == j + base + half) & (j < half)).astype(jnp.float32)
            lower = ((i == j + base - half) & (j >= half) & (j < ROPE)).astype(jnp.float32)
            straight = jnp.dot(
                query, same.astype(jnp.bfloat16), preferred_element_type=jnp.float32
            )
            crossed = jnp.dot(
                query, (lower - upper).astype(jnp.bfloat16), preferred_element_type=jnp.float32
            )
            turned[h] = (straight * cosine[...] + crossed * sine[...]).astype(jnp.bfloat16)
        peak[...] = jnp.full_like(peak, NEG_FILL)
        total[...] = jnp.zeros_like(total)
        mixed[...] = jnp.zeros_like(mixed)


def attend_block(sizes, packed, index, sp, key_ws, value_ws, scratch):
    latent_width = key_ws[0].shape[0]
    tok = scratch[0].shape[1]
    start = pl.ds(pl.multiple_of(index * tok, tok), tok)
    latent = packed[start, :latent_width]
    turned_rows = packed[start, latent_width:]
    i, j = grid((tok, tok))
    visible = index * tok + j <= sp * tok + i
    across = (((1,), (1,)), ((), ()))
    for g, size in enumerate(sizes):
        plain, turned, peak, total, mixed = scratch[5 * g : 5 * g + 5]
        factor = (size + ROPE) ** (-0.5)
        keys = jnp.dot(latent, key_ws[g][...], preferred_element_type=jnp.float32)
        keys = keys.astype(jnp.bfloat16)
        values = jnp.dot(latent, value_ws[g][...], preferred_element_type=jnp.float32)
        values = values.astype(jnp.bfloat16)
        for h in range(plain.shape[0]):
            scores = lax.dot_general(
                plain[h], keys, across, preferred_element_type=jnp.float32
            ) + lax.dot_general(
                turned[h], turned_rows, across, preferred_element_type=jnp.float32
            )
            scores = jnp.where(visible, scores * factor, NEG_FILL)
            old = peak[h]
            new = jnp.maximum(old, jnp.max(scores, axis=1, keepdims=True))
            probs = jnp.where(visible, jnp.exp(scores - new), 0.0)
            fading = jnp.exp(old - new)
            peak[h] = new
            total[h] = total[h] * fading + jnp.sum(probs, axis=1, keepdims=True)
            mixed[h] = mixed[h] * fading + jnp.dot(
                probs.astype(jnp.bfloat16), values, preferred_element_type=jnp.float32
            )


def attend_end(sizes, outs, scratch):
    for g, size in enumerate(sizes):
        plain, turned, peak, total, mixed = scratch[5 * g : 5 * g + 5]
        i, j = grid(outs[g].shape)
        result = jnp.zeros(outs[g].shape, jnp.float32)
        for h in range(plain.shape[0]):
            own = (j >= h * size) & (j < (h + 1) * size)
            result = jnp.where(own, mixed[h] / total[h], result)
        outs[g][...] = result.astype(jnp.bfloat16)


def attend_kernel(sizes, packed, cosine, sine, *refs):
    groups = len(sizes)
    queries, key_ws, value_ws = refs[:groups], refs[groups : 2 * groups], refs[2 * groups : 3 * groups]
    outs = refs[3 * groups : 4 * groups]
    scratch = refs[4 * groups :]
    sp = lax.axis_index("sp")
    attend_start(sizes, cosine, sine, queries, [w.shape[1] for w in key_ws], scratch)

    def one_block(index, carry):
        attend_block(sizes, packed, index, sp, key_ws, value_ws, scratch)
        return carry

    lax.fori_loop(0, sp + 1, one_block, 0)
    attend_end(sizes, outs, scratch)


def attend_scratch(tok, lanes, key_ws, value_ws, sizes):
    scratch = []
    for g, size in enumerate(sizes):
        heads = value_ws[g].shape[1] // size
        scratch += [
            pltpu.VMEM((heads, tok, key_ws[g].shape[1]), jnp.bfloat16),
            pltpu.VMEM((heads, tok, lanes), jnp.bfloat16),
            pltpu.VMEM((heads, tok, 1), jnp.float32),
            pltpu.VMEM((heads, tok, 1), jnp.float32),
            pltpu.VMEM((heads, tok, value_ws[g].shape[1]), jnp.float32),
        ]
    return scratch


def attend(packed, cosine, sine, queries, key_ws, value_ws, sizes):
    tok, lanes = cosine.shape
    scratch = attend_scratch(tok, lanes, key_ws, value_ws, sizes)
    return pl.pallas_call(
        lambda *refs: attend_kernel(sizes, *refs),
        out_shape=[jax.ShapeDtypeStruct((tok, w.shape[1]), jnp.bfloat16) for w in value_ws],
        in_specs=[VMEM] * (3 + 3 * len(sizes)),
        out_specs=[VMEM] * len(sizes),
        scratch_shapes=scratch,
    )(packed, cosine, sine, *queries, *key_ws, *value_ws)


class Exchange:
    def __init__(self, source, dest, send, recv, own_sem):
        self.refs = source, dest, send, recv
        self.sp, self.tp = lax.axis_index("sp"), lax.axis_index("tp")
        self.n_sp, self.n_tp = lax.axis_size("sp"), lax.axis_size("tp")
        self.count = self.n_sp * self.n_tp
        self.me = self.sp * self.n_tp + self.tp
        self.own = pltpu.make_async_copy(source.at[self.me], dest.at[self.me], own_sem)

    def target(self, k):
        return (
            lax.rem(self.sp + k // self.n_tp, self.n_sp),
            lax.rem(self.tp + lax.rem(k, self.n_tp), self.n_tp),
        )

    def greet(self):
        barrier = pltpu.get_barrier_semaphore()

        def one(k, carry):
            sp, tp = self.target(k)
            pl.semaphore_signal(
                barrier, inc=1, device_id={"sp": sp, "tp": tp}, device_id_type=MESH
            )
            return carry

        lax.fori_loop(1, self.count, one, 0)
        pl.semaphore_wait(barrier, self.count - 1)

    def copy(self, k):
        source, dest, send, recv = self.refs
        sp, tp = self.target(k)
        return remote(
            source.at[sp * self.n_tp + tp],
            dest.at[self.me],
            send.at[k],
            recv.at[k],
            {"sp": sp, "tp": tp},
        )

    def start(self):
        def one(k, carry):
            self.copy(self.count - k).start()
            return carry

        lax.fori_loop(1, self.count, one, 0)
        self.own.start()

    def finish(self):
        def one(k, carry):
            self.copy(k).wait()
            return carry

        lax.fori_loop(1, self.count, one, 0)
        self.own.wait()


def exchange_semaphores(count):
    return [
        pltpu.SemaphoreType.DMA((count,)),
        pltpu.SemaphoreType.DMA((count,)),
        pltpu.SemaphoreType.DMA,
    ]


def turn(straight, crossed, cosine, sine):
    return (straight * cosine + crossed * sine).astype(jnp.bfloat16)


def turn_picks(height, lanes, base):
    half = ROPE // 2
    i, j = grid((height, lanes))
    same = ((i == j + base) & (j < ROPE)).astype(jnp.float32)
    upper = ((i == j + base + half) & (j < half)).astype(jnp.float32)
    lower = ((i == j + base - half) & (j >= half) & (j < ROPE)).astype(jnp.float32)
    return same.astype(jnp.bfloat16), (lower - upper).astype(jnp.bfloat16)


class Heads:
    def __init__(self, sizes, widths, refs):
        self.sizes, self.widths = sizes, widths
        self.joined, self.peak, self.total, self.mixed, self.turned_ws = refs
        self.list = []
        row = 0
        for g, size in enumerate(sizes):
            for h in range(widths[g] // size):
                self.list.append((g, h, size, row))
                row += size

    def start(self, queries, value_ws, cosine, sine):
        lanes = cosine.shape[1]
        cosine, sine = cosine[...], sine[...]
        for n, (g, h, size, row) in enumerate(self.list):
            query = queries[g][...]
            i, j = grid((query.shape[1], lanes))
            base = h * (size + ROPE)
            start = h * size % lanes
            select = (i == j - start + base) & (j >= start) & (j < start + size)
            self.joined[n, :, :lanes] = jnp.dot(
                query, select.astype(jnp.bfloat16), preferred_element_type=jnp.float32
            ).astype(jnp.bfloat16)
            same, cross = turn_picks(query.shape[1], lanes, base + size)
            straight = jnp.dot(query, same, preferred_element_type=jnp.float32)
            crossed = jnp.dot(query, cross, preferred_element_type=jnp.float32)
            self.joined[n, :, lanes:] = turn(straight, crossed, cosine, sine)
        row = 0
        for weight in value_ws:
            self.turned_ws[row : row + weight.shape[1], :] = weight[...].T
            row += weight.shape[1]
        self.peak[...] = jnp.full_like(self.peak, NEG_FILL)
        self.total[...] = jnp.zeros_like(self.total)
        self.mixed[...] = jnp.zeros_like(self.mixed)

    def block(self, latent, turned_rows, key_ws, diagonal):
        lanes = turned_rows.shape[1]
        across = (((1,), (1,)), ((), ()))
        bf16, f32 = jnp.bfloat16, jnp.float32
        keys = [jnp.dot(latent, w[...], preferred_element_type=f32).astype(bf16) for w in key_ws]
        values = lax.dot_general(
            self.turned_ws[...], latent, across, preferred_element_type=f32
        ).astype(bf16)
        for n, (g, h, size, row) in enumerate(self.list):
            scale = (size + ROPE) ** (-0.5) * 1.4426950408889634
            start = h * size // lanes * lanes
            joined = jnp.concatenate([keys[g][:, start : start + lanes], turned_rows], axis=1)
            scores = lax.dot_general(joined, self.joined[n], across, preferred_element_type=f32)
            if diagonal:
                i, j = grid(scores.shape)
                scores = jnp.where(i <= j, scores, NEG_FILL)
            old = self.peak[n : n + 1, :]
            new = jnp.maximum(old, jnp.max(scores, axis=0, keepdims=True))
            probs = jnp.exp2((scores - new) * scale)
            fading = jnp.exp2((old - new) * scale)
            self.peak[n : n + 1, :] = new
            self.total[n : n + 1, :] = self.total[n : n + 1, :] * fading + jnp.sum(
                probs, axis=0, keepdims=True
            )
            at = slice(row, row + size)
            self.mixed[at, :] = self.mixed[at, :] * fading + jnp.dot(
                values[at, :], probs.astype(bf16), preferred_element_type=f32
            )

    def end(self, outs):
        for n, (g, h, size, row) in enumerate(self.list):
            at = slice(row, row + size)
            self.mixed[at, :] = self.mixed[at, :] / self.total[n : n + 1, :]
        row = 0
        for out in outs:
            out[...] = self.mixed[row : row + out.shape[1], :].T.astype(jnp.bfloat16)
            row += out.shape[1]


def layer_kernel(chunks, cap, sizes, *refs):
    groups = len(sizes)
    latent_ref, rope_ref, latent_gain = refs[:3]
    queries, key_ws, value_ws = (refs[3 + k * groups : 3 + (k + 1) * groups] for k in range(3))
    refs = refs[3 + 3 * groups :]
    routes_ref, weights_ref, gain_ref, residual_ref = refs[:4]
    hbm, tables, out_ref, refs = refs[4:12], refs[12:14], refs[14], refs[15:]
    heads = Heads(sizes, [w.shape[1] for w in value_ws], refs[:5])
    cosine, sine, facts_ref, refs = refs[5], refs[6], refs[7], refs[8:]
    packed, mixes, refs = refs[0], refs[1 : 1 + groups], refs[1 + groups :]
    meta, factors, factor_out, stream, x_scr = refs[:5]
    blk, plane, gbuf, crow, chs, chin, fin = refs[5:12]
    bsent, bgot, sent, got = refs[12:16]
    local = refs[16:24]
    ow, on, sg, su, sd, eg, eu, ed = local
    smat, som, wcol, hg, hu, aout, ain, spread_act, shg, shu, sact, facc, squares = refs[24:37]
    refs = refs[37:]
    wsem, lsend, lrecv, psend_l, precv_l, msend, mrecv, fsend, frecv_f = refs[:9]
    psend, precv, csend, crecv, gsend, grecv, asend, arecv = refs[9:17]
    dsend, drecv, frecv, rsend, rrecv, bsend, brecv, esend, erecv, ysend = refs[17:27]
    z, tp = lax.axis_index("sp"), lax.axis_index("tp")
    group = lax.axis_index("grp")
    n_sp, n_tp = lax.axis_size("sp"), lax.axis_size("tp")
    count = n_sp * n_tp
    me = z * n_tp + tp
    rows, width = stream.shape
    tok = latent_ref.shape[0]
    latent_width = latent_ref.shape[1]
    part = width // chunks
    hidden_width = eg.shape[0]
    way = 1 - 2 * (z // 2)
    f32, bf16 = jnp.float32, jnp.bfloat16

    def cols(q):
        return pl.ds(pl.multiple_of(q * part, part), part)

    def peer(d):
        return {"tp": flip(tp, d)}

    def dot(a, b):
        return jnp.dot(a, b, preferred_element_type=f32)

    def dot_nt(a, b):
        return lax.dot_general(a, b, (((1,), (1,)), ((), ())), preferred_element_type=f32)

    def dot_tn(a, b):
        return lax.dot_general(a, b, (((0,), (0,)), ((), ())), preferred_element_type=f32)

    def other(k):
        return {
            "sp": lax.rem(z + k // n_tp, n_sp),
            "tp": lax.rem(tp + lax.rem(k, n_tp), n_tp),
        }

    def others(step):
        def one(k, carry):
            step(k)
            return carry

        lax.fori_loop(1, count, one, 0)

    barrier = pltpu.get_barrier_semaphore()
    others(
        lambda k: pl.semaphore_signal(barrier, inc=1, device_id=other(k), device_id_type=MESH)
    )
    pl.semaphore_signal(barrier, inc=1, device_id={"grp": 1 - group}, device_id_type=MESH)
    landing = [ed.at[0] if k == 7 else local[k] for k in range(8)]
    loads = [pltpu.make_async_copy(a, b, wsem.at[k]) for k, (a, b) in enumerate(zip(hbm, landing))]
    own_rows = pl.ds(pl.multiple_of(z * tok, tok), tok)
    tables = [
        pltpu.make_async_copy(a.at[own_rows], b, wsem.at[8 + k])
        for k, (a, b) in enumerate(zip(tables, (cosine, sine)))
    ]
    for table in tables:
        table.start()
    for k in (7, 0, 1, 5, 6, 2, 3, 4):
        loads[k].start()

    latent = latent_ref[...].astype(f32)
    latent = rms_scale(latent, latent_gain[...])
    packed[own_rows, :latent_width] = latent.astype(bf16)
    firsts = routes_ref[...].astype(f32)
    facts_ref[...] = jnp.full_like(facts_ref, -1.0)
    i, j = grid((rows, rows))
    named = [firsts[k : k + 1, :] for k in range(2)]
    columns = [
        jnp.sum(jnp.where(i == j, name, 0.0), axis=1, keepdims=True) for name in named
    ]
    for k in range(2):
        before = [((column == named[k]) & (i < j)).astype(f32) for column in columns]
        slot = jnp.sum(before[0] + before[1], axis=0, keepdims=True)
        facts_ref[k : k + 1, :rows] = named[k] * cap + slot
    facts_ref[2:4, :rows] = weights_ref[...]
    same, cross = turn_picks(rope_ref.shape[0], cosine.shape[1], 0)
    straight, crossed = dot_tn(rope_ref[...], same), dot_tn(rope_ref[...], cross)
    for table in tables:
        table.wait()
    packed[own_rows, latent_width:] = turn(straight, crossed, cosine[...], sine[...])
    pl.semaphore_wait(barrier, count)

    pieces = lsend.shape[1]
    size = tok // (2 * pieces)
    mine = lax.rem(tp, 2) * pieces

    def latent_rows(block, piece):
        return packed.at[pl.ds(pl.multiple_of(block * tok + piece * size, size), size)]

    def latent_out(block, k):
        into = latent_rows(block, mine + k)
        return remote(into, into, lsend.at[block, k], lrecv.at[block, k], {"sp": z + 1})

    def latent_over(block, k):
        at = latent_rows(block, mine + k)
        return remote(at, at, psend_l.at[block, k], precv_l.at[block, k], peer(1))

    def latent_here(block, k):
        at = latent_rows(block, pieces - mine + k)
        remote(at, at, psend_l.at[block, k], precv_l.at[block, k], peer(1)).wait_recv()

    @pl.when(z < n_sp - 1)
    def _():
        for k in range(pieces):
            latent_out(z, k).start()

    def fact_out(k):
        return remote(facts_ref, meta.at[me], msend.at[k], mrecv.at[me], other(k))

    def factor_send(k):
        return remote(factor_out, factors.at[me], fsend.at[k], frecv_f.at[me], other(k))

    others(lambda k: fact_out(k).start())
    meta[me] = facts_ref[...]

    def down_out(m, q):
        return remote(
            ed.at[0, :, cols(q)],
            ed.at[m, :, cols(q)],
            esend.at[m, q],
            erecv.at[m, q],
            peer(m),
        )

    def down_on(q):
        return remote(
            ed.at[2, :, cols(q)],
            ed.at[3, :, cols(q)],
            esend.at[3, q],
            erecv.at[3, q],
            peer(1),
        )

    def down_across(q):
        at = ed.at[2, :, cols(q)]
        return remote(at, at, ysend.at[q], erecv.at[2, q], {"grp": 1 - group})

    loads[7].wait()
    for i in range(chunks // 2):
        down_out(2, 2 * i + group).start()
    for q in range(chunks):
        down_out(1, q).start()

    heads.start(queries, value_ws, cosine, sine)

    def attend_rows(block, diagonal):
        at = pl.ds(pl.multiple_of(block * tok, tok), tok)
        heads.block(packed[at, :latent_width], packed[at, latent_width:], key_ws, diagonal)

    attend_rows(z, True)

    def earlier(k, carry):
        block = z - k
        for n in range(pieces):
            at = latent_rows(block, mine + n)
            remote(at, at, lsend.at[block, n], lrecv.at[block, n], peer(1)).wait_recv()

            @pl.when(z < n_sp - 1)
            def _():
                latent_out(block, n).start()

            latent_over(block, n).start()
        for n in range(pieces):
            latent_here(block, n)
        attend_rows(block, False)
        return carry

    lax.fori_loop(1, z + 1, earlier, 0)
    heads.end(mixes)

    def block_out(p, q, k, target, source=None):
        source = blk.at[p, :, cols(q)] if source is None else source
        return remote(source, blk.at[p, :, cols(q)], csend.at[k, q], crecv.at[p, q], target)

    def own_out(q, step):
        return block_out(z, q, (1 - step) // 2, {"sp": z + step}, x_scr.at[:, cols(q)])

    def gather_out(m, q):
        return remote(
            x_scr.at[:, cols(q)],
            plane.at[pl.ds(m * rows, rows), cols(q)],
            psend.at[m, q],
            precv.at[m, q],
            peer(m),
        )

    def gather_on(q):
        return remote(
            plane.at[pl.ds(2 * rows, rows), cols(q)],
            plane.at[pl.ds(3 * rows, rows), cols(q)],
            psend.at[3, q],
            precv.at[3, q],
            peer(1),
        )

    def fold_in(sends, gets, send_sem, recv_sem):
        def fold(d, q, mask):
            return remote(
                sends.at[d, :, cols(q)],
                gets.at[d, :, cols(q)],
                send_sem.at[d, q],
                recv_sem.at[d, q],
                peer(mask),
            )

        return fold

    first_fold = fold_in(bsent, bgot, bsend, brecv)
    fold = fold_in(sent, got, rsend, rrecv)

    def projected(d, q):
        start = pl.ds(pl.multiple_of(flip(tp, d) * rows, rows), rows)
        return dot(mixes[0][start, :], ow[:, cols(q)]) + dot(mixes[1][start, :], on[:, cols(q)])

    def b1(q):
        for d in (3, 1):
            bsent[d, :, cols(q)] = projected(d, q).astype(bf16)
            first_fold(d, q, 1).start()

    def b2(q):
        total = projected(2, q)
        first_fold(3, q, 1).wait_recv()
        bsent[2, :, cols(q)] = (total + bgot[3, :, cols(q)].astype(f32)).astype(bf16)
        first_fold(2, q, 2).start()

    def b3(q):
        total = projected(0, q) + residual_ref[:, cols(q)].astype(f32)
        first_fold(1, q, 1).wait_recv()
        total = total + bgot[1, :, cols(q)].astype(f32)
        first_fold(2, q, 2).wait_recv()
        total = (total + bgot[2, :, cols(q)].astype(f32)).astype(bf16)
        stream[:, cols(q)] = total
        total = total.astype(f32)
        squares[...] += jnp.sum(total * total, axis=1, keepdims=True)
        scaled = (total * gain_ref[:, cols(q)]).astype(bf16)
        x_scr[:, cols(q)] = scaled

        @pl.when(z < n_sp - 1)
        def _():
            own_out(q, 1).start()

        @pl.when(z > 0)
        def _():
            own_out(q, -1).start()

        plane[:rows, cols(q)] = scaled

        @pl.when(q < chunks // 2)
        def _():
            down_out(2, 2 * q + group).wait_recv()
            down_across(2 * q + group).start()

    def staged(*stages):
        def one(q, carry):
            for lag, stage in enumerate(stages):
                if stage is None:
                    continue

                @pl.when((q >= lag) & (q < chunks + lag))
                def _():
                    stage(q - lag)

            return carry

        lax.fori_loop(0, chunks + len(stages) - 1, one, 0)

    hg[...] = jnp.zeros_like(hg)
    hu[...] = jnp.zeros_like(hu)
    shg[...] = jnp.zeros_like(shg)
    shu[...] = jnp.zeros_like(shu)
    som[...] = jnp.zeros_like(som)
    lanes = meta.shape[2]
    iota = lax.broadcasted_iota(jnp.int32, (cap, lanes), 0)

    def fact_wait(k):
        source = lax.rem(z + k // n_tp, n_sp) * n_tp + lax.rem(tp + lax.rem(k, n_tp), n_tp)
        remote(facts_ref, meta.at[source], msend.at[k], mrecv.at[source], peer(1)).wait_recv()

    others(fact_wait)

    def held(p, d):
        info = meta[p * n_tp + flip(tp, d)]
        slot = ((z * n_tp + tp) * cap + iota).astype(f32)
        return info, info[0:1, :] == slot, info[1:2, :] == slot

    for step in range(n_sp):
        p = lax.rem(z + step, n_sp)
        for d in range(n_tp):
            info = meta[p * n_tp + tp]
            slot = ((z * n_tp + flip(tp, d)) * cap + iota).astype(f32)
            hit = (info[0:1, :] == slot) | (info[1:2, :] == slot)
            smat[p, d * cap : (d + 1) * cap, :] = hit.astype(f32)[:, :rows].astype(bf16)
            info, first, second = held(p, d)
            weight = jnp.where(first, info[2:3, :], 0.0) + jnp.where(second, info[3:4, :], 0.0)
            wcol[p, d * cap : (d + 1) * cap, :] = jnp.sum(weight, axis=1, keepdims=True)
            if not step:
                hit = (first | second).astype(f32)[:, :rows].astype(bf16)
                som[d * cap : (d + 1) * cap, d * rows : (d + 1) * rows] = hit

    def piece(p, d, q):
        return p, pl.ds(d * cap, cap), cols(q)

    def spread_out(p, d, q):
        at = piece(p, d, q)
        return remote(gbuf.at[at], crow.at[at], gsend.at[p, d, q], grecv.at[p, d, q], peer(d))

    def c_unit(p, q, k=None, target=None):
        block_out(p, q, 0, peer(1)).wait_recv()
        if k is not None:
            block_out(p, q, k, target).start()
        picked = dot(smat[p], blk[p, :, cols(q)]).astype(bf16)
        gbuf[p, :, cols(q)] = picked
        crow[p, :cap, cols(q)] = picked[:cap]
        for d in (2, 3, 1):
            spread_out(p, d, q).start()

    def hidden(p, q):
        taken = crow[p, :, cols(q)]
        hg[p] += dot_nt(taken, eg[:, cols(q)])
        hu[p] += dot_nt(taken, eu[:, cols(q)])

    def h_unit(p, q):
        for d in (1, 2, 3):
            spread_out(p, d, q).wait_recv()
        hidden(p, q)

    def act_out(p, d):
        at = (p, pl.ds(d * cap, cap))
        return remote(aout.at[at], ain.at[at], asend.at[p, d], arecv.at[p, d], peer(d))

    def factor_of(p, d):
        source = p * n_tp + flip(tp, d)

        @pl.when(source != me)
        def _():
            remote(
                factor_out, factors.at[source], fsend.at[0], frecv_f.at[source], peer(1)
            ).wait_recv()

        return factors[source][0:1, :]

    def silu(gate):
        return gate / (1.0 + jnp.exp(-gate))

    def activate(p, values=None):
        for d in range(n_tp):
            at = pl.ds(d * cap, cap)
            value = factor_of(p, d) if values is None else values[d]
            _, first, second = held(p, d)
            scale = jnp.sum(jnp.where(first | second, value, 0.0), axis=1, keepdims=True)
            made = silu(hg[p, at, :] * scale) * (hu[p, at, :] * scale) * wcol[p, at, :]
            made = made.astype(bf16)
            if d:
                aout[p, at, :] = made
                act_out(p, d).start()
            else:
                ain[p, at, :] = made

    def mix_in(p):
        for d in range(n_tp):
            if d:
                act_out(p, d).wait_recv()
            at = pl.ds(d * cap, cap)
            spread_act[p, d] = dot_tn(smat[p, at, :], ain[p, at, :]).astype(bf16)

    def own_spread(q):
        gather_out(2, q).start()
        gather_out(1, q).start()

    def own_relay(q):
        gather_out(2, q).wait_recv()
        gather_on(q).start()

    def own_unit(q):
        gather_out(1, q).wait_recv()
        gather_on(q).wait_recv()
        full = plane[:, cols(q)]
        crow[z, :, cols(q)] = dot(som[...], full).astype(bf16)
        shg[...] += dot(full, sg[cols(q), :])
        shu[...] += dot(full, su[cols(q), :])
        hidden(z, q)

    def own_activate():
        values = [factor_of(z, d) for d in range(n_tp)]
        activate(z, values)
        i, j = grid((rows, lanes))
        for d in range(n_tp):
            at = pl.ds(d * rows, rows)
            scale = jnp.sum(jnp.where(i == j, values[d], 0.0), axis=1, keepdims=True)
            sact[at, :] = (silu(shg[at, :] * scale) * (shu[at, :] * scale)).astype(bf16)

    def outcome(p, q):
        total = dot(spread_act[p, 0], ed[0, :, cols(q)])
        for d in range(1, n_tp):
            total = total + dot(spread_act[p, d], ed[d, :, cols(q)])
        return total

    def down_relay(q):
        @pl.when(lax.rem(q, 2) != group)
        def _():
            down_out(2, q).wait_recv()

        down_on(q).start()

    def down_ready(q):
        down_out(1, q).wait_recv()
        down_on(q).wait_recv()

    def chain_out(p, q, last, step):
        into, sem = chin.at[p, :, cols(q)], drecv.at[p, q]
        if last:
            side = (1 - step) // 2
            into, sem = fin.at[side, :, cols(q)], frecv.at[side, q]
        return remote(chs.at[p, :, cols(q)], into, dsend.at[p, q], sem, {"sp": z + step})

    def d_unit(p, q, incoming, last, step):
        total = outcome(p, q)
        if incoming:
            chain_out(p, q, False, step).wait_recv()
            total = total + chin[p, :, cols(q)].astype(f32)
        chs[p, :, cols(q)] = total.astype(bf16)
        chain_out(p, q, last, step).start()

    def product(d, q):
        return dot(sact[d * rows : (d + 1) * rows, :], sd[:, cols(q)])

    def rs1(q):
        for d in (3, 1):
            sent[d, :, cols(q)] = product(d, q).astype(bf16)
            fold(d, q, 1).start()

    def rs2(q):
        total = product(2, q)
        fold(3, q, 1).wait_recv()
        sent[2, :, cols(q)] = (total + got[3, :, cols(q)].astype(f32)).astype(bf16)
        fold(2, q, 2).start()

    def base(q):
        total = product(0, q) + outcome(z, q) + stream[:, cols(q)].astype(f32)
        fold(1, q, 1).wait_recv()
        total = total + got[1, :, cols(q)].astype(f32)
        fold(2, q, 2).wait_recv()
        facc[:, cols(q)] = total + got[2, :, cols(q)].astype(f32)

    def arrive(side, q):
        at = fin.at[side, :, cols(q)]
        remote(at, at, dsend.at[0, q], frecv.at[side, q], peer(1)).wait_recv()
        return fin[side, :, cols(q)].astype(f32)

    def run(*steps):
        def each(q):
            for step in steps:
                step(q)

        return each

    def at_first(step):
        def each(q):
            @pl.when(q == 0)
            def _():
                step()

        return each

    def sends_done(copies):
        def one(q, carry):
            for copy in copies(q):
                copy.wait_send()
            return carry

        lax.fori_loop(0, chunks, one, 0)

    loads[0].wait()
    loads[1].wait()
    squares[...] = jnp.zeros_like(squares)
    is_end = (z == 0) | (z == n_sp - 1)
    ahead, behind = {"sp": z + way}, {"sp": z - way}

    def c_first(q):
        @pl.when(is_end)
        def _():
            c_unit(z + way, q)

        @pl.when(jnp.logical_not(is_end))
        def _():
            c_unit(z - way, q, 2, ahead)
            c_unit(z + way, q, 3, behind)

    def h_first(q):
        @pl.when(is_end)
        def _():
            h_unit(z + way, q)

        @pl.when(jnp.logical_not(is_end))
        def _():
            h_unit(z - way, q)
            h_unit(z + way, q)

    for k in (5, 6):
        loads[k].wait()
    staged(b1, b2, b3, None, c_first, None, h_first)
    factor = lax.rsqrt(squares[...] * (1.0 / width) + EPS)
    i, j = grid((rows, factor_out.shape[1]))
    factor = jnp.sum(jnp.where(i == j, factor, 0.0), axis=0, keepdims=True)
    factor_out[...] = jnp.broadcast_to(factor, factor_out.shape)
    others(lambda k: factor_send(k).start())
    factors[me] = factor_out[...]

    for k in (2, 3, 4):
        loads[k].wait()

    @pl.when(is_end)
    def _():
        p0, p1, p2 = z + way, z + 2 * way, z + 3 * way
        activate(p0)
        staged(
            run(lambda q: c_unit(p1, q), down_relay),
            None,
            run(
                lambda q: h_unit(p1, q),
                at_first(lambda: mix_in(p0)),
                down_ready,
                lambda q: d_unit(p0, q, False, True, way),
            ),
        )
        activate(p1)
        staged(
            lambda q: c_unit(p2, q),
            None,
            run(
                lambda q: h_unit(p2, q),
                at_first(lambda: mix_in(p1)),
                lambda q: d_unit(p1, q, False, False, way),
            ),
        )
        activate(p2)
        staged(own_spread)
        mix_in(p2)
        staged(lambda q: d_unit(p2, q, False, False, way))
        staged(own_relay, own_unit)
        own_activate()
        staged(rs1, rs2)
        mix_in(z)
        staged(base)

        def last(q):
            out_ref[:, cols(q)] = (facc[:, cols(q)] + arrive((1 + way) // 2, q)).astype(bf16)

        staged(last)
        sends_done(
            lambda q: [own_out(q, way)]
            + [spread_out(p, d, q) for p in (p0, p1, p2) for d in (1, 2, 3)]
            + [chain_out(p, q, False, way) for p in (p0, p1, p2)]
        )

    @pl.when(jnp.logical_not(is_end))
    def _():
        s0, s1, s2 = z - way, z + way, z + 2 * way
        activate(s0)
        activate(s1)
        staged(
            run(lambda q: c_unit(s2, q, 4, behind), down_relay),
            None,
            run(lambda q: h_unit(s2, q), down_ready),
        )
        activate(s2)
        staged(own_spread)
        mix_in(s1)
        mix_in(s0)
        mix_in(s2)
        staged(run(own_relay, lambda q: d_unit(s1, q, True, True, way)), own_unit)
        own_activate()
        staged(
            run(lambda q: d_unit(s2, q, True, False, way), rs1),
            rs2,
            lambda q: d_unit(s0, q, True, True, -way),
        )
        mix_in(z)
        staged(base)

        def last(q):
            total = facc[:, cols(q)] + arrive(0, q) + arrive(1, q)
            out_ref[:, cols(q)] = total.astype(bf16)

        staged(last)
        sends_done(
            lambda q: [own_out(q, way), own_out(q, -way)]
            + [block_out(s0, q, 2, ahead), block_out(s1, q, 3, behind)]
            + [block_out(s2, q, 4, behind)]
            + [spread_out(p, d, q) for p in (s0, s1, s2) for d in (1, 2, 3)]
            + [chain_out(p, q, False, way) for p in (s0, s1, s2)]
        )

    sends_done(
        lambda q: [gather_out(2, q), gather_out(1, q), gather_on(q)]
        + [down_out(1, q), down_on(q)]
        + [f(d, q, 1) for f in (fold, first_fold) for d in (3, 1, 2)]
    )
    for i in range(chunks // 2):
        down_out(2, 2 * i + group).wait_send()
        down_across(2 * i + group).wait_send()
    for p in range(n_sp):
        for d in range(1, n_tp):
            act_out(p, d).wait_send()

    def finish(k):
        fact_out(k).wait_send()
        factor_send(k).wait_send()

    others(finish)

    def latents_done(block, carry):
        @pl.when(z < n_sp - 1)
        def _():
            for k in range(pieces):
                latent_out(block, k).wait_send()

        @pl.when(block < z)
        def _():
            for k in range(pieces):
                latent_over(block, k).wait_send()

        return carry

    lax.fori_loop(0, z + 1, latents_done, 0)


def rotary_tables(tokens, lanes):
    half = ROPE // 2
    lane = np.arange(lanes) % half
    inverse = np.float32(ROPE_BASE) ** (-lane.astype(np.float32) * np.float32(2.0 / ROPE))
    angles = np.arange(tokens, dtype=np.float32)[:, None] * inverse.astype(np.float32)[None, :]
    return jnp.asarray(np.cos(angles)), jnp.asarray(np.sin(angles))


def layer(near, far, n_sp, n_tp, cap, sizes, chunks=4):
    groups = len(sizes)
    tok, latent_width = near[0].shape
    key_ws, value_ws = (near[3 + k * groups : 3 + (k + 1) * groups] for k in (1, 2))
    residual = near[-1]
    lanes = ROPE + -ROPE % 128
    tables = rotary_tables(n_sp * tok, lanes)
    rows, width = residual.shape
    ow, on, sg, su, sd, eg, eu, ed = far
    slots = n_tp * cap
    hidden, share = eg.shape[0], sg.shape[1]
    bf16, f32 = jnp.bfloat16, jnp.float32
    count = n_sp * n_tp

    def sems(*shape):
        return pltpu.SemaphoreType.DMA(shape)

    def half(*shape):
        return pltpu.VMEM(shape, bf16)

    def full(*shape):
        return pltpu.VMEM(shape, f32)

    depth = sum(w.shape[1] for w in value_ws)
    number = sum(w.shape[1] // size for w, size in zip(value_ws, sizes))
    fact_shape = (8, rows + -rows % 128)
    scratch = [half(number, tok, 2 * lanes), full(-(-number // 8) * 8, tok)]
    scratch += [full(-(-number // 8) * 8, tok), full(depth, tok), half(depth, latent_width)]
    scratch += [full(tok, lanes), full(tok, lanes), full(*fact_shape)]
    scratch += [half(n_sp * tok, latent_width + lanes)]
    scratch += [half(tok, w.shape[1]) for w in value_ws]
    scratch += [full(count, *fact_shape), full(count, *fact_shape), full(*fact_shape)]
    scratch += [half(rows, width), half(rows, width)]
    scratch += [half(n_sp, rows, width), half(n_tp * rows, width)]
    scratch += [half(n_sp, slots, width)] * 2
    scratch += [half(n_sp, rows, width)] * 2 + [half(2, rows, width)]
    scratch += [half(n_tp, rows, width)] * 4
    scratch += [half(*w.shape) for w in far[:-1]] + [half(n_tp, *ed.shape)]
    scratch += [half(n_sp, slots, rows), half(slots, n_tp * rows), full(n_sp, slots, 1)]
    scratch += [full(n_sp, slots, hidden)] * 2
    scratch += [half(n_sp, slots, hidden)] * 2
    scratch += [half(n_sp, n_tp, rows, hidden)]
    scratch += [full(n_tp * rows, share)] * 2 + [half(n_tp * rows, share)]
    scratch += [full(rows, width), full(rows, 1)]
    scratch += [sems(10)] + [sems(n_sp, 2)] * 4
    scratch += [sems(count)] * 4
    scratch += [sems(n_tp, chunks)] * 2
    scratch += [sems(5, chunks), sems(n_sp, chunks)]
    scratch += [sems(n_sp, n_tp, chunks)] * 2
    scratch += [sems(n_sp, n_tp)] * 2
    scratch += [sems(n_sp, chunks), sems(n_sp, chunks), sems(2, chunks)]
    scratch += [sems(n_tp, chunks)] * 6 + [sems(chunks)]
    return pl.pallas_call(
        lambda *refs: layer_kernel(chunks, cap, sizes, *refs),
        out_shape=jax.ShapeDtypeStruct((rows, width), bf16),
        in_specs=[VMEM] * len(near) + [pl.BlockSpec(memory_space=pl.ANY)] * (len(far) + 2),
        out_specs=VMEM,
        scratch_shapes=scratch,
        compiler_params=pltpu.CompilerParams(
            collective_id=4, has_side_effects=True, vmem_limit_bytes=60 << 20
        ),
    )(*near, *far, *tables)


def rms_scale(values, gain):
    return values * lax.rsqrt(jnp.mean(values * values, axis=-1, keepdims=True) + EPS) * gain


def body(
    latent,
    rope_key,
    wide_query,
    narrow_query,
    wide_key_weight,
    wide_value_weight,
    narrow_key_weight,
    narrow_value_weight,
    latent_norm_scale,
    out_wide,
    out_narrow,
    residual,
    ffn_gain,
    shared_gate,
    shared_up,
    shared_down,
    expert_gate,
    expert_up,
    expert_down,
    routes,
    route_weights,
):
    tok_dev = latent.shape[0]
    seq_index = lax.axis_index("sp")
    own_pos = seq_index * tok_dev + jnp.arange(tok_dev, dtype=jnp.int32)
    n_sp, n_tp = lax.axis_size("sp"), lax.axis_size("tp")
    rows_here, top_count = routes.shape
    local_experts = expert_gate.shape[0]
    experts_all = local_experts * lax.axis_size(("sp", "tp"))
    capacity = max(2, 2 * top_count * rows_here // experts_all)
    queries = (wide_query, narrow_query)
    key_ws = (wide_key_weight, narrow_key_weight)
    value_ws = (wide_value_weight, narrow_value_weight)
    sizes = (WIDE_HEAD_SIZE, NARROW_HEAD_SIZE)
    planes = n_sp == 4 and n_tp == 4 and local_experts == 1 and capacity % 16 == 0
    if planes and top_count == 2 and rows_here <= 128 and lax.axis_size("grp") == 2:
        near = (latent, rope_key.T, latent_norm_scale[None, :], *queries, *key_ws, *value_ws)
        near += (routes.T, route_weights.T, ffn_gain[None, :], residual)
        far = (out_wide, out_narrow, shared_gate, shared_up, shared_down)
        far += (expert_gate[0].T, expert_up[0].T, expert_down[0])
        return layer(near, far, n_sp, n_tp, capacity, sizes)
    normed_latent = rms_scale(latent.astype(jnp.float32), latent_norm_scale).astype(jnp.bfloat16)
    half = ROPE // 2
    lane = jnp.arange(ROPE + -ROPE % 128, dtype=jnp.int32)
    inverse = ROPE_BASE ** (-(lane % half).astype(jnp.float32) * 2.0 / ROPE)
    angles = own_pos.astype(jnp.float32)[:, None] * inverse[None, :]
    cosine, sine = jnp.cos(angles), jnp.sin(angles)
    row = jnp.arange(ROPE, dtype=jnp.int32)[:, None]
    same = (row == lane[None, :]).astype(jnp.bfloat16)
    cross = (row == lane[None, :] - half).astype(jnp.bfloat16) * (lane < ROPE)[None, :] - (
        (row == lane[None, :] + half) & (lane < half)[None, :]
    ).astype(jnp.bfloat16)
    turned_key = (
        jnp.dot(rope_key, same, preferred_element_type=jnp.float32) * cosine
        + jnp.dot(rope_key, cross.astype(jnp.bfloat16), preferred_element_type=jnp.float32) * sine
    ).astype(jnp.bfloat16)
    flat_routes = routes.reshape(-1)
    assigned = flat_routes.shape[0]
    choose = (flat_routes[:, None] == jnp.arange(experts_all, dtype=jnp.int32)[None, :]).astype(
        jnp.float32
    )
    lower_mask = (jnp.arange(assigned)[:, None] > jnp.arange(assigned)[None, :]).astype(jnp.float32)
    earlier = jnp.dot(lower_mask, choose, precision=lax.Precision.HIGHEST)
    slots = jnp.sum(earlier * choose, axis=1).astype(jnp.int32)
    target = flat_routes * capacity + slots
    by_choice = target.reshape(rows_here, top_count)
    rows_packed = jnp.concatenate([normed_latent, turned_key], axis=1)
    packed = spread(rows_packed, n_sp, n_tp)
    wide_mix, narrow_mix = attend(packed, cosine, sine, queries, key_ws, value_ws, sizes)
    (projected,) = dot_scatter((wide_mix, narrow_mix), (out_wide, out_narrow), n_tp, 2)
    stream = (residual.astype(jnp.float32) + projected).astype(jnp.bfloat16)
    normed = rms_scale(stream.astype(jnp.float32), ffn_gain).astype(jnp.bfloat16)
    model_width = normed.shape[1]
    send_map = jnp.any(
        target.reshape(rows_here, top_count)[None, :, :]
        == jnp.arange(experts_all * capacity, dtype=jnp.int32)[:, None, None],
        axis=2,
    ).astype(jnp.bfloat16)
    outgoing = jnp.dot(send_map, normed, preferred_element_type=jnp.float32).astype(jnp.bfloat16)
    devices = n_sp * n_tp
    outgoing = outgoing.reshape(devices, local_experts * capacity, model_width)
    piece, incoming = gather_rows(normed, outgoing, n_tp)
    sources = devices
    incoming = incoming.reshape(experts_all, capacity, model_width)
    grouped = incoming.reshape(sources, local_experts, incoming.shape[1], model_width)
    gate_part = jnp.einsum(
        "sxcd,xdf->sxcf", grouped, expert_gate, preferred_element_type=jnp.float32
    )
    up_part = jnp.einsum("sxcd,xdf->sxcf", grouped, expert_up, preferred_element_type=jnp.float32)
    active = (jax.nn.silu(gate_part) * up_part).astype(jnp.bfloat16)
    finished = jnp.einsum(
        "sxcf,xfd->sxcd", active, expert_down, preferred_element_type=jnp.float32
    ).astype(jnp.bfloat16)
    gate_part = jnp.dot(piece, shared_gate, preferred_element_type=jnp.float32)
    up_part = jnp.dot(piece, shared_up, preferred_element_type=jnp.float32)
    active = (jax.nn.silu(gate_part) * up_part).astype(jnp.bfloat16)
    shared, returned = dot_scatter(
        (active,), (shared_down,), n_tp, 3, finished.reshape(outgoing.shape)
    )
    slot_rows = returned.reshape(experts_all * capacity, model_width)
    routed = jnp.zeros((rows_here, model_width), jnp.float32)
    for choice in range(top_count):
        hot = by_choice[:, choice : choice + 1] == jnp.arange(experts_all * capacity)[None, :]
        picked = jnp.dot(
            hot.astype(jnp.bfloat16), slot_rows, preferred_element_type=jnp.float32
        )
        routed = routed + picked * route_weights[:, choice : choice + 1]
    return (stream.astype(jnp.float32) + shared + routed).astype(jnp.bfloat16)


def solution(mesh):
    placed = (
        P(("grp", "sp"), None),
        P(("grp", "sp"), None),
        P(("grp", "sp"), "tp"),
        P(("grp", "sp"), "tp"),
        P(None, "tp"),
        P(None, "tp"),
        P(None, "tp"),
        P(None, "tp"),
        P(),
        P("tp", None),
        P("tp", None),
        P(("grp", "sp", "tp"), None),
        P(),
        P(None, "tp"),
        P(None, "tp"),
        P("tp", None),
        P(("sp", "tp"), None, None),
        P(("sp", "tp"), None, None),
        P(("sp", "tp"), None, None),
        P(("grp", "sp", "tp"), None),
        P(("grp", "sp", "tp"), None),
    )
    return jax.shard_map(
        body, mesh=mesh, in_specs=placed, out_specs=P(("grp", "sp", "tp"), None), check_vma=False
    )
```

```python
import jax
import jax.numpy as jnp
import numpy as np
from jax import lax
from jax.experimental import pallas as pl
from jax.experimental.pallas import tpu as pltpu
from jax.sharding import PartitionSpec as P

ROPE = 64
WIDE_HEAD_SIZE = 128
NARROW_HEAD_SIZE = 64
EPS = 1e-06
ROPE_BASE = 10000.0
NEG_FILL = -1e30


MESH = pl.DeviceIdType.MESH
VMEM = pl.BlockSpec(memory_space=pltpu.VMEM)


def flip(index, bits):
    mask = 1
    while mask <= bits:
        if bits & mask:
            index = index + mask - 2 * mask * ((index // mask) % 2)
        mask *= 2
    return index


def masks_of(count):
    return [1 << k for k in range(count.bit_length() - 1)]


def low_bit(number):
    return number & -number


def greet(partners):
    barrier = pltpu.get_barrier_semaphore()
    for partner in partners:
        pl.semaphore_signal(barrier, inc=1, device_id=partner, device_id_type=MESH)
    pl.semaphore_wait(barrier, len(partners))


def doubling_order(count):
    return sorted(range(count), key=lambda d: (bin(d).count("1"), -d))


def remote(src, dst, send_sem, recv_sem, target):
    return pltpu.make_async_remote_copy(
        src_ref=src,
        dst_ref=dst,
        send_sem=send_sem,
        recv_sem=recv_sem,
        device_id=target,
        device_id_type=MESH,
    )


def spread_kernel(n_sp, n_tp, x_ref, out_ref, z_send, z_recv, t_send, t_recv, own_sem):
    sp, tp = lax.axis_index("sp"), lax.axis_index("tp")
    tok = x_ref.shape[0]
    part = tok // n_tp
    targets = [{"sp": lax.rem(sp + r, n_sp)} for r in range(1, n_sp)]
    greet(targets + [{"tp": flip(tp, m)} for m in masks_of(n_tp)])

    def rows(block, member):
        return pl.ds(pl.multiple_of(block * tok + member * part, part), part)

    own = pltpu.make_async_copy(
        x_ref, out_ref.at[pl.ds(pl.multiple_of(sp * tok, tok), tok)], own_sem
    )
    sends = []
    for r in range(1, n_sp):
        copy = remote(
            x_ref.at[pl.ds(pl.multiple_of(tp * part, part), part)],
            out_ref.at[rows(sp, tp)],
            z_send.at[r],
            z_recv.at[r],
            targets[r - 1],
        )
        copy.start()
        sends.append(copy)
    own.start()

    def piece(r, d):
        return out_ref.at[rows(lax.rem(sp + n_sp - r, n_sp), flip(tp, d))]

    for d in doubling_order(n_tp):
        for r in range(1, n_sp):
            block = piece(r, d)
            if d == 0:
                sends[r - 1].wait_recv()
            else:
                remote(
                    block, block, t_send.at[r, d], t_recv.at[r, d], {"tp": flip(tp, low_bit(d))}
                ).wait_recv()
            for mask in reversed(masks_of(low_bit(d) if d else n_tp)):
                copy = remote(
                    block,
                    block,
                    t_send.at[r, d + mask],
                    t_recv.at[r, d + mask],
                    {"tp": flip(tp, mask)},
                )
                copy.start()
                sends.append(copy)
    for copy in sends:
        copy.wait_send()
    own.wait()


def spread(x, n_sp, n_tp):
    tok, width = x.shape
    return pl.pallas_call(
        lambda *refs: spread_kernel(n_sp, n_tp, *refs),
        out_shape=jax.ShapeDtypeStruct((n_sp * tok, width), x.dtype),
        in_specs=[VMEM],
        out_specs=VMEM,
        scratch_shapes=[
            pltpu.SemaphoreType.DMA((n_sp,)),
            pltpu.SemaphoreType.DMA((n_sp,)),
            pltpu.SemaphoreType.DMA((n_sp, n_tp)),
            pltpu.SemaphoreType.DMA((n_sp, n_tp)),
            pltpu.SemaphoreType.DMA,
        ],
        compiler_params=pltpu.CompilerParams(collective_id=0, has_side_effects=True),
        cost_estimate=pl.CostEstimate(flops=0, bytes_accessed=30_000_000, transcendentals=0),
    )(x)


def gather_kernel(
    n_tp, pieces, x_ref, blocks_ref, out_ref, moved_ref, send, recv, own_sem, *semaphores
):
    exchange = Exchange(blocks_ref, moved_ref, *semaphores)
    tp = lax.axis_index("tp")
    rows, width = x_ref.shape
    part = width // pieces
    exchange.greet()

    def block(d, c):
        start = pl.multiple_of(flip(tp, d) * rows, rows)
        return out_ref.at[pl.ds(start, rows), pl.ds(c * part, part)]

    own = pltpu.make_async_copy(
        x_ref, out_ref.at[pl.ds(pl.multiple_of(tp * rows, rows), rows)], own_sem
    )
    sends = []
    for d in doubling_order(n_tp):
        for c in range(pieces):
            source = x_ref.at[:, pl.ds(c * part, part)] if d == 0 else block(d, c)
            if d:
                remote(
                    source, source, send.at[d, c], recv.at[d, c], {"tp": flip(tp, low_bit(d))}
                ).wait_recv()
            for mask in reversed(masks_of(low_bit(d) if d else n_tp)):
                copy = remote(
                    source,
                    block(d, c),
                    send.at[d + mask, c],
                    recv.at[d + mask, c],
                    {"tp": flip(tp, mask)},
                )
                copy.start()
                sends.append(copy)
        if d == 0:
            exchange.start()
            own.start()
    for copy in sends:
        copy.wait_send()
    own.wait()
    exchange.finish()


def gather_rows(x, blocks, n_tp, pieces=2):
    rows, width = x.shape
    return pl.pallas_call(
        lambda *refs: gather_kernel(n_tp, pieces, *refs),
        out_shape=[
            jax.ShapeDtypeStruct((n_tp * rows, width), x.dtype),
            jax.ShapeDtypeStruct(blocks.shape, blocks.dtype),
        ],
        in_specs=[VMEM] * 2,
        out_specs=[VMEM] * 2,
        scratch_shapes=[
            pltpu.SemaphoreType.DMA((n_tp, pieces)),
            pltpu.SemaphoreType.DMA((n_tp, pieces)),
            pltpu.SemaphoreType.DMA,
        ]
        + exchange_semaphores(blocks.shape[0]),
        compiler_params=pltpu.CompilerParams(collective_id=1, has_side_effects=True),
        cost_estimate=pl.CostEstimate(flops=0, bytes_accessed=40_000_000, transcendentals=0),
    )(x, blocks)


def scatter_kernel(n_tp, pieces, pairs, moving, *refs):
    lefts, rights = refs[:pairs], refs[pairs : 2 * pairs]
    refs = refs[2 * pairs :]
    exchange = None
    if moving:
        blocks_ref, out_ref, moved_ref, sent, got, send, recv = refs[:7]
        exchange = Exchange(blocks_ref, moved_ref, *refs[7:])
    else:
        out_ref, sent, got, send, recv = refs
    tp = lax.axis_index("tp")
    rows, width = out_ref.shape
    part = width // pieces
    if moving:
        exchange.greet()
        exchange.start()
    else:
        greet([{"tp": flip(tp, m)} for m in masks_of(n_tp)])
    copies = {}

    def product(d, c):
        start = pl.multiple_of(flip(tp, d) * rows, rows)
        total = None
        for left, right in zip(lefts, rights):
            term = jnp.dot(
                left[pl.ds(start, rows), :],
                right[:, pl.ds(c * part, part)],
                preferred_element_type=jnp.float32,
            )
            total = term if total is None else total + term
        return total

    def summed(d, c, below):
        total = product(d, c)
        if below > 1:
            total = total.astype(jnp.bfloat16).astype(jnp.float32)
        for mask in masks_of(below):
            copies[d + mask, c].wait_recv()
            total = total + got[d + mask, :, pl.ds(c * part, part)].astype(jnp.float32)
        return total

    def pass_on(mask, c):
        for d in range(mask, n_tp, 2 * mask):
            sent[d, :, pl.ds(c * part, part)] = summed(d, c, mask).astype(jnp.bfloat16)
            copies[d, c] = remote(
                sent.at[d, :, pl.ds(c * part, part)],
                got.at[d, :, pl.ds(c * part, part)],
                send.at[d, c],
                recv.at[d, c],
                {"tp": flip(tp, mask)},
            )
            copies[d, c].start()

    masks = masks_of(n_tp)
    for step in range(pieces + len(masks) - 1):
        for stage, mask in enumerate(masks):
            if 0 <= step - stage < pieces:
                pass_on(mask, step - stage)
    for c in range(pieces):
        out_ref[:, pl.ds(c * part, part)] = summed(0, c, n_tp)
    for copy in copies.values():
        copy.wait_send()
    if moving:
        exchange.finish()


def dot_scatter(lefts, rights, n_tp, collective, blocks=None, pieces=4):
    rows, width = lefts[0].shape[0] // n_tp, rights[0].shape[1]
    pairs, moving = len(lefts), blocks is not None
    shapes = [jax.ShapeDtypeStruct((rows, width), jnp.float32)]
    operands = (*lefts, *rights)
    scratch = [
        pltpu.VMEM((n_tp, rows, width), jnp.bfloat16),
        pltpu.VMEM((n_tp, rows, width), jnp.bfloat16),
        pltpu.SemaphoreType.DMA((n_tp, pieces)),
        pltpu.SemaphoreType.DMA((n_tp, pieces)),
    ]
    if moving:
        shapes.append(jax.ShapeDtypeStruct(blocks.shape, blocks.dtype))
        operands += (blocks,)
        scratch += exchange_semaphores(blocks.shape[0])
    return pl.pallas_call(
        lambda *refs: scatter_kernel(n_tp, pieces, pairs, moving, *refs),
        out_shape=shapes,
        in_specs=[VMEM] * len(operands),
        out_specs=[VMEM] * len(shapes),
        scratch_shapes=scratch,
        compiler_params=pltpu.CompilerParams(collective_id=collective, has_side_effects=True),
        cost_estimate=pl.CostEstimate(flops=0, bytes_accessed=40_000_000, transcendentals=0),
    )(*operands)


def grid(shape):
    return lax.broadcasted_iota(jnp.int32, shape, 0), lax.broadcasted_iota(jnp.int32, shape, 1)


def attend_start(sizes, cosine, sine, queries, widths, scratch):
    half = ROPE // 2
    lanes = cosine.shape[1]
    for g, size in enumerate(sizes):
        plain, turned, peak, total, mixed = scratch[5 * g : 5 * g + 5]
        query = queries[g][...]
        width = query.shape[1]
        for h in range(plain.shape[0]):
            i, j = grid((width, widths[g]))
            select = (i == j + h * ROPE) & (j >= h * size) & (j < (h + 1) * size)
            plain[h] = jnp.dot(
                query, select.astype(jnp.bfloat16), preferred_element_type=jnp.float32
            ).astype(jnp.bfloat16)
            i, j = grid((width, lanes))
            base = h * (size + ROPE) + size
            same = ((i == j + base) & (j < ROPE)).astype(jnp.float32)
            upper = ((i == j + base + half) & (j < half)).astype(jnp.float32)
            lower = ((i == j + base - half) & (j >= half) & (j < ROPE)).astype(jnp.float32)
            straight = jnp.dot(
                query, same.astype(jnp.bfloat16), preferred_element_type=jnp.float32
            )
            crossed = jnp.dot(
                query, (lower - upper).astype(jnp.bfloat16), preferred_element_type=jnp.float32
            )
            turned[h] = (straight * cosine[...] + crossed * sine[...]).astype(jnp.bfloat16)
        peak[...] = jnp.full_like(peak, NEG_FILL)
        total[...] = jnp.zeros_like(total)
        mixed[...] = jnp.zeros_like(mixed)


def attend_block(sizes, packed, index, sp, key_ws, value_ws, scratch):
    latent_width = key_ws[0].shape[0]
    tok = scratch[0].shape[1]
    start = pl.ds(pl.multiple_of(index * tok, tok), tok)
    latent = packed[start, :latent_width]
    turned_rows = packed[start, latent_width:]
    i, j = grid((tok, tok))
    visible = index * tok + j <= sp * tok + i
    across = (((1,), (1,)), ((), ()))
    for g, size in enumerate(sizes):
        plain, turned, peak, total, mixed = scratch[5 * g : 5 * g + 5]
        factor = (size + ROPE) ** (-0.5)
        keys = jnp.dot(latent, key_ws[g][...], preferred_element_type=jnp.float32)
        keys = keys.astype(jnp.bfloat16)
        values = jnp.dot(latent, value_ws[g][...], preferred_element_type=jnp.float32)
        values = values.astype(jnp.bfloat16)
        for h in range(plain.shape[0]):
            scores = lax.dot_general(
                plain[h], keys, across, preferred_element_type=jnp.float32
            ) + lax.dot_general(
                turned[h], turned_rows, across, preferred_element_type=jnp.float32
            )
            scores = jnp.where(visible, scores * factor, NEG_FILL)
            old = peak[h]
            new = jnp.maximum(old, jnp.max(scores, axis=1, keepdims=True))
            probs = jnp.where(visible, jnp.exp(scores - new), 0.0)
            fading = jnp.exp(old - new)
            peak[h] = new
            total[h] = total[h] * fading + jnp.sum(probs, axis=1, keepdims=True)
            mixed[h] = mixed[h] * fading + jnp.dot(
                probs.astype(jnp.bfloat16), values, preferred_element_type=jnp.float32
            )


def attend_end(sizes, outs, scratch):
    for g, size in enumerate(sizes):
        plain, turned, peak, total, mixed = scratch[5 * g : 5 * g + 5]
        i, j = grid(outs[g].shape)
        result = jnp.zeros(outs[g].shape, jnp.float32)
        for h in range(plain.shape[0]):
            own = (j >= h * size) & (j < (h + 1) * size)
            result = jnp.where(own, mixed[h] / total[h], result)
        outs[g][...] = result.astype(jnp.bfloat16)


def attend_kernel(sizes, packed, cosine, sine, *refs):
    groups = len(sizes)
    queries, key_ws, value_ws = refs[:groups], refs[groups : 2 * groups], refs[2 * groups : 3 * groups]
    outs = refs[3 * groups : 4 * groups]
    scratch = refs[4 * groups :]
    sp = lax.axis_index("sp")
    attend_start(sizes, cosine, sine, queries, [w.shape[1] for w in key_ws], scratch)

    def one_block(index, carry):
        attend_block(sizes, packed, index, sp, key_ws, value_ws, scratch)
        return carry

    lax.fori_loop(0, sp + 1, one_block, 0)
    attend_end(sizes, outs, scratch)


def attend_scratch(tok, lanes, key_ws, value_ws, sizes):
    scratch = []
    for g, size in enumerate(sizes):
        heads = value_ws[g].shape[1] // size
        scratch += [
            pltpu.VMEM((heads, tok, key_ws[g].shape[1]), jnp.bfloat16),
            pltpu.VMEM((heads, tok, lanes), jnp.bfloat16),
            pltpu.VMEM((heads, tok, 1), jnp.float32),
            pltpu.VMEM((heads, tok, 1), jnp.float32),
            pltpu.VMEM((heads, tok, value_ws[g].shape[1]), jnp.float32),
        ]
    return scratch


def attend(packed, cosine, sine, queries, key_ws, value_ws, sizes):
    tok, lanes = cosine.shape
    scratch = attend_scratch(tok, lanes, key_ws, value_ws, sizes)
    return pl.pallas_call(
        lambda *refs: attend_kernel(sizes, *refs),
        out_shape=[jax.ShapeDtypeStruct((tok, w.shape[1]), jnp.bfloat16) for w in value_ws],
        in_specs=[VMEM] * (3 + 3 * len(sizes)),
        out_specs=[VMEM] * len(sizes),
        scratch_shapes=scratch,
    )(packed, cosine, sine, *queries, *key_ws, *value_ws)


class Exchange:
    def __init__(self, source, dest, send, recv, own_sem):
        self.refs = source, dest, send, recv
        self.sp, self.tp = lax.axis_index("sp"), lax.axis_index("tp")
        self.n_sp, self.n_tp = lax.axis_size("sp"), lax.axis_size("tp")
        self.count = self.n_sp * self.n_tp
        self.me = self.sp * self.n_tp + self.tp
        self.own = pltpu.make_async_copy(source.at[self.me], dest.at[self.me], own_sem)

    def target(self, k):
        return (
            lax.rem(self.sp + k // self.n_tp, self.n_sp),
            lax.rem(self.tp + lax.rem(k, self.n_tp), self.n_tp),
        )

    def greet(self):
        barrier = pltpu.get_barrier_semaphore()

        def one(k, carry):
            sp, tp = self.target(k)
            pl.semaphore_signal(
                barrier, inc=1, device_id={"sp": sp, "tp": tp}, device_id_type=MESH
            )
            return carry

        lax.fori_loop(1, self.count, one, 0)
        pl.semaphore_wait(barrier, self.count - 1)

    def copy(self, k):
        source, dest, send, recv = self.refs
        sp, tp = self.target(k)
        return remote(
            source.at[sp * self.n_tp + tp],
            dest.at[self.me],
            send.at[k],
            recv.at[k],
            {"sp": sp, "tp": tp},
        )

    def start(self):
        def one(k, carry):
            self.copy(self.count - k).start()
            return carry

        lax.fori_loop(1, self.count, one, 0)
        self.own.start()

    def finish(self):
        def one(k, carry):
            self.copy(k).wait()
            return carry

        lax.fori_loop(1, self.count, one, 0)
        self.own.wait()


def exchange_semaphores(count):
    return [
        pltpu.SemaphoreType.DMA((count,)),
        pltpu.SemaphoreType.DMA((count,)),
        pltpu.SemaphoreType.DMA,
    ]


def turn(straight, crossed, cosine, sine):
    return (straight * cosine + crossed * sine).astype(jnp.bfloat16)


def turn_picks(height, lanes, base):
    half = ROPE // 2
    i, j = grid((height, lanes))
    same = ((i == j + base) & (j < ROPE)).astype(jnp.float32)
    upper = ((i == j + base + half) & (j < half)).astype(jnp.float32)
    lower = ((i == j + base - half) & (j >= half) & (j < ROPE)).astype(jnp.float32)
    return same.astype(jnp.bfloat16), (lower - upper).astype(jnp.bfloat16)


class Heads:
    def __init__(self, sizes, widths, refs):
        self.sizes, self.widths = sizes, widths
        self.joined, self.peak, self.total, self.mixed, self.turned_ws = refs
        self.list = []
        row = 0
        for g, size in enumerate(sizes):
            for h in range(widths[g] // size):
                self.list.append((g, h, size, row))
                row += size

    def start(self, queries, value_ws, cosine, sine):
        lanes = cosine.shape[1]
        cosine, sine = cosine[...], sine[...]
        for n, (g, h, size, row) in enumerate(self.list):
            query = queries[g][...]
            i, j = grid((query.shape[1], lanes))
            base = h * (size + ROPE)
            start = h * size % lanes
            select = (i == j - start + base) & (j >= start) & (j < start + size)
            self.joined[n, :, :lanes] = jnp.dot(
                query, select.astype(jnp.bfloat16), preferred_element_type=jnp.float32
            ).astype(jnp.bfloat16)
            same, cross = turn_picks(query.shape[1], lanes, base + size)
            straight = jnp.dot(query, same, preferred_element_type=jnp.float32)
            crossed = jnp.dot(query, cross, preferred_element_type=jnp.float32)
            self.joined[n, :, lanes:] = turn(straight, crossed, cosine, sine)
        row = 0
        for weight in value_ws:
            self.turned_ws[row : row + weight.shape[1], :] = weight[...].T
            row += weight.shape[1]
        self.peak[...] = jnp.full_like(self.peak, NEG_FILL)
        self.total[...] = jnp.zeros_like(self.total)
        self.mixed[...] = jnp.zeros_like(self.mixed)

    def block(self, latent, turned_rows, key_ws, diagonal):
        lanes = turned_rows.shape[1]
        across = (((1,), (1,)), ((), ()))
        bf16, f32 = jnp.bfloat16, jnp.float32
        keys = [jnp.dot(latent, w[...], preferred_element_type=f32).astype(bf16) for w in key_ws]
        values = lax.dot_general(
            self.turned_ws[...], latent, across, preferred_element_type=f32
        ).astype(bf16)
        for n, (g, h, size, row) in enumerate(self.list):
            scale = (size + ROPE) ** (-0.5) * 1.4426950408889634
            start = h * size // lanes * lanes
            joined = jnp.concatenate([keys[g][:, start : start + lanes], turned_rows], axis=1)
            scores = lax.dot_general(joined, self.joined[n], across, preferred_element_type=f32)
            if diagonal:
                i, j = grid(scores.shape)
                scores = jnp.where(i <= j, scores, NEG_FILL)
            old = self.peak[n : n + 1, :]
            new = jnp.maximum(old, jnp.max(scores, axis=0, keepdims=True))
            probs = jnp.exp2((scores - new) * scale)
            fading = jnp.exp2((old - new) * scale)
            self.peak[n : n + 1, :] = new
            self.total[n : n + 1, :] = self.total[n : n + 1, :] * fading + jnp.sum(
                probs, axis=0, keepdims=True
            )
            at = slice(row, row + size)
            self.mixed[at, :] = self.mixed[at, :] * fading + jnp.dot(
                values[at, :], probs.astype(bf16), preferred_element_type=f32
            )

    def end(self, outs):
        for n, (g, h, size, row) in enumerate(self.list):
            at = slice(row, row + size)
            self.mixed[at, :] = self.mixed[at, :] / self.total[n : n + 1, :]
        row = 0
        for out in outs:
            out[...] = self.mixed[row : row + out.shape[1], :].T.astype(jnp.bfloat16)
            row += out.shape[1]


def layer_kernel(chunks, cap, sizes, *refs):
    groups = len(sizes)
    latent_ref, rope_ref, latent_gain = refs[:3]
    queries, key_ws, value_ws = (refs[3 + k * groups : 3 + (k + 1) * groups] for k in range(3))
    refs = refs[3 + 3 * groups :]
    routes_ref, weights_ref, gain_ref, residual_ref = refs[:4]
    hbm, tables, out_ref, refs = refs[4:12], refs[12:14], refs[14], refs[15:]
    heads = Heads(sizes, [w.shape[1] for w in value_ws], refs[:5])
    cosine, sine, facts_ref, refs = refs[5], refs[6], refs[7], refs[8:]
    packed, mixes, refs = refs[0], refs[1 : 1 + groups], refs[1 + groups :]
    meta, factors, factor_out, stream, x_scr = refs[:5]
    blk, plane, gbuf, crow, chs, chin, fin = refs[5:12]
    bsent, bgot, sent, got = refs[12:16]
    local = refs[16:24]
    ow, on, sg, su, sd, eg, eu, ed = local
    smat, som, wcol, hg, hu, aout, ain, spread_act, shg, shu, sact, facc, squares = refs[24:37]
    refs = refs[37:]
    wsem, lsend, lrecv, psend_l, precv_l, msend, mrecv, fsend, frecv_f = refs[:9]
    psend, precv, csend, crecv, gsend, grecv, asend, arecv = refs[9:17]
    dsend, drecv, frecv, rsend, rrecv, bsend, brecv, esend, erecv, ysend = refs[17:27]
    z, tp = lax.axis_index("sp"), lax.axis_index("tp")
    group = lax.axis_index("grp")
    n_sp, n_tp = lax.axis_size("sp"), lax.axis_size("tp")
    count = n_sp * n_tp
    me = z * n_tp + tp
    rows, width = stream.shape
    tok = latent_ref.shape[0]
    latent_width = latent_ref.shape[1]
    part = width // chunks
    hidden_width = eg.shape[0]
    way = 1 - 2 * (z // 2)
    f32, bf16 = jnp.float32, jnp.bfloat16

    def cols(q):
        return pl.ds(pl.multiple_of(q * part, part), part)

    def peer(d):
        return {"tp": flip(tp, d)}

    def dot(a, b):
        return jnp.dot(a, b, preferred_element_type=f32)

    def dot_nt(a, b):
        return lax.dot_general(a, b, (((1,), (1,)), ((), ())), preferred_element_type=f32)

    def dot_tn(a, b):
        return lax.dot_general(a, b, (((0,), (0,)), ((), ())), preferred_element_type=f32)

    def other(k):
        return {
            "sp": lax.rem(z + k // n_tp, n_sp),
            "tp": lax.rem(tp + lax.rem(k, n_tp), n_tp),
        }

    def others(step):
        def one(k, carry):
            step(k)
            return carry

        lax.fori_loop(1, count, one, 0)

    barrier = pltpu.get_barrier_semaphore()
    others(
        lambda k: pl.semaphore_signal(barrier, inc=1, device_id=other(k), device_id_type=MESH)
    )
    pl.semaphore_signal(barrier, inc=1, device_id={"grp": 1 - group}, device_id_type=MESH)
    landing = [ed.at[0] if k == 7 else local[k] for k in range(8)]
    loads = [pltpu.make_async_copy(a, b, wsem.at[k]) for k, (a, b) in enumerate(zip(hbm, landing))]
    own_rows = pl.ds(pl.multiple_of(z * tok, tok), tok)
    tables = [
        pltpu.make_async_copy(a.at[own_rows], b, wsem.at[8 + k])
        for k, (a, b) in enumerate(zip(tables, (cosine, sine)))
    ]
    for table in tables:
        table.start()
    for k in (7, 0, 1, 5, 6, 2, 3, 4):
        loads[k].start()

    latent = latent_ref[...].astype(f32)
    latent = rms_scale(latent, latent_gain[...])
    packed[own_rows, :latent_width] = latent.astype(bf16)
    firsts = routes_ref[...].astype(f32)
    facts_ref[...] = jnp.full_like(facts_ref, -1.0)
    i, j = grid((rows, rows))
    named = [firsts[k : k + 1, :] for k in range(2)]
    columns = [
        jnp.sum(jnp.where(i == j, name, 0.0), axis=1, keepdims=True) for name in named
    ]
    for k in range(2):
        before = [((column == named[k]) & (i < j)).astype(f32) for column in columns]
        slot = jnp.sum(before[0] + before[1], axis=0, keepdims=True)
        facts_ref[k : k + 1, :rows] = named[k] * cap + slot
    facts_ref[2:4, :rows] = weights_ref[...]
    same, cross = turn_picks(rope_ref.shape[0], cosine.shape[1], 0)
    straight, crossed = dot_tn(rope_ref[...], same), dot_tn(rope_ref[...], cross)
    for table in tables:
        table.wait()
    packed[own_rows, latent_width:] = turn(straight, crossed, cosine[...], sine[...])
    pl.semaphore_wait(barrier, count)

    pieces = lsend.shape[1]
    size = tok // (2 * pieces)
    mine = lax.rem(tp, 2) * pieces

    def latent_rows(block, piece):
        return packed.at[pl.ds(pl.multiple_of(block * tok + piece * size, size), size)]

    def latent_out(block, k):
        into = latent_rows(block, mine + k)
        return remote(into, into, lsend.at[block, k], lrecv.at[block, k], {"sp": z + 1})

    def latent_over(block, k):
        at = latent_rows(block, mine + k)
        return remote(at, at, psend_l.at[block, k], precv_l.at[block, k], peer(1))

    def latent_here(block, k):
        at = latent_rows(block, pieces - mine + k)
        remote(at, at, psend_l.at[block, k], precv_l.at[block, k], peer(1)).wait_recv()

    @pl.when(z < n_sp - 1)
    def _():
        for k in range(pieces):
            latent_out(z, k).start()

    def fact_out(k):
        return remote(facts_ref, meta.at[me], msend.at[k], mrecv.at[me], other(k))

    def factor_send(k):
        return remote(factor_out, factors.at[me], fsend.at[k], frecv_f.at[me], other(k))

    others(lambda k: fact_out(k).start())
    meta[me] = facts_ref[...]

    def down_out(m, q):
        return remote(
            ed.at[0, :, cols(q)],
            ed.at[m, :, cols(q)],
            esend.at[m, q],
            erecv.at[m, q],
            peer(m),
        )

    def down_on(q):
        return remote(
            ed.at[2, :, cols(q)],
            ed.at[3, :, cols(q)],
            esend.at[3, q],
            erecv.at[3, q],
            peer(1),
        )

    def down_across(q):
        at = ed.at[2, :, cols(q)]
        return remote(at, at, ysend.at[q], erecv.at[2, q], {"grp": 1 - group})

    loads[7].wait()
    for i in range(chunks // 2):
        down_out(2, 2 * i + group).start()
    for q in range(chunks):
        down_out(1, q).start()

    heads.start(queries, value_ws, cosine, sine)

    def attend_rows(block, diagonal):
        at = pl.ds(pl.multiple_of(block * tok, tok), tok)
        heads.block(packed[at, :latent_width], packed[at, latent_width:], key_ws, diagonal)

    attend_rows(z, True)

    def earlier(k, carry):
        block = z - k
        for n in range(pieces):
            at = latent_rows(block, mine + n)
            remote(at, at, lsend.at[block, n], lrecv.at[block, n], peer(1)).wait_recv()

            @pl.when(z < n_sp - 1)
            def _():
                latent_out(block, n).start()

            latent_over(block, n).start()
        for n in range(pieces):
            latent_here(block, n)
        attend_rows(block, False)
        return carry

    lax.fori_loop(1, z + 1, earlier, 0)
    heads.end(mixes)

    def block_out(p, q, k, target, source=None):
        source = blk.at[p, :, cols(q)] if source is None else source
        return remote(source, blk.at[p, :, cols(q)], csend.at[k, q], crecv.at[p, q], target)

    def own_out(q, step):
        return block_out(z, q, (1 - step) // 2, {"sp": z + step}, x_scr.at[:, cols(q)])

    def gather_out(m, q):
        return remote(
            x_scr.at[:, cols(q)],
            plane.at[pl.ds(m * rows, rows), cols(q)],
            psend.at[m, q],
            precv.at[m, q],
            peer(m),
        )

    def gather_on(q):
        return remote(
            plane.at[pl.ds(2 * rows, rows), cols(q)],
            plane.at[pl.ds(3 * rows, rows), cols(q)],
            psend.at[3, q],
            precv.at[3, q],
            peer(1),
        )

    def fold_in(sends, gets, send_sem, recv_sem):
        def fold(d, q, mask):
            return remote(
                sends.at[d, :, cols(q)],
                gets.at[d, :, cols(q)],
                send_sem.at[d, q],
                recv_sem.at[d, q],
                peer(mask),
            )

        return fold

    first_fold = fold_in(bsent, bgot, bsend, brecv)
    fold = fold_in(sent, got, rsend, rrecv)

    def projected(d, q):
        start = pl.ds(pl.multiple_of(flip(tp, d) * rows, rows), rows)
        return dot(mixes[0][start, :], ow[:, cols(q)]) + dot(mixes[1][start, :], on[:, cols(q)])

    def b1(q):
        for d in (3, 1):
            bsent[d, :, cols(q)] = projected(d, q).astype(bf16)
            first_fold(d, q, 1).start()

    def b2(q):
        total = projected(2, q)
        first_fold(3, q, 1).wait_recv()
        bsent[2, :, cols(q)] = (total + bgot[3, :, cols(q)].astype(f32)).astype(bf16)
        first_fold(2, q, 2).start()

    def b3(q):
        total = projected(0, q) + residual_ref[:, cols(q)].astype(f32)
        first_fold(1, q, 1).wait_recv()
        total = total + bgot[1, :, cols(q)].astype(f32)
        first_fold(2, q, 2).wait_recv()
        total = (total + bgot[2, :, cols(q)].astype(f32)).astype(bf16)
        stream[:, cols(q)] = total
        total = total.astype(f32)
        squares[...] += jnp.sum(total * total, axis=1, keepdims=True)
        scaled = (total * gain_ref[:, cols(q)]).astype(bf16)
        x_scr[:, cols(q)] = scaled

        @pl.when(z < n_sp - 1)
        def _():
            own_out(q, 1).start()

        @pl.when(z > 0)
        def _():
            own_out(q, -1).start()

        plane[:rows, cols(q)] = scaled

        @pl.when(q == chunks - 1)
        def _():
            send_factor()

        @pl.when(q < chunks // 2)
        def _():
            down_out(2, 2 * q + group).wait_recv()
            down_across(2 * q + group).start()

    def send_factor():
        factor = lax.rsqrt(squares[...] * (1.0 / width) + EPS)
        i, j = grid((rows, factor_out.shape[1]))
        factor = jnp.sum(jnp.where(i == j, factor, 0.0), axis=0, keepdims=True)
        factor_out[...] = jnp.broadcast_to(factor, factor_out.shape)
        others(lambda k: factor_send(k).start())
        factors[me] = factor_out[...]

    def staged(*stages):
        def one(q, carry):
            for lag, stage in enumerate(stages):
                if stage is None:
                    continue

                @pl.when((q >= lag) & (q < chunks + lag))
                def _():
                    stage(q - lag)

            return carry

        lax.fori_loop(0, chunks + len(stages) - 1, one, 0)

    hg[...] = jnp.zeros_like(hg)
    hu[...] = jnp.zeros_like(hu)
    shg[...] = jnp.zeros_like(shg)
    shu[...] = jnp.zeros_like(shu)
    som[...] = jnp.zeros_like(som)
    lanes = meta.shape[2]
    iota = lax.broadcasted_iota(jnp.int32, (cap, lanes), 0)

    def fact_wait(k):
        source = lax.rem(z + k // n_tp, n_sp) * n_tp + lax.rem(tp + lax.rem(k, n_tp), n_tp)
        remote(facts_ref, meta.at[source], msend.at[k], mrecv.at[source], peer(1)).wait_recv()

    others(fact_wait)

    def held(p, d):
        info = meta[p * n_tp + flip(tp, d)]
        slot = ((z * n_tp + tp) * cap + iota).astype(f32)
        return info, info[0:1, :] == slot, info[1:2, :] == slot

    for step in range(n_sp):
        p = lax.rem(z + step, n_sp)
        for d in range(n_tp):
            info = meta[p * n_tp + tp]
            slot = ((z * n_tp + flip(tp, d)) * cap + iota).astype(f32)
            hit = (info[0:1, :] == slot) | (info[1:2, :] == slot)
            smat[p, d * cap : (d + 1) * cap, :] = hit.astype(f32)[:, :rows].astype(bf16)
            info, first, second = held(p, d)
            weight = jnp.where(first, info[2:3, :], 0.0) + jnp.where(second, info[3:4, :], 0.0)
            wcol[p, d * cap : (d + 1) * cap, :] = jnp.sum(weight, axis=1, keepdims=True)
            if not step:
                hit = (first | second).astype(f32)[:, :rows].astype(bf16)
                som[d * cap : (d + 1) * cap, d * rows : (d + 1) * rows] = hit

    def piece(p, d, q):
        return p, pl.ds(d * cap, cap), cols(q)

    def spread_out(p, d, q):
        at = piece(p, d, q)
        return remote(gbuf.at[at], crow.at[at], gsend.at[p, d, q], grecv.at[p, d, q], peer(d))

    def c_unit(p, q, k=None, target=None):
        block_out(p, q, 0, peer(1)).wait_recv()
        if k is not None:
            block_out(p, q, k, target).start()
        picked = dot(smat[p], blk[p, :, cols(q)]).astype(bf16)
        gbuf[p, :, cols(q)] = picked
        crow[p, :cap, cols(q)] = picked[:cap]
        for d in (2, 3, 1):
            spread_out(p, d, q).start()

    def hidden(p, q):
        taken = crow[p, :, cols(q)]
        hg[p] += dot_nt(taken, eg[:, cols(q)])
        hu[p] += dot_nt(taken, eu[:, cols(q)])

    def h_unit(p, q):
        for d in (1, 2, 3):
            spread_out(p, d, q).wait_recv()
        hidden(p, q)

    def act_out(p, d):
        at = (p, pl.ds(d * cap, cap))
        return remote(aout.at[at], ain.at[at], asend.at[p, d], arecv.at[p, d], peer(d))

    def factor_of(p, d):
        source = p * n_tp + flip(tp, d)

        @pl.when(source != me)
        def _():
            remote(
                factor_out, factors.at[source], fsend.at[0], frecv_f.at[source], peer(1)
            ).wait_recv()

        return factors[source][0:1, :]

    def silu(gate):
        return gate / (1.0 + jnp.exp(-gate))

    def activate(p, values=None):
        for d in range(n_tp):
            at = pl.ds(d * cap, cap)
            value = factor_of(p, d) if values is None else values[d]
            _, first, second = held(p, d)
            scale = jnp.sum(jnp.where(first | second, value, 0.0), axis=1, keepdims=True)
            made = silu(hg[p, at, :] * scale) * (hu[p, at, :] * scale) * wcol[p, at, :]
            made = made.astype(bf16)
            if d:
                aout[p, at, :] = made
                act_out(p, d).start()
            else:
                ain[p, at, :] = made

    def mix_in(p):
        for d in range(n_tp):
            if d:
                act_out(p, d).wait_recv()
            at = pl.ds(d * cap, cap)
            spread_act[p, d] = dot_tn(smat[p, at, :], ain[p, at, :]).astype(bf16)

    def own_spread(q):
        gather_out(2, q).start()
        gather_out(1, q).start()

    def own_relay(q):
        gather_out(2, q).wait_recv()
        gather_on(q).start()

    def own_unit(q):
        gather_out(1, q).wait_recv()
        gather_on(q).wait_recv()
        full = plane[:, cols(q)]
        crow[z, :, cols(q)] = dot(som[...], full).astype(bf16)
        shg[...] += dot(full, sg[cols(q), :])
        shu[...] += dot(full, su[cols(q), :])
        hidden(z, q)

    def own_activate():
        values = [factor_of(z, d) for d in range(n_tp)]
        activate(z, values)
        i, j = grid((rows, lanes))
        for d in range(n_tp):
            at = pl.ds(d * rows, rows)
            scale = jnp.sum(jnp.where(i == j, values[d], 0.0), axis=1, keepdims=True)
            sact[at, :] = (silu(shg[at, :] * scale) * (shu[at, :] * scale)).astype(bf16)

    def outcome(p, q):
        total = dot(spread_act[p, 0], ed[0, :, cols(q)])
        for d in range(1, n_tp):
            total = total + dot(spread_act[p, d], ed[d, :, cols(q)])
        return total

    def down_relay(q):
        @pl.when(lax.rem(q, 2) != group)
        def _():
            down_out(2, q).wait_recv()

        down_on(q).start()

    def down_ready(q):
        down_out(1, q).wait_recv()
        down_on(q).wait_recv()

    def chain_out(p, q, last, step):
        into, sem = chin.at[p, :, cols(q)], drecv.at[p, q]
        if last:
            side = (1 - step) // 2
            into, sem = fin.at[side, :, cols(q)], frecv.at[side, q]
        return remote(chs.at[p, :, cols(q)], into, dsend.at[p, q], sem, {"sp": z + step})

    def d_unit(p, q, incoming, last, step):
        total = outcome(p, q)
        if incoming:
            chain_out(p, q, False, step).wait_recv()
            total = total + chin[p, :, cols(q)].astype(f32)
        chs[p, :, cols(q)] = total.astype(bf16)
        chain_out(p, q, last, step).start()

    def product(d, q):
        return dot(sact[d * rows : (d + 1) * rows, :], sd[:, cols(q)])

    def rs1(q):
        for d in (3, 1):
            sent[d, :, cols(q)] = product(d, q).astype(bf16)
            fold(d, q, 1).start()

    def rs2(q):
        total = product(2, q)
        fold(3, q, 1).wait_recv()
        sent[2, :, cols(q)] = (total + got[3, :, cols(q)].astype(f32)).astype(bf16)
        fold(2, q, 2).start()

    def base(q):
        total = product(0, q) + outcome(z, q) + stream[:, cols(q)].astype(f32)
        fold(1, q, 1).wait_recv()
        total = total + got[1, :, cols(q)].astype(f32)
        fold(2, q, 2).wait_recv()
        facc[:, cols(q)] = total + got[2, :, cols(q)].astype(f32)

    def arrive(side, q):
        at = fin.at[side, :, cols(q)]
        remote(at, at, dsend.at[0, q], frecv.at[side, q], peer(1)).wait_recv()
        return fin[side, :, cols(q)].astype(f32)

    def run(*steps):
        def each(q):
            for step in steps:
                step(q)

        return each

    def at_first(step):
        def each(q):
            @pl.when(q == 0)
            def _():
                step()

        return each

    def at_last(step):
        def each(q):
            @pl.when(q == chunks - 1)
            def _():
                step()

        return each

    def spread_some(first, stop):
        def step():
            for k in range(first, stop):
                own_spread(k)

        return step

    def sends_done(copies):
        def one(q, carry):
            for copy in copies(q):
                copy.wait_send()
            return carry

        lax.fori_loop(0, chunks, one, 0)

    loads[0].wait()
    loads[1].wait()
    squares[...] = jnp.zeros_like(squares)
    is_end = (z == 0) | (z == n_sp - 1)
    ahead, behind = {"sp": z + way}, {"sp": z - way}

    def c_first(q):
        @pl.when(is_end)
        def _():
            c_unit(z + way, q)

        @pl.when(jnp.logical_not(is_end))
        def _():
            c_unit(z - way, q, 2, ahead)
            c_unit(z + way, q, 3, behind)

    def h_first(q):
        @pl.when(is_end)
        def _():
            h_unit(z + way, q)

        @pl.when(jnp.logical_not(is_end))
        def _():
            h_unit(z - way, q)
            h_unit(z + way, q)

    for k in (5, 6):
        loads[k].wait()
    staged(b1, b2, b3, None, c_first, None, h_first)

    for k in (2, 3, 4):
        loads[k].wait()

    @pl.when(is_end)
    def _():
        p0, p1, p2 = z + way, z + 2 * way, z + 3 * way
        staged(
            run(lambda q: c_unit(p1, q), down_relay, at_last(spread_some(0, chunks // 4))),
            at_first(lambda: activate(p0)),
            run(
                lambda q: h_unit(p1, q),
                at_first(lambda: mix_in(p0)),
                down_ready,
                lambda q: d_unit(p0, q, False, True, way),
            ),
        )
        staged(
            lambda q: c_unit(p2, q),
            at_first(lambda: activate(p1)),
            run(
                lambda q: h_unit(p2, q),
                at_first(lambda: mix_in(p1)),
                lambda q: d_unit(p1, q, False, False, way),
            ),
        )
        activate(p2)
        spread_some(chunks // 4, chunks)()
        mix_in(p2)
        staged(lambda q: d_unit(p2, q, False, False, way))
        staged(own_relay, own_unit)
        own_activate()
        staged(rs1, rs2)
        mix_in(z)
        staged(base)

        def last(q):
            out_ref[:, cols(q)] = (facc[:, cols(q)] + arrive((1 + way) // 2, q)).astype(bf16)

        staged(last)
        sends_done(
            lambda q: [own_out(q, way)]
            + [spread_out(p, d, q) for p in (p0, p1, p2) for d in (1, 2, 3)]
            + [chain_out(p, q, False, way) for p in (p0, p1, p2)]
        )

    @pl.when(jnp.logical_not(is_end))
    def _():
        s0, s1, s2 = z - way, z + way, z + 2 * way
        staged(
            run(lambda q: c_unit(s2, q, 4, behind), down_relay),
            run(at_first(lambda: activate(s0)), at_first(lambda: activate(s1))),
            run(lambda q: h_unit(s2, q), down_ready),
        )
        activate(s2)
        staged(own_spread)
        mix_in(s1)
        mix_in(s0)
        mix_in(s2)
        staged(run(own_relay, lambda q: d_unit(s1, q, True, True, way)), own_unit)
        own_activate()
        staged(
            run(lambda q: d_unit(s2, q, True, False, way), rs1),
            rs2,
            lambda q: d_unit(s0, q, True, True, -way),
        )
        mix_in(z)
        staged(base)

        def last(q):
            total = facc[:, cols(q)] + arrive(0, q) + arrive(1, q)
            out_ref[:, cols(q)] = total.astype(bf16)

        staged(last)
        sends_done(
            lambda q: [own_out(q, way), own_out(q, -way)]
            + [block_out(s0, q, 2, ahead), block_out(s1, q, 3, behind)]
            + [block_out(s2, q, 4, behind)]
            + [spread_out(p, d, q) for p in (s0, s1, s2) for d in (1, 2, 3)]
            + [chain_out(p, q, False, way) for p in (s0, s1, s2)]
        )

    sends_done(
        lambda q: [gather_out(2, q), gather_out(1, q), gather_on(q)]
        + [down_out(1, q), down_on(q)]
        + [f(d, q, 1) for f in (fold, first_fold) for d in (3, 1, 2)]
    )
    for i in range(chunks // 2):
        down_out(2, 2 * i + group).wait_send()
        down_across(2 * i + group).wait_send()
    for p in range(n_sp):
        for d in range(1, n_tp):
            act_out(p, d).wait_send()

    def finish(k):
        fact_out(k).wait_send()
        factor_send(k).wait_send()

    others(finish)

    def latents_done(block, carry):
        @pl.when(z < n_sp - 1)
        def _():
            for k in range(pieces):
                latent_out(block, k).wait_send()

        @pl.when(block < z)
        def _():
            for k in range(pieces):
                latent_over(block, k).wait_send()

        return carry

    lax.fori_loop(0, z + 1, latents_done, 0)


def rotary_tables(tokens, lanes):
    half = ROPE // 2
    lane = np.arange(lanes) % half
    inverse = np.float32(ROPE_BASE) ** (-lane.astype(np.float32) * np.float32(2.0 / ROPE))
    angles = np.arange(tokens, dtype=np.float32)[:, None] * inverse.astype(np.float32)[None, :]
    return jnp.asarray(np.cos(angles)), jnp.asarray(np.sin(angles))


def layer(near, far, n_sp, n_tp, cap, sizes, chunks=4):
    groups = len(sizes)
    tok, latent_width = near[0].shape
    key_ws, value_ws = (near[3 + k * groups : 3 + (k + 1) * groups] for k in (1, 2))
    residual = near[-1]
    lanes = ROPE + -ROPE % 128
    tables = rotary_tables(n_sp * tok, lanes)
    rows, width = residual.shape
    ow, on, sg, su, sd, eg, eu, ed = far
    slots = n_tp * cap
    hidden, share = eg.shape[0], sg.shape[1]
    bf16, f32 = jnp.bfloat16, jnp.float32
    count = n_sp * n_tp

    def sems(*shape):
        return pltpu.SemaphoreType.DMA(shape)

    def half(*shape):
        return pltpu.VMEM(shape, bf16)

    def full(*shape):
        return pltpu.VMEM(shape, f32)

    depth = sum(w.shape[1] for w in value_ws)
    number = sum(w.shape[1] // size for w, size in zip(value_ws, sizes))
    fact_shape = (8, rows + -rows % 128)
    scratch = [half(number, tok, 2 * lanes), full(-(-number // 8) * 8, tok)]
    scratch += [full(-(-number // 8) * 8, tok), full(depth, tok), half(depth, latent_width)]
    scratch += [full(tok, lanes), full(tok, lanes), full(*fact_shape)]
    scratch += [half(n_sp * tok, latent_width + lanes)]
    scratch += [half(tok, w.shape[1]) for w in value_ws]
    scratch += [full(count, *fact_shape), full(count, *fact_shape), full(*fact_shape)]
    scratch += [half(rows, width), half(rows, width)]
    scratch += [half(n_sp, rows, width), half(n_tp * rows, width)]
    scratch += [half(n_sp, slots, width)] * 2
    scratch += [half(n_sp, rows, width)] * 2 + [half(2, rows, width)]
    scratch += [half(n_tp, rows, width)] * 4
    scratch += [half(*w.shape) for w in far[:-1]] + [half(n_tp, *ed.shape)]
    scratch += [half(n_sp, slots, rows), half(slots, n_tp * rows), full(n_sp, slots, 1)]
    scratch += [full(n_sp, slots, hidden)] * 2
    scratch += [half(n_sp, slots, hidden)] * 2
    scratch += [half(n_sp, n_tp, rows, hidden)]
    scratch += [full(n_tp * rows, share)] * 2 + [half(n_tp * rows, share)]
    scratch += [full(rows, width), full(rows, 1)]
    scratch += [sems(10)] + [sems(n_sp, 2)] * 4
    scratch += [sems(count)] * 4
    scratch += [sems(n_tp, chunks)] * 2
    scratch += [sems(5, chunks), sems(n_sp, chunks)]
    scratch += [sems(n_sp, n_tp, chunks)] * 2
    scratch += [sems(n_sp, n_tp)] * 2
    scratch += [sems(n_sp, chunks), sems(n_sp, chunks), sems(2, chunks)]
    scratch += [sems(n_tp, chunks)] * 6 + [sems(chunks)]
    return pl.pallas_call(
        lambda *refs: layer_kernel(chunks, cap, sizes, *refs),
        out_shape=jax.ShapeDtypeStruct((rows, width), bf16),
        in_specs=[VMEM] * len(near) + [pl.BlockSpec(memory_space=pl.ANY)] * (len(far) + 2),
        out_specs=VMEM,
        scratch_shapes=scratch,
        compiler_params=pltpu.CompilerParams(
            collective_id=4, has_side_effects=True, vmem_limit_bytes=60 << 20
        ),
    )(*near, *far, *tables)


def rms_scale(values, gain):
    return values * lax.rsqrt(jnp.mean(values * values, axis=-1, keepdims=True) + EPS) * gain


def body(
    latent,
    rope_key,
    wide_query,
    narrow_query,
    wide_key_weight,
    wide_value_weight,
    narrow_key_weight,
    narrow_value_weight,
    latent_norm_scale,
    out_wide,
    out_narrow,
    residual,
    ffn_gain,
    shared_gate,
    shared_up,
    shared_down,
    expert_gate,
    expert_up,
    expert_down,
    routes,
    route_weights,
):
    tok_dev = latent.shape[0]
    seq_index = lax.axis_index("sp")
    own_pos = seq_index * tok_dev + jnp.arange(tok_dev, dtype=jnp.int32)
    n_sp, n_tp = lax.axis_size("sp"), lax.axis_size("tp")
    rows_here, top_count = routes.shape
    local_experts = expert_gate.shape[0]
    experts_all = local_experts * lax.axis_size(("sp", "tp"))
    capacity = max(2, 2 * top_count * rows_here // experts_all)
    queries = (wide_query, narrow_query)
    key_ws = (wide_key_weight, narrow_key_weight)
    value_ws = (wide_value_weight, narrow_value_weight)
    sizes = (WIDE_HEAD_SIZE, NARROW_HEAD_SIZE)
    planes = n_sp == 4 and n_tp == 4 and local_experts == 1 and capacity % 16 == 0
    if planes and top_count == 2 and rows_here <= 128 and lax.axis_size("grp") == 2:
        near = (latent, rope_key.T, latent_norm_scale[None, :], *queries, *key_ws, *value_ws)
        near += (routes.T, route_weights.T, ffn_gain[None, :], residual)
        far = (out_wide, out_narrow, shared_gate, shared_up, shared_down)
        far += (expert_gate[0].T, expert_up[0].T, expert_down[0])
        return layer(near, far, n_sp, n_tp, capacity, sizes)
    normed_latent = rms_scale(latent.astype(jnp.float32), latent_norm_scale).astype(jnp.bfloat16)
    half = ROPE // 2
    lane = jnp.arange(ROPE + -ROPE % 128, dtype=jnp.int32)
    inverse = ROPE_BASE ** (-(lane % half).astype(jnp.float32) * 2.0 / ROPE)
    angles = own_pos.astype(jnp.float32)[:, None] * inverse[None, :]
    cosine, sine = jnp.cos(angles), jnp.sin(angles)
    row = jnp.arange(ROPE, dtype=jnp.int32)[:, None]
    same = (row == lane[None, :]).astype(jnp.bfloat16)
    cross = (row == lane[None, :] - half).astype(jnp.bfloat16) * (lane < ROPE)[None, :] - (
        (row == lane[None, :] + half) & (lane < half)[None, :]
    ).astype(jnp.bfloat16)
    turned_key = (
        jnp.dot(rope_key, same, preferred_element_type=jnp.float32) * cosine
        + jnp.dot(rope_key, cross.astype(jnp.bfloat16), preferred_element_type=jnp.float32) * sine
    ).astype(jnp.bfloat16)
    flat_routes = routes.reshape(-1)
    assigned = flat_routes.shape[0]
    choose = (flat_routes[:, None] == jnp.arange(experts_all, dtype=jnp.int32)[None, :]).astype(
        jnp.float32
    )
    lower_mask = (jnp.arange(assigned)[:, None] > jnp.arange(assigned)[None, :]).astype(jnp.float32)
    earlier = jnp.dot(lower_mask, choose, precision=lax.Precision.HIGHEST)
    slots = jnp.sum(earlier * choose, axis=1).astype(jnp.int32)
    target = flat_routes * capacity + slots
    by_choice = target.reshape(rows_here, top_count)
    rows_packed = jnp.concatenate([normed_latent, turned_key], axis=1)
    packed = spread(rows_packed, n_sp, n_tp)
    wide_mix, narrow_mix = attend(packed, cosine, sine, queries, key_ws, value_ws, sizes)
    (projected,) = dot_scatter((wide_mix, narrow_mix), (out_wide, out_narrow), n_tp, 2)
    stream = (residual.astype(jnp.float32) + projected).astype(jnp.bfloat16)
    normed = rms_scale(stream.astype(jnp.float32), ffn_gain).astype(jnp.bfloat16)
    model_width = normed.shape[1]
    send_map = jnp.any(
        target.reshape(rows_here, top_count)[None, :, :]
        == jnp.arange(experts_all * capacity, dtype=jnp.int32)[:, None, None],
        axis=2,
    ).astype(jnp.bfloat16)
    outgoing = jnp.dot(send_map, normed, preferred_element_type=jnp.float32).astype(jnp.bfloat16)
    devices = n_sp * n_tp
    outgoing = outgoing.reshape(devices, local_experts * capacity, model_width)
    piece, incoming = gather_rows(normed, outgoing, n_tp)
    sources = devices
    incoming = incoming.reshape(experts_all, capacity, model_width)
    grouped = incoming.reshape(sources, local_experts, incoming.shape[1], model_width)
    gate_part = jnp.einsum(
        "sxcd,xdf->sxcf", grouped, expert_gate, preferred_element_type=jnp.float32
    )
    up_part = jnp.einsum("sxcd,xdf->sxcf", grouped, expert_up, preferred_element_type=jnp.float32)
    active = (jax.nn.silu(gate_part) * up_part).astype(jnp.bfloat16)
    finished = jnp.einsum(
        "sxcf,xfd->sxcd", active, expert_down, preferred_element_type=jnp.float32
    ).astype(jnp.bfloat16)
    gate_part = jnp.dot(piece, shared_gate, preferred_element_type=jnp.float32)
    up_part = jnp.dot(piece, shared_up, preferred_element_type=jnp.float32)
    active = (jax.nn.silu(gate_part) * up_part).astype(jnp.bfloat16)
    shared, returned = dot_scatter(
        (active,), (shared_down,), n_tp, 3, finished.reshape(outgoing.shape)
    )
    slot_rows = returned.reshape(experts_all * capacity, model_width)
    routed = jnp.zeros((rows_here, model_width), jnp.float32)
    for choice in range(top_count):
        hot = by_choice[:, choice : choice + 1] == jnp.arange(experts_all * capacity)[None, :]
        picked = jnp.dot(
            hot.astype(jnp.bfloat16), slot_rows, preferred_element_type=jnp.float32
        )
        routed = routed + picked * route_weights[:, choice : choice + 1]
    return (stream.astype(jnp.float32) + shared + routed).astype(jnp.bfloat16)


def solution(mesh):
    placed = (
        P(("grp", "sp"), None),
        P(("grp", "sp"), None),
        P(("grp", "sp"), "tp"),
        P(("grp", "sp"), "tp"),
        P(None, "tp"),
        P(None, "tp"),
        P(None, "tp"),
        P(None, "tp"),
        P(),
        P("tp", None),
        P("tp", None),
        P(("grp", "sp", "tp"), None),
        P(),
        P(None, "tp"),
        P(None, "tp"),
        P("tp", None),
        P(("sp", "tp"), None, None),
        P(("sp", "tp"), None, None),
        P(("sp", "tp"), None, None),
        P(("grp", "sp", "tp"), None),
        P(("grp", "sp", "tp"), None),
    )
    return jax.shard_map(
        body, mesh=mesh, in_specs=placed, out_specs=P(("grp", "sp", "tp"), None), check_vma=False
    )
```
